256 devices in a mesh: st: 64 (over z, y, core), tp: 4 (over x).
Axes of the slice: x: 4, y: 4, z: 8, core: 2. Of those that a mesh axis runs over, the one named last changes fastest.
Arguments:
- tokens: bfloat16 [24576, 2048], P('st', 'tp'), may hold values from -6 to 6
- cotangent: bfloat16 [24576, 1024], P('st', 'tp'), may hold values from -48 to 48
- mix_query: bfloat16 [24576, 1024], P('st', 'tp'), may hold values from -6 to 6
- mix_key: bfloat16 [24576, 1024], P('st', 'tp'), may hold values from -6 to 6
- mix_value: bfloat16 [24576, 1024], P('st', 'tp'), may hold values from -24 to 24
- beta_pre: float32 [8, 24576], P('tp', 'st'), may hold values from -9 to 9
- decay_pre: float32 [8, 24576], P('tp', 'st'), may hold values from -8 to 6
- decay_rate: float32 [8], P('tp'), may hold values from 0.001 to 0.06
- passages: bfloat16 [1024, 64, 2048], P('st'), may hold values from -16 to 16
- passage_ids: int32 [384, 4], P('st'), may hold values from 0 to 1023, as said below
- query_weight: bfloat16 [2048, 1024], P(None, 'tp'), may hold values from -0.125 to 0.125
- key_weight: bfloat16 [2048, 1024], P(None, 'tp'), may hold values from -0.125 to 0.125
- value_weight: bfloat16 [2048, 1024], P(None, 'tp'), may hold values from -0.125 to 0.125
- gate_weight: bfloat16 [4, 2048], P('tp'), may hold values from -0.125 to 0.125
Outputs:
- token_grad: bfloat16 [24576, 2048], P('st', 'tp')
- passage_grad: bfloat16 [1024, 64, 2048], P('st', None, 'tp')
- key_weight_grad: float32 [2048, 1024], P('st', 'tp')
The draws below stay inside these ranges and needn't reach their ends.
Inputs may be any that keep to these rules, and one draw needn't show every extreme that they name: Passage p is stored on index p // 16 of st. The rows of passage_ids read by one index of st name at most 1 passages stored on any one index of st, and exactly 1 on some.
All inputs are finite; a program needn't handle non-finite values.
Results may differ from the reference program's by a relative error of at most 0.012.
The reference program's roundings to bfloat16 on the way count: a program that leaves them out, or rounds other values in their place, can miss the bound.
Values may be sent and summed in bfloat16 or wider, within the bound.
A program may use at most 128 MiB of HBM per device.

```python
import math
import jax
import jax.numpy as jnp
from jax import lax

D = 2048
HEADS = 4
HEAD = 256
MIX_HEADS = 8
MIX_DIM = 128
SPAN = 64
BLOCK = 64
PER_BLOCK = 4
PROWS = 64
TOK_DEV = 384
PASS_DEV = 16
TOKENS = 24576
BLOCKS = 384
REQ_DEV = 24
CAP = 1
PASSAGES = 1024
N_ST = 64


def draw_passage_ids(key, part):
    slot_count = N_ST * CAP
    shift_table = jax.random.randint(jax.random.fold_in(key, 9001), (N_ST,), 0, PASS_DEV)

    def per_reader(reader_idx):
        keys_split = jax.random.split(jax.random.fold_in(key, reader_idx), 4)
        rank_score = jax.random.permutation(keys_split[0], slot_count).astype(jnp.int32)
        slot_owner = jnp.arange(slot_count, dtype=jnp.int32) // CAP
        forced = (slot_owner == (reader_idx - 1) % N_ST) | (slot_owner == (reader_idx + N_ST // 2) % N_ST)
        rank_score = rank_score + forced.astype(jnp.int32) * (2 * slot_count)
        _, chosen = lax.top_k(rank_score, REQ_DEV)
        chosen = chosen.astype(jnp.int32)[jax.random.permutation(keys_split[1], REQ_DEV)]
        owner_ids = chosen // CAP
        first_draw = jax.random.randint(keys_split[2], (REQ_DEV,), 0, PASS_DEV)
        second_draw = jax.random.randint(keys_split[3], (REQ_DEV,), 0, PASS_DEV)
        local_ids = (jnp.minimum(first_draw, second_draw) + shift_table[owner_ids]) % PASS_DEV
        return (owner_ids * PASS_DEV + local_ids).astype(jnp.int32)
    every_id = jax.vmap(per_reader)(jnp.arange(N_ST, dtype=jnp.int32))
    return every_id.reshape(BLOCKS, PER_BLOCK)


def draw_decay_pre(key, part):
    keys_split = jax.random.split(key, 3)
    noise_part = 0.7 * jax.random.normal(keys_split[0], (MIX_HEADS, TOKENS), jnp.float32)
    slow_part = jax.random.uniform(keys_split[1], (MIX_HEADS, TOKENS // SPAN), jnp.float32, -1.2, 1.2)
    device_part = jax.random.uniform(keys_split[2], (MIX_HEADS, N_ST), jnp.float32, -1.0, 1.0)
    values_out = noise_part + jnp.repeat(slow_part, SPAN, axis=1) + jnp.repeat(device_part, TOK_DEV, axis=1)
    return jnp.clip(values_out, -8.0, 6.0)


def spiked(array, rng, source, target, parts, factor):
    owner, partner = [(jnp.arange(array.shape[dim]) // (array.shape[dim] // parts)).reshape([-1 if axis == dim else 1 for axis in range(array.ndim)]) for dim in (source, target)]
    chosen = jax.random.permutation(rng, parts)[partner]
    strong = (owner == chosen) | (owner == (partner + parts // 2) % parts)
    return jnp.where(strong, factor * array, array)


def level_of(key, extent, cuts, low, largest):
    def one(axis_at, blocks):
        draws = jax.random.uniform(jax.random.fold_in(jax.random.fold_in(key, 6), axis_at), (blocks,), jnp.float32, low / len(cuts), largest / len(cuts))
        return jnp.repeat(jnp.exp(draws), extent[axis_at] // blocks).reshape((-1,) + (1,) * (len(extent) - axis_at - 1))

    level = one(*cuts[0])
    for cut in cuts[1:]:
        level = level * one(*cut)
    return level


def scatter_about(rng, shape, scale, reach, pieces=(), kind=jnp.bfloat16):
    loudness = level_of(rng, shape, pieces, -0.22, 0.18) if pieces else 1.0
    values = jax.random.normal(rng, shape, jnp.float32) * scale * loudness
    return jnp.minimum(jnp.maximum(values, -reach), reach).astype(kind)


def noise_with(rng, extent, deviation, most, cuts, heavy, kind=jnp.bfloat16):
    entries = deviation * jax.random.normal(rng, extent, jnp.float32)
    if cuts:
        entries = entries * level_of(rng, extent, cuts, -0.22, 0.18)
    return jnp.clip(spiked(entries, jax.random.fold_in(rng, 3), *heavy), -most, most).astype(kind)


def setup_inputs(seed: int = 0) -> dict:
    streams_of = jax.random.split(jax.random.key(seed), 15)
    tokens = scatter_about(streams_of[0], (TOKENS, D), 1.0, 6.0, ((0, 64), (1, 4)))
    cotangent = scatter_about(streams_of[1], (TOKENS, HEADS * HEAD), 8.0, 48.0, ((0, 64), (1, 4)))
    mix_query = scatter_about(streams_of[2], (TOKENS, MIX_HEADS * MIX_DIM), 1.0, 6.0, ((0, 64), (1, 4)))
    mix_key = scatter_about(streams_of[3], (TOKENS, MIX_HEADS * MIX_DIM), 1.0, 6.0, ((0, 64), (1, 4)))
    mix_value = scatter_about(streams_of[4], (TOKENS, MIX_HEADS * MIX_DIM), 4.0, 24.0, ((0, 64), (1, 4)))
    beta_pre = scatter_about(streams_of[5], (MIX_HEADS, TOKENS), 1.5, 9.0, ((0, 4), (1, 64)), jnp.float32)
    decay_pre = draw_decay_pre(jax.random.fold_in(streams_of[14], 71), 0)
    decay_rate = jnp.clip(jnp.exp(math.log(0.06) - 4.0943445 * jax.random.uniform(streams_of[7], (MIX_HEADS,), jnp.float32) ** level_of(streams_of[7], (MIX_HEADS,), ((0, 4),), -0.2, 0.2)), 0.001, 0.06)
    passages = noise_with(streams_of[8], (PASSAGES, PROWS, D), 1.0, 16.0, ((0, 64),), (0, 2, 64, 4.0))
    passage_ids = draw_passage_ids(jax.random.fold_in(streams_of[14], 71), 0)
    query_weight = scatter_about(streams_of[10], (D, HEADS * HEAD), D ** -0.5, 0.125, ((1, 4),))
    key_weight = scatter_about(streams_of[11], (D, HEADS * HEAD), D ** -0.5, 0.125, ((1, 4),))
    value_weight = scatter_about(streams_of[12], (D, HEADS * HEAD), D ** -0.5, 0.125, ((1, 4),))
    gate_weight = scatter_about(streams_of[13], (HEADS, D), D ** -0.5, 0.125, ((0, 4),))
    return dict(tokens=tokens, cotangent=cotangent, mix_query=mix_query, mix_key=mix_key, mix_value=mix_value, beta_pre=beta_pre, decay_pre=decay_pre, decay_rate=decay_rate, passages=passages, passage_ids=passage_ids, query_weight=query_weight, key_weight=key_weight, value_weight=value_weight, gate_weight=gate_weight)


NORM_FLOOR = 1.0
SCORE_GAIN = 4.0
HIGHEST = lax.Precision.HIGHEST

def to_low(value):
    return lax.optimization_barrier(value.astype(jnp.bfloat16))

def neumann_inverse(strict_part):
    span_size = strict_part.shape[-1]
    unit_eye = jnp.eye(span_size, dtype=jnp.float32)
    running = unit_eye - strict_part
    power_term = strict_part
    for _ in range(span_size.bit_length() - 2):
        power_term = jnp.einsum('...ij,...jk->...ik', power_term, power_term, precision=HIGHEST)
        running = jnp.einsum('...ij,...jk->...ik', running, unit_eye + power_term, precision=HIGHEST)
    return running

def delta_mixer(queries, keys_in, values_in, strength, log_decay):
    heads_n, length, key_dim = queries.shape
    blocks_n = length // SPAN

    def to_blocks(tensor):
        return tensor.reshape(heads_n, blocks_n, SPAN, *tensor.shape[2:])
    queries, keys_in, values_in = (to_blocks(queries), to_blocks(keys_in), to_blocks(values_in))
    strength, log_decay = (to_blocks(strength), to_blocks(log_decay))
    cumulative = jnp.cumsum(log_decay, axis=-1)
    position = jnp.arange(SPAN)
    inclusive = position[:, None] >= position[None, :]
    strictly = position[:, None] > position[None, :]
    spread = jnp.where(inclusive, cumulative[..., :, None] - cumulative[..., None, :], -jnp.inf)
    decay_map = jnp.exp(spread)
    key_gram = jnp.einsum('hncd,hnmd->hncm', keys_in, keys_in, precision=HIGHEST)
    strict_part = jnp.where(strictly, strength[..., :, None] * key_gram * decay_map, 0.0)
    inverse = neumann_inverse(strict_part)
    fresh_vals = jnp.einsum('hncm,hnme->hnce', inverse, values_in * strength[..., None], precision=HIGHEST)
    correction = jnp.einsum('hncm,hnmd->hncd', inverse, keys_in * (strength * jnp.exp(cumulative))[..., None], precision=HIGHEST)
    attend_map = jnp.where(inclusive, jnp.einsum('hncd,hnmd->hncm', queries, keys_in, precision=HIGHEST) * decay_map, 0.0)
    query_dec = queries * jnp.exp(cumulative)[..., None]
    key_dec = keys_in * jnp.exp(cumulative[..., -1:] - cumulative)[..., None]
    carry_decay = jnp.exp(cumulative[..., -1])

    def advance(memory_state, inputs):
        fresh_blk, correct_blk, attend_blk, query_blk, key_blk, decay_blk = inputs
        new_values = fresh_blk - jnp.einsum('hcd,hde->hce', correct_blk, memory_state, precision=HIGHEST)
        output = jnp.einsum('hcd,hde->hce', query_blk, memory_state, precision=HIGHEST) + jnp.einsum('hcm,hme->hce', attend_blk, new_values, precision=HIGHEST)
        memory_state = memory_state * decay_blk[:, None, None] + jnp.einsum('hcd,hce->hde', key_blk, new_values, precision=HIGHEST)
        return (memory_state, output)
    stacked = tuple((jnp.moveaxis(tensor, 1, 0) for tensor in (fresh_vals, correction, attend_map, query_dec, key_dec, carry_decay)))
    initial = jnp.zeros((heads_n, key_dim, values_in.shape[-1]), jnp.float32)
    _, outputs = lax.scan(advance, initial, stacked)
    return jnp.transpose(outputs, (1, 0, 2, 3)).reshape(heads_n, length, -1)

def mixer_output(query_raw, key_raw, value_raw, beta_raw, decay_raw, rate_vals):
    length = query_raw.shape[0]
    heads_n = beta_raw.shape[0]

    def heads_first(matrix):
        return jnp.transpose(matrix.astype(jnp.float32).reshape(length, heads_n, -1), (1, 0, 2))
    queries = heads_first(query_raw)
    keys_in = heads_first(key_raw)
    values_in = heads_first(value_raw)
    queries = queries * lax.rsqrt(lax.optimization_barrier(jnp.sum(queries * queries, axis=-1, keepdims=True)) + NORM_FLOOR) * queries.shape[-1] ** (-0.5)
    keys_in = keys_in * lax.rsqrt(lax.optimization_barrier(jnp.sum(keys_in * keys_in, axis=-1, keepdims=True)) + NORM_FLOOR)
    strength = jax.nn.sigmoid(beta_raw)
    log_decay = -rate_vals[:, None] * jax.nn.softplus(decay_raw)
    mixer_out = delta_mixer(queries, keys_in, values_in, strength, log_decay)
    return jnp.transpose(mixer_out, (1, 0, 2)).reshape(length, -1)

def request_slots(id_rows, pass_count):
    owners = id_rows // pass_count
    local_idx = id_rows % pass_count
    req_count = id_rows.shape[-1]
    req_order = jnp.arange(req_count, dtype=jnp.int32)
    earlier = (owners[..., :, None] == owners[..., None, :]) & (req_order[None, :] < req_order[:, None])
    ranks = lax.optimization_barrier(jnp.sum(earlier.astype(jnp.int32), axis=-1, dtype=jnp.int32))
    return (owners, local_idx, ranks)

def reference(tokens, cotangent, mix_query, mix_key, mix_value, beta_pre, decay_pre, decay_rate, passages, passage_ids, query_weight, key_weight, value_weight, gate_weight):
    score_scale = SCORE_GAIN * HEAD ** (-0.5)
    every_id = passage_ids.reshape(N_ST, REQ_DEV)
    query_heads = query_weight.astype(jnp.float32).reshape(D, HEADS, HEAD)
    key_heads = key_weight.astype(jnp.float32).reshape(D, HEADS, HEAD)
    value_heads = value_weight.astype(jnp.float32).reshape(D, HEADS, HEAD)
    gate_float = gate_weight.astype(jnp.float32)
    blocks_n = TOK_DEV // BLOCK

    def reader(reader_idx):
        first_row = reader_idx * TOK_DEV
        tok_block = lax.dynamic_slice_in_dim(tokens, first_row, TOK_DEV, 0)
        query_low = to_low(jnp.dot(tok_block, query_weight, preferred_element_type=jnp.float32))
        query_float = query_low.astype(jnp.float32).reshape(TOK_DEV, HEADS, HEAD)
        query_scale = lax.rsqrt(lax.optimization_barrier(jnp.mean(query_float * query_float, axis=-1, keepdims=True)) + NORM_FLOOR)
        query_hat = to_low(query_float * query_scale)
        gate_open = jax.nn.sigmoid(jnp.dot(tok_block, gate_weight.T, preferred_element_type=jnp.float32))
        row_block = passages[every_id[reader_idx]].reshape(REQ_DEV * PROWS, D)
        key_low = to_low(jnp.dot(row_block, key_weight, preferred_element_type=jnp.float32))
        key_float = key_low.astype(jnp.float32).reshape(REQ_DEV * PROWS, HEADS, HEAD)
        key_scale = lax.rsqrt(lax.optimization_barrier(jnp.mean(key_float * key_float, axis=-1, keepdims=True)) + NORM_FLOOR)
        key_hat = to_low(key_float * key_scale)
        value_low = to_low(jnp.dot(row_block, value_weight, preferred_element_type=jnp.float32))
        key_blocks = key_hat.astype(jnp.float32).reshape(blocks_n, PER_BLOCK * PROWS, HEADS, HEAD)
        value_blocks = value_low.astype(jnp.float32).reshape(blocks_n, PER_BLOCK * PROWS, HEADS, HEAD)
        query_blocks = query_hat.astype(jnp.float32).reshape(blocks_n, BLOCK, HEADS, HEAD)
        scores = jnp.einsum('bihd,bjhd->bhij', query_blocks, key_blocks) * score_scale
        exp_scores = jnp.exp(scores)
        attn_probs = exp_scores / lax.optimization_barrier(jnp.sum(exp_scores, axis=-1, keepdims=True))
        probs_low = to_low(attn_probs).astype(jnp.float32)
        retrieved = jnp.einsum('bhij,bjhd->bihd', probs_low, value_blocks).reshape(TOK_DEV, HEADS, HEAD)
        mixer_out = mixer_output(lax.dynamic_slice_in_dim(mix_query, first_row, TOK_DEV, 0), lax.dynamic_slice_in_dim(mix_key, first_row, TOK_DEV, 0), lax.dynamic_slice_in_dim(mix_value, first_row, TOK_DEV, 0), lax.dynamic_slice_in_dim(beta_pre, first_row, TOK_DEV, 1), lax.dynamic_slice_in_dim(decay_pre, first_row, TOK_DEV, 1), decay_rate).reshape(TOK_DEV, HEADS, HEAD)
        grad_out = lax.dynamic_slice_in_dim(cotangent, first_row, TOK_DEV, 0).astype(jnp.float32).reshape(TOK_DEV, HEADS, HEAD)
        grad_ret = to_low(gate_open[..., None] * grad_out).astype(jnp.float32)
        gate_grad = lax.optimization_barrier(jnp.sum(grad_out * (retrieved - mixer_out), axis=-1)) * gate_open * (1.0 - gate_open)
        grad_blocks = grad_ret.reshape(blocks_n, BLOCK, HEADS, HEAD)
        grad_probs = jnp.einsum('bihd,bjhd->bhij', grad_blocks, value_blocks)
        score_grad = to_low(attn_probs * (grad_probs - lax.optimization_barrier(jnp.sum(grad_probs * attn_probs, axis=-1, keepdims=True)))).astype(jnp.float32)
        qhat_grad = score_scale * jnp.einsum('bhij,bjhd->bihd', score_grad, key_blocks).reshape(TOK_DEV, HEADS, HEAD)
        khat_grad = to_low(score_scale * jnp.einsum('bhij,bihd->bjhd', score_grad, query_blocks)).astype(jnp.float32).reshape(REQ_DEV, PROWS, HEADS, HEAD)
        value_grad = to_low(jnp.einsum('bhij,bihd->bjhd', probs_low, grad_blocks)).astype(jnp.float32).reshape(REQ_DEV, PROWS, HEADS, HEAD)
        query_grad = to_low(query_scale * qhat_grad - query_scale ** 3 * query_float * lax.optimization_barrier(jnp.mean(query_float * qhat_grad, axis=-1, keepdims=True))).astype(jnp.float32)
        partial_value = jnp.einsum('thd,ehd->the', query_grad, query_heads) + gate_grad[..., None] * gate_float[None]
        token_rows = lax.optimization_barrier(jnp.sum(to_low(partial_value).astype(jnp.float32), axis=1)).astype(jnp.bfloat16)
        return (token_rows, khat_grad, value_grad)
    token_rows, khat_all, value_all = lax.map(reader, jnp.arange(N_ST, dtype=jnp.int32))
    owner_all, local_all, rank_all = request_slots(every_id, PASS_DEV)
    cap_iota = jnp.arange(CAP, dtype=jnp.int32)
    req_iota = jnp.arange(REQ_DEV, dtype=jnp.int32)
    readers = jnp.arange(N_ST, dtype=jnp.int32)[:, None]
    pass_iota = jnp.arange(PASS_DEV, dtype=jnp.int32)

    def owner_step(weight_acc, owner_idx):
        wanted = (owner_all == owner_idx)[:, None, :] & (rank_all[:, None, :] == cap_iota[None, :, None])
        slot_used = jnp.any(wanted, axis=-1)
        slot_local = lax.optimization_barrier(jnp.sum(jnp.where(wanted, local_all[:, None, :], 0), axis=-1, dtype=jnp.int32))
        req_pick = lax.optimization_barrier(jnp.sum(jnp.where(wanted, req_iota[None, None, :], 0), axis=-1, dtype=jnp.int32))
        khat_slots = jnp.where(slot_used[:, :, None, None, None], khat_all[readers, req_pick], 0.0)
        value_slots = jnp.where(slot_used[:, :, None, None, None], value_all[readers, req_pick], 0.0)
        onehot = ((slot_local.reshape(-1)[None, :] == pass_iota[:, None]) & slot_used.reshape(-1)[None, :]).astype(jnp.float32)
        khat_pass = jnp.dot(onehot, khat_slots.reshape(N_ST * CAP, -1), precision=HIGHEST).reshape(PASS_DEV * PROWS, HEADS, HEAD)
        value_pass = jnp.dot(onehot, value_slots.reshape(N_ST * CAP, -1), precision=HIGHEST).reshape(PASS_DEV * PROWS, HEADS, HEAD)
        row_block = lax.dynamic_slice_in_dim(passages, owner_idx * PASS_DEV, PASS_DEV, 0).reshape(PASS_DEV * PROWS, D)
        key_low = to_low(jnp.dot(row_block, key_weight, preferred_element_type=jnp.float32))
        key_float = key_low.astype(jnp.float32).reshape(PASS_DEV * PROWS, HEADS, HEAD)
        key_scale = lax.rsqrt(lax.optimization_barrier(jnp.mean(key_float * key_float, axis=-1, keepdims=True)) + NORM_FLOOR)
        key_grad = to_low(key_scale * khat_pass - key_scale ** 3 * key_float * lax.optimization_barrier(jnp.mean(key_float * khat_pass, axis=-1, keepdims=True)))
        value_grad_low = to_low(value_pass)
        partial_value = jnp.einsum('rhd,ehd->rhe', key_grad.astype(jnp.float32), key_heads) + jnp.einsum('rhd,ehd->rhe', value_grad_low.astype(jnp.float32), value_heads)
        rows_grad = lax.optimization_barrier(jnp.sum(to_low(partial_value).astype(jnp.float32), axis=1)).astype(jnp.bfloat16).reshape(PASS_DEV, PROWS, D)
        weight_acc = weight_acc + jnp.dot(row_block.T, key_grad.reshape(PASS_DEV * PROWS, HEADS * HEAD), preferred_element_type=jnp.float32)
        return (weight_acc, rows_grad)
    weight_grad, store_grad = lax.scan(owner_step, jnp.zeros((D, HEADS * HEAD), jnp.float32), jnp.arange(N_ST, dtype=jnp.int32))
    return (token_rows.reshape(TOKENS, D), store_grad.reshape(PASSAGES, PROWS, D), weight_grad)
```

```python
import functools

import jax
import jax.numpy as jnp
from jax import lax
from jax.experimental import pallas as pl
from jax.experimental.pallas import tpu as pltpu
from jax.sharding import PartitionSpec as P

SPAN = 64
BLOCK = 64
NORM_FLOOR = 1.0
SCORE_GAIN = 4.0
HIGHEST = lax.Precision.HIGHEST
CONTRACT_LAST = (((1,), (1,)), ((), ()))
CONTRACT_FIRST = (((0,), (0,)), ((), ()))
F32, BF16 = jnp.float32, jnp.bfloat16

MESH = pl.DeviceIdType.MESH
VMEM_SPEC = pl.BlockSpec(memory_space=pltpu.VMEM)
ANY_SPEC = pl.BlockSpec(memory_space=pl.ANY)
SMEM_SPEC = pl.BlockSpec(memory_space=pltpu.SMEM)
DMA = pltpu.SemaphoreType.DMA

ZN, YN, CN, XN = 8, 4, 2, 4
ROW = 128


def settle_kernel(*refs):
    count = len(refs) // 2
    for source, target in zip(refs[:count], refs[count:]):
        target[...] = source[...]


def settle_call(*arrays):
    return pl.pallas_call(
        settle_kernel,
        out_shape=tuple(jax.ShapeDtypeStruct(x.shape, x.dtype) for x in arrays),
        in_specs=[VMEM_SPEC] * len(arrays),
        out_specs=(VMEM_SPEC,) * len(arrays),
        name="settle",
    )(*arrays)


def exact_dot(left, right, dims=(((1,), (0,)), ((), ()))):
    return lax.dot_general(left, right, dims, precision=HIGHEST, preferred_element_type=F32)


def low_dot(left, right, dims=(((1,), (0,)), ((), ()))):
    return lax.dot_general(left, right, dims, preferred_element_type=F32)


def mixer_span(queries, keys_in, values_in, strength, log_decay, state):
    span = queries.shape[0]
    row_at = lax.broadcasted_iota(jnp.int32, (span, span), 0)
    col_at = lax.broadcasted_iota(jnp.int32, (span, span), 1)
    inclusive = row_at >= col_at
    unit_eye = jnp.where(row_at == col_at, 1.0, 0.0)
    decay_row = jnp.sum(unit_eye * log_decay, axis=0, keepdims=True)
    cum_row = jnp.sum(jnp.where(row_at <= col_at, log_decay, 0.0), axis=0, keepdims=True)
    cum_col = jnp.sum(jnp.where(inclusive, decay_row, 0.0), axis=1, keepdims=True)
    total = jnp.sum(log_decay, axis=0, keepdims=True)
    decay_map = jnp.exp(jnp.where(inclusive, cum_col - cum_row, -1e30))
    queries = (
        queries
        * lax.rsqrt(jnp.sum(queries * queries, axis=-1, keepdims=True) + NORM_FLOOR)
        * queries.shape[-1] ** (-0.5)
    )
    keys_in = keys_in * lax.rsqrt(jnp.sum(keys_in * keys_in, axis=-1, keepdims=True) + NORM_FLOOR)
    power = jnp.where(
        row_at > col_at, strength * exact_dot(keys_in, keys_in, CONTRACT_LAST) * decay_map, 0.0
    )
    inverse = unit_eye - power
    for _ in range(span.bit_length() - 2):
        power = exact_dot(power, power)
        inverse = exact_dot(inverse, unit_eye + power)
    attend = exact_dot(queries, keys_in, CONTRACT_LAST) * decay_map
    fresh = exact_dot(inverse, values_in * strength)
    correction = exact_dot(inverse, keys_in * (strength * jnp.exp(cum_col)))
    new_values = fresh - exact_dot(correction, state)
    output = exact_dot(queries * jnp.exp(cum_col), state) + exact_dot(attend, new_values)
    state = state * jnp.exp(total) + exact_dot(
        keys_in * jnp.exp(total - cum_col), new_values, CONTRACT_FIRST
    )
    return output, state


def scratch_spec(tok_n, rows_n, width, head, heads_n, mix_dim):
    model = width * XN
    slab = YN * CN
    passes = rows_n // BLOCK
    chunks = rows_n // ROW
    half = chunks // 2
    part = model // (ZN * slab)
    keys = slab * BLOCK
    vmem = dict(
        rows_v=((rows_n, model), BF16),
        kw=((model, head), BF16),
        vw=((model, head), BF16),
        qw=((model, head), BF16),
        tok4=((XN, tok_n, width), BF16),
        kv=((slab * passes, BLOCK, 2 * head), BF16),
        qc=((ZN, 2, tok_n, head), BF16),
        gates=((ZN, 8, tok_n), F32),
        mq=((tok_n, head), BF16),
        mk=((tok_n, head), BF16),
        mv=((tok_n, head), BF16),
        ids_all=((CN, ZN, 8, 128), jnp.int32),
        tab_v=((2, CN * ZN, 128), jnp.int32),
        code=((YN, CN, 8, ZN * BLOCK), jnp.int32),
        turned=((tok_n, 8), F32),
        mixed=((tok_n, head), F32),
        states=((heads_n, mix_dim, mix_dim), F32),
        key_low=((rows_n, head), BF16),
        query_low=((tok_n, head), BF16),
        query_grad=((tok_n, head), BF16),
        gate_grad=((tok_n, 1), F32),
        gw=((1, model), F32),
        kvr=((keys, 2 * head), BF16),
        e_buf=((ZN, keys, tok_n), F32),
        g_buf=((keys, tok_n), F32),
        sg=((keys, tok_n), BF16),
        pg=((keys, tok_n), BF16),
        zt=((ZN, 2, tok_n), F32),
        zt_r=((ZN, ZN, 2, tok_n), F32),
        terms=((YN, CN, ZN, BLOCK, 2 * head), BF16),
        term_r=((YN, ZN, BLOCK, 2 * head), BF16),
        qg=((ZN, tok_n, head), BF16),
        z_s=((2, ZN // 2, tok_n, head), BF16),
        z_r=((2, ZN // 2, tok_n, head), BF16),
        yf_s=((2, half, ROW, 2 * head), BF16),
        yf_r=((2, half, ROW, 2 * head), BF16),
        yd_s=((2, chunks, ROW, 2 * head), BF16),
        yd_r=((2, chunks, ROW, 2 * head), BF16),
        key_grad=((rows_n, head), BF16),
        value_grad=((rows_n, head), BF16),
        xf_s=((2, half, ROW, width), BF16),
        xf_r=((2, half, ROW, width), BF16),
        xd_s=((2, chunks, ROW, width), BF16),
        xd_r=((2, chunks, ROW, width), BF16),
        tf_s=((2, tok_n // 2, width), BF16),
        tf_r=((2, tok_n // 2, width), BF16),
        td_s=((2, 2, tok_n // 2, width), BF16),
        td_r=((2, 2, tok_n // 2, width), BF16),
        wbuf=((CN, YN, ZN, part, head), BF16),
        wc_r=((YN, ZN, part, head), BF16),
        w1=((YN, ZN, part, head), BF16),
        wy_r=((YN, ZN, part, head), BF16),
        w2=((ZN, part, head), BF16),
        wz_r=((ZN, part, head), BF16),
    )
    sems = dict(
        load=(16,),
        idsem=(2, CN, ZN),
        tokx=(2, 2, 2),
        cotz=(2, ZN // 2, 2),
        qz=(2, ZN // 2, 2),
        gz=(2, ZN // 2, 2),
        kvy=(2, 2, 2, 4),
        kvd=(2, YN, 4),
        zts=(2, ZN),
        ters=(2, YN),
        zrs=(2, 2, ZN // 2),
        yfs=(2, 2, half),
        yds=(2, 2, chunks),
        xfs=(2, 2, half),
        xds=(2, 2, chunks),
        tfs=(2, 2),
        tds=(2, 2, 2),
        wcs=(2,),
        wys=(2, YN),
        wzs=(2, ZN),
    )
    return vmem, sems


def fused_kernel(names, *refs):
    r = dict(zip(names, refs))

    def get(*keys):
        return [r[k] for k in keys]

    rate, ids, gate_w, beta, decay = get("rate", "ids", "gate_w", "beta", "decay")
    tok_out, out_ref, weight_ref = get("tok_out", "out_ref", "weight_ref")
    rows_v, kw, vw, qw, tok4, kv, qc, gates = get(
        "rows_v", "kw", "vw", "qw", "tok4", "kv", "qc", "gates"
    )
    tab_v, tab_s, code = get("tab_v", "tab_s", "code")
    kvr, e_buf, g_buf, sg, pg, zt, zt_r = get("kvr", "e_buf", "g_buf", "sg", "pg", "zt", "zt_r")
    terms, term_r, qg, z_s, z_r = get("terms", "term_r", "qg", "z_s", "z_r")
    key_low, key_grad, value_grad = get("key_low", "key_grad", "value_grad")
    query_low, query_grad, gate_grad = get("query_low", "query_grad", "gate_grad")
    turned, mixed, states = get("turned", "mixed", "states")
    gw = r["gw"]

    rows_n, model = rows_v.shape
    head = kw.shape[1]
    tok_n, width = tok_out.shape
    heads_n = beta.shape[0]
    mix_dim = head // heads_n
    slab = YN * CN
    passes = rows_n // BLOCK
    chunks = rows_n // ROW
    half = chunks // 2
    per_dev = tok_n // BLOCK
    score_scale = SCORE_GAIN * head ** (-0.5)

    st = lax.axis_index("st")
    x = lax.axis_index("tp")
    c = lax.rem(st, CN)
    y = lax.rem(st // CN, YN)
    z = st // slab
    other = 1 - c

    def at(zi, yi, ci):
        return (zi * YN + yi) * CN + ci

    def step(value, by, n):
        return lax.rem(value + (by % n), n)

    xs = [step(x, i, XN) for i in range(XN)]
    ys = [step(y, i, YN) for i in range(YN)]
    zs = [step(z, i, ZN) for i in range(ZN)]
    partner = at(z, y, other)
    x_to = (xs[1], xs[XN - 1])
    y_to = (at(z, ys[1], c), at(z, ys[YN - 1], c))
    z_to = (at(zs[1], y, c), at(zs[ZN - 1], y, c))

    started = []

    def remote(src, dst, sem, index, st_id=None, tp_id=None):
        sems = r[sem]
        device = {}
        if st_id is not None:
            device["st"] = st_id
        if tp_id is not None:
            device["tp"] = tp_id
        return pltpu.make_async_remote_copy(
            src_ref=src,
            dst_ref=dst,
            send_sem=sems.at[(0, *index)],
            recv_sem=sems.at[(1, *index)],
            device_id=device,
            device_id_type=MESH,
        )

    def go(copy):
        copy.start()
        started.append(copy)

    loads = {}

    def load(key, src, dst):
        loads[key] = pltpu.make_async_copy(src, dst, r["load"].at[len(loads)])
        loads[key].start()

    load("cot", r["cot_h"], qc.at[z, 1])
    load("tok", r["tok_h"], tok4.at[x])
    load("kw", r["kw_h"], kw)
    load("vw", r["vw_h"], vw)
    proj_rows = rows_n // 4
    proj_order = (0, 2, 1, 3)
    for k in proj_order:
        here = pl.ds(k * proj_rows, proj_rows)
        load(("rows", k), r["rows_h"].at[here, :], rows_v.at[here, :])
    load("mq", r["mq_h"], r["mq"])
    load("mk", r["mk_h"], r["mk"])
    load("mv", r["mv_h"], r["mv"])
    load("qw", r["qw_h"], qw)

    barrier = pltpu.get_barrier_semaphore()
    greeted = 0
    for target in x_to:
        pl.semaphore_signal(barrier, inc=1, device_id={"tp": target}, device_id_type=MESH)
        greeted += 1
    friends = [partner] + [at(z, ys[d], c) for d in range(1, YN)]
    friends += [at(zs[d], y, ci) for d in range(1, ZN) for ci in (c, other)]
    for target in friends:
        pl.semaphore_signal(barrier, inc=1, device_id={"st": target}, device_id_type=MESH)
        greeted += 1
    pl.semaphore_wait(barrier, greeted)

    t_half = tok_n // 2
    half_rows = (pl.ds(0, t_half), pl.ds(t_half, t_half))

    def cot_copy(hop, d):
        source = zs[(1 - hop) % ZN] if d == 0 else zs[(hop - 1) % ZN]
        ref = qc.at[source, 1]
        if hop == ZN // 2:
            ref = qc.at[source, 1, half_rows[d]]
        return remote(ref, ref, "cotz", (hop - 1, d), st_id=z_to[d])

    def q_copies(hop, d):
        source = zs[(1 - hop) % ZN] if d == 0 else zs[(hop - 1) % ZN]
        ref = qc.at[source, 0]
        if hop == ZN // 2:
            ref = qc.at[source, 0, half_rows[d]]
        copies = [remote(ref, ref, "qz", (hop - 1, d), st_id=z_to[d])]
        if hop < ZN // 2 or d == 0:
            copies.append(
                remote(gates.at[source], gates.at[source], "gz", (hop - 1, d), st_id=z_to[d])
            )
        return copies

    def tok_copy(hop, d):
        if hop == 1:
            ref = tok4.at[x]
        else:
            ref = tok4.at[xs[XN - 1] if d == 0 else xs[1], half_rows[d]]
        return remote(ref, ref, "tokx", (hop - 1, d), tp_id=x_to[d])

    loads["tok"].wait()
    for d in range(2):
        go(tok_copy(1, d))
    loads["cot"].wait()
    for d in range(2):
        go(cot_copy(1, d))

    def ids_copy(dc, dz):
        return remote(
            ids, r["ids_all"].at[c, z], "idsem", (dc, dz), st_id=at(zs[dz], y, other if dc else c)
        )

    id_peers = [(dc, dz) for dz in range(ZN) for dc in range(CN) if (dc, dz) != (0, 0)]
    for dc, dz in id_peers:
        go(ids_copy(dc, dz))
    r["ids_all"][c, z] = ids[...]

    per_chunk = proj_rows // BLOCK

    def kv_piece(yi, ci, k):
        return kv.at[pl.ds((yi * CN + ci) * passes + k * per_chunk, per_chunk)]

    def kv_copy(hop, d, k):
        yi = y if hop == 1 else (ys[YN - 1] if d == 0 else ys[1])
        ref = kv_piece(yi, c, k)
        return remote(ref, ref, "kvy", (hop - 1, d, k), st_id=y_to[d])

    def kv_across(rel, k):
        ref = kv_piece(ys[rel], c, k)
        return remote(ref, ref, "kvd", (rel, k), st_id=partner)

    loads["kw"].wait()
    loads["vw"].wait()
    for k in proj_order:
        loads[("rows", k)].wait()
        here = pl.ds(k * proj_rows, proj_rows)
        block = rows_v[here, :]
        low = low_dot(block, kw[...]).astype(BF16)
        key_low[here, :] = low
        low = low.astype(F32)
        scale = lax.rsqrt(jnp.mean(low * low, axis=-1, keepdims=True) + NORM_FLOOR)
        first = (y * CN + c) * passes + k * per_chunk
        kv[pl.ds(first, per_chunk), :, :head] = (
            (low * scale).astype(BF16).reshape(per_chunk, BLOCK, head)
        )
        kv[pl.ds(first, per_chunk), :, head:] = (
            low_dot(block, vw[...]).astype(BF16).reshape(per_chunk, BLOCK, head)
        )
        for d in range(2):
            go(kv_copy(1, d, k))
        go(kv_across(0, k))

    for dc, dz in id_peers:
        ids_copy(dc, dz).wait_recv()
    every = jnp.concatenate(
        [r["ids_all"][ci, zi, 0:1, :] for ci in range(CN) for zi in range(ZN)], axis=0
    )
    lane = lax.broadcasted_iota(jnp.int32, (CN * ZN, 128), 1)
    loc_tab = jnp.zeros((CN * ZN, 128), jnp.int32)
    blk_tab = jnp.zeros((CN * ZN, 128), jnp.int32)
    owner = lax.shift_right_logical(every, 4)
    local = every & (passes - 1)
    for o in range(slab):
        match = (owner == z * slab + o) & (lane < per_dev * 4)
        loc = jnp.sum(jnp.where(match, local, 0), axis=1, keepdims=True)
        blk = jnp.sum(
            jnp.where(match, lax.shift_right_logical(lane, 2) + 1, 0), axis=1, keepdims=True
        )
        loc_tab = jnp.where(lane == o, jnp.minimum(loc, passes - 1), loc_tab)
        blk_tab = jnp.where(lane == o, blk - 1, blk_tab)
    tab_v[0] = loc_tab
    tab_v[1] = blk_tab
    tab_copy = pltpu.make_async_copy(tab_v, tab_s, r["load"].at[len(loads)])
    tab_copy.start()

    gw[...] = gate_w[...].astype(F32)
    turned[...] = jnp.transpose(
        jnp.concatenate(
            [beta[...], decay[...], jnp.zeros((8 - 2 * heads_n, tok_n), F32)], axis=0
        )
    )
    states[...] = jnp.zeros_like(states)
    for key in ("mq", "mk", "mv", "qw"):
        loads[key].wait()

    def mix(b):
        here = pl.ds(pl.multiple_of(b * SPAN, SPAN), SPAN)
        for m in range(heads_n):
            cols = pl.ds(m * mix_dim, mix_dim)
            raw = turned[here, heads_n + m : heads_n + m + 1]
            softplus = jnp.maximum(raw, 0.0) + jnp.log1p(jnp.exp(-jnp.abs(raw)))
            mixed[here, cols], states[m] = mixer_span(
                r["mq"][here, cols].astype(F32),
                r["mk"][here, cols].astype(F32),
                r["mv"][here, cols].astype(F32),
                jax.nn.sigmoid(turned[here, m : m + 1]),
                -rate[m] * softplus,
                states[m],
            )

    spans_n = tok_n // SPAN

    def cot_pass(hop):
        for d in range(2):
            cot_copy(hop - 1, d).wait_recv()
            go(cot_copy(hop, d))

    def q_pass(hop):
        for d in range(2):
            for copy in q_copies(hop - 1, d):
                copy.wait_recv()
            for copy in q_copies(hop, d):
                go(copy)

    def kv_pass(k):
        for d, rel in ((0, YN - 1), (1, 1)):
            kv_copy(1, d, k).wait_recv()
            if (k < 2) == (d == 0):
                go(kv_copy(2, d, k))
            go(kv_across(rel, k))

    pl.loop(0, 1)(mix)
    cot_pass(2)
    for d in range(2):
        tok_copy(1, d).wait_recv()
        go(tok_copy(2, d))
    pl.loop(1, 2)(mix)
    for d in range(2):
        tok_copy(2, d).wait_recv()

    gate_rows = jnp.broadcast_to(gate_w[...], (16, model))
    logit = low_dot(gate_rows[:, :width], tok4[0], CONTRACT_LAST)
    for i in range(1, XN):
        logit += low_dot(gate_rows[:, i * width : (i + 1) * width], tok4[i], CONTRACT_LAST)
    gates[z] = jax.nn.sigmoid(logit[:8])

    @pl.loop(0, tok_n // ROW)
    def _(k):
        here = pl.ds(pl.multiple_of(k * ROW, ROW), ROW)
        low = low_dot(tok4[0, here, :], qw[pl.ds(0, width), :])
        for i in range(1, XN):
            low += low_dot(tok4[i, here, :], qw[pl.ds(i * width, width), :])
        low = low.astype(BF16)
        query_low[here, :] = low
        low = low.astype(F32)
        scale = lax.rsqrt(jnp.mean(low * low, axis=-1, keepdims=True) + NORM_FLOOR)
        qc[z, 0, here, :] = (low * scale).astype(BF16)

    for d in range(2):
        for copy in q_copies(1, d):
            go(copy)
    cot_pass(3)
    kv_pass(0)
    pl.loop(2, 4)(mix)
    kv_pass(2)
    cot_pass(4)
    q_pass(2)
    pl.loop(4, spans_n)(mix)
    kv_pass(1)
    q_pass(3)
    kv_pass(3)
    q_pass(4)
    tab_copy.wait()
    lane_of = lax.broadcasted_iota(jnp.int32, (8, ZN * BLOCK), 1)
    for yi in range(YN):
        for which, ci in ((0, c), (1, other)):
            start = jnp.full((8, ZN * BLOCK), -1000000, jnp.int32)
            for zi in range(ZN):
                row = ci * ZN + zi
                base = jnp.where(
                    tab_s[1, row, yi * CN + c] >= 0,
                    tab_s[0, row, yi * CN + c] * BLOCK,
                    -1000000,
                )
                start = jnp.where(lax.shift_right_logical(lane_of, 6) == zi, base, start)
            code[yi, which] = start + (lane_of & (BLOCK - 1))
    for d in range(2):
        cot_copy(ZN // 2, d).wait_recv()
        for copy in q_copies(ZN // 2, d):
            copy.wait_recv()
    for d, k in ((0, 0), (1, 2), (0, 1), (1, 3)):
        kv_copy(2, d, k).wait_recv()
        go(kv_across(2, k))
    for rel in range(YN):
        for k in range(4):
            kv_across(rel, k).wait_recv()

    tok_block = lax.shift_right_logical(lax.broadcasted_iota(jnp.int32, (BLOCK, tok_n), 1), 6)
    key_halves = [pl.ds(i * ROW * 2, ROW * 2) for i in range(slab * BLOCK // (2 * ROW))]

    def gather(reader):
        for o in range(slab):
            local_at = jnp.clip(tab_s[0, c * ZN + reader, o], 0, passes - 1)
            kvr[pl.ds(o * BLOCK, BLOCK), :] = kv[o * passes + local_at]

    @pl.loop(0, ZN)
    def _(reader):
        gather(reader)
        for part in key_halves:
            e_buf[reader, part, :] = low_dot(kvr[part, :head], qc[reader, 0], CONTRACT_LAST)
            g_buf[part, :] = low_dot(kvr[part, head:], qc[reader, 1], CONTRACT_LAST)
        total = jnp.zeros((1, tok_n), F32)
        product = jnp.zeros((1, tok_n), F32)
        for o in range(slab):
            here = pl.ds(o * BLOCK, BLOCK)
            mine = tok_block == tab_s[1, c * ZN + reader, o]
            e = jnp.where(mine, jnp.exp(e_buf[reader, here, :] * score_scale), 0.0)
            e_buf[reader, here, :] = e
            total += jnp.sum(e, axis=0, keepdims=True)
            product += jnp.sum(e * g_buf[here, :], axis=0, keepdims=True)
        zt[reader, 0:1, :] = total
        zt[reader, 1:2, :] = product * gates[reader, 0:1, :]

    def zt_copy(d):
        return remote(zt, zt_r.at[d], "zts", (d,), st_id=at(zs[d], y, c))

    for d in range(1, ZN):
        go(zt_copy(d))
    for d in range(1, ZN):
        zt_copy(d).wait_recv()

    def summed(reader):
        both = zt[reader]
        for d in range(1, ZN):
            both += zt_r[d, reader]
        return both[0:1, :], both[1:2, :]

    @pl.loop(0, ZN)
    def _(i):
        reader = lax.rem(z + jnp.where(lax.rem(i, 2) == 1, 4 - (i + 1) // 2, 4 + i // 2), ZN)
        total, product = summed(reader)
        inverse = 1.0 / total
        mean = product * inverse
        gate = gates[reader, 0:1, :]
        gather(reader)
        for part in key_halves:
            g_buf[part, :] = low_dot(kvr[part, head:], qc[reader, 1], CONTRACT_LAST)
        for o in range(slab):
            here = pl.ds(o * BLOCK, BLOCK)
            probs = e_buf[reader, here, :] * inverse
            sg[here, :] = (probs * (g_buf[here, :] * gate - mean)).astype(BF16)
            pg[here, :] = (probs * gate).astype(BF16)
        for n, part in enumerate(key_halves):
            key_term = (low_dot(sg[part, :], qc[reader, 0]) * score_scale).astype(BF16)
            value_term = low_dot(pg[part, :], qc[reader, 1]).astype(BF16)
            for k in range(2 * ROW // BLOCK):
                o = n * (2 * ROW // BLOCK) + k
                piece = slice(k * BLOCK, (k + 1) * BLOCK)
                terms[o // CN, o % CN, reader, :, :head] = key_term[piece]
                terms[o // CN, o % CN, reader, :, head:] = value_term[piece]
        qg[reader] = (low_dot(sg[...], kvr[:, :head], CONTRACT_FIRST) * score_scale).astype(BF16)

    def z_copy(hop, d):
        if hop == 1:
            src = qg.at[zs[ZN // 2], half_rows[d]]
            dst = z_r.at[d, 0, half_rows[d]]
        else:
            src = z_s.at[d, hop - 1]
            dst = z_r.at[d, hop - 1]
        return remote(src, dst, "zrs", (d, hop - 1), st_id=z_to[d])

    def z_pass(hop):
        for d in range(2):
            z_copy(hop - 1, d).wait_recv()
            away = ZN // 2 + 1 - hop
            target = zs[away] if d == 0 else zs[(-away) % ZN]
            if hop == 2:
                mid, rest = half_rows[d], half_rows[1 - d]
                z_s[d, hop - 1, mid, :] = (
                    qg[target, mid, :].astype(F32) + z_r[d, 0, mid, :].astype(F32)
                ).astype(BF16)
                z_s[d, hop - 1, rest, :] = qg[target, rest, :]
            else:
                z_s[d, hop - 1] = (
                    qg[target].astype(F32) + z_r[d, hop - 2].astype(F32)
                ).astype(BF16)
            go(z_copy(hop, d))

    def term_copy(rel):
        return remote(
            terms.at[ys[rel], other], term_r.at[ys[rel]], "ters", (rel,), st_id=partner
        )

    for rel in (2, 1, 3, 0):
        go(term_copy(rel))
    for d in range(2):
        go(z_copy(1, d))

    row_iota = lax.broadcasted_iota(jnp.int32, (ROW, ZN * BLOCK), 0)

    def pick(rel, q):
        yi = ys[rel]
        rows = row_iota + q * ROW
        ones = [
            jnp.where(rows == code[yi, which, 0:1, :], 1.0, 0.0).astype(BF16) for which in range(2)
        ]
        return low_dot(ones[0], terms[yi, c].reshape(ZN * BLOCK, 2 * head)) + low_dot(
            ones[1], term_r[yi].reshape(ZN * BLOCK, 2 * head)
        )

    yf_s, yf_r, yd_s, yd_r = get("yf_s", "yf_r", "yd_s", "yd_r")
    xf_s, xf_r, xd_s, xd_r = get("xf_s", "xf_r", "xd_s", "xd_r")

    def two_step(far_s, far_r, near_s, near_r, far_sem, near_sem, term, axis):
        def target(d):
            return {"st_id": y_to[d]} if axis == "y" else {"tp_id": x_to[d]}

        def far(d, j):
            return remote(far_s.at[d, j], far_r.at[d, j], far_sem, (d, j), **target(d))

        def near(d, q):
            return remote(near_s.at[d, q], near_r.at[d, q], near_sem, (d, q), **target(d))

        def send(j):
            for d in range(2):
                q = j + half * d
                far_s[d, j] = term(2, q).astype(BF16)
                go(far(d, j))
            for d in range(2):
                q = j + half * (1 - d)
                near_s[d, q] = term(1 if d == 0 else 3, q).astype(BF16)
                go(near(d, q))

        def forward(j):
            for d in range(2):
                q = j + half * d
                value = term(1 if d == 0 else 3, q)
                far(d, j).wait_recv()
                near_s[d, q] = (value + far_r[d, j].astype(F32)).astype(BF16)
                go(near(d, q))

        def final(q):
            value = term(0, q)
            for d in range(2):
                near(d, q).wait_recv()
            return value + near_r[0, q].astype(F32) + near_r[1, q].astype(F32)

        return send, forward, final

    y_send, y_forward, y_final = two_step(yf_s, yf_r, yd_s, yd_r, "yfs", "yds", pick, "y")

    def row_term(rel, q):
        here = pl.ds(q * ROW, ROW)
        cols = pl.ds(pl.multiple_of(xs[rel] * width, width), width)
        return low_dot(key_grad[here, :], kw[cols, :], CONTRACT_LAST) + low_dot(
            value_grad[here, :], vw[cols, :], CONTRACT_LAST
        )

    x_send, x_forward, x_final = two_step(xf_s, xf_r, xd_s, xd_r, "xfs", "xds", row_term, "x")

    def finish_rows(j):
        for q in (j, j + half):
            here = pl.ds(q * ROW, ROW)
            value = y_final(q)
            hat = value[:, :head]
            low = key_low[here, :].astype(F32)
            scale = lax.rsqrt(jnp.mean(low * low, axis=-1, keepdims=True) + NORM_FLOOR)
            key_grad[here, :] = (
                scale * hat
                - scale * scale * scale * low * jnp.mean(low * hat, axis=-1, keepdims=True)
            ).astype(BF16)
            value_grad[here, :] = value[:, head:].astype(BF16)

    def finish_out(j):
        for q in (j, j + half):
            out_ref[pl.ds(q * ROW, ROW), :] = x_final(q).astype(out_ref.dtype)

    for rel in (2, 1, 3):
        term_copy(rel).wait_recv()
    y_send(0)
    y_send(1)
    y_forward(0)
    z_pass(2)
    y_send(2)
    y_forward(1)
    z_pass(3)
    y_send(3)
    term_copy(0).wait_recv()
    finish_rows(0)
    x_send(0)
    z_pass(4)
    y_forward(2)
    x_forward(0)

    for d in range(2):
        z_copy(ZN // 2, d).wait_recv()
    total, product = summed(z)
    stack = jnp.transpose(
        jnp.concatenate(
            [gates[z, 0:1, :], product / total, jnp.zeros((6, tok_n), F32)], axis=0
        )
    )

    for k in range(tok_n // ROW):
        here = pl.ds(k * ROW, ROW)
        hat_grad = qg[z, here, :].astype(F32)
        for d in range(2):
            hat_grad += z_r[d, ZN // 2 - 1, here, :].astype(F32)
        low = query_low[here, :].astype(F32)
        scale = lax.rsqrt(jnp.mean(low * low, axis=-1, keepdims=True) + NORM_FLOOR)
        query_grad[here, :] = (
            scale * hat_grad
            - scale * scale * scale * low * jnp.mean(low * hat_grad, axis=-1, keepdims=True)
        ).astype(BF16)
        opened = stack[k * ROW : (k + 1) * ROW, 0:1]
        ratio = stack[k * ROW : (k + 1) * ROW, 1:2]
        along = jnp.sum(
            qc[z, 1, here, :].astype(F32) * mixed[here, :], axis=-1, keepdims=True
        )
        gate_grad[here, :] = (1.0 - opened) * (ratio - opened * along)

    tf_s, tf_r, td_s, td_r = get("tf_s", "tf_r", "td_s", "td_r")

    def token_term(rel, h):
        cols = pl.ds(pl.multiple_of(xs[rel] * width, width), width)
        here = half_rows[h]
        return (
            low_dot(query_grad[here, :], qw[cols, :], CONTRACT_LAST)
            + gate_grad[here, :] * gw[:, cols]
        )

    def t_far(d):
        return remote(tf_s.at[d], tf_r.at[d], "tfs", (d,), tp_id=x_to[d])

    def t_near(d, h):
        return remote(td_s.at[d, h], td_r.at[d, h], "tds", (d, h), tp_id=x_to[d])

    for d in range(2):
        tf_s[d] = token_term(2, d).astype(BF16)
        go(t_far(d))
    for d in range(2):
        td_s[d, 1 - d] = token_term(1 if d == 0 else 3, 1 - d).astype(BF16)
        go(t_near(d, 1 - d))

    finish_rows(1)
    x_send(1)
    y_forward(3)
    for d in range(2):
        value = token_term(1 if d == 0 else 3, d)
        t_far(d).wait_recv()
        td_s[d, d] = (value + tf_r[d].astype(F32)).astype(BF16)
        go(t_near(d, d))
    x_forward(1)
    finish_out(0)
    finish_rows(2)
    x_send(2)
    finish_rows(3)
    x_send(3)

    wbuf, wc_r, w1, wy_r, w2, wz_r = get("wbuf", "wc_r", "w1", "wy_r", "w2", "wz_r")
    part = weight_ref.shape[0]

    @pl.loop(0, ZN)
    def _(k):
        cols = pl.ds(pl.multiple_of(k * slab * part, slab * part), slab * part)
        tile = low_dot(rows_v[:, cols], key_grad[...], CONTRACT_FIRST).astype(BF16)
        for o in range(slab):
            wbuf[o % CN, o // CN, k] = tile[o * part : (o + 1) * part]

    wc_copy = remote(wbuf.at[other], wc_r, "wcs", (), st_id=partner)
    go(wc_copy)
    x_forward(2)
    wc_copy.wait_recv()
    for yi in range(YN):
        w1[yi] = (wbuf[c, yi].astype(F32) + wc_r[yi].astype(F32)).astype(BF16)

    def wy_copy(d):
        return remote(w1.at[ys[d]], wy_r.at[d], "wys", (d,), st_id=at(z, ys[d], c))

    def wz_copy(d):
        return remote(w2.at[zs[d]], wz_r.at[d], "wzs", (d,), st_id=at(zs[d], y, c))

    for d in (2, 1, 3):
        go(wy_copy(d))
    finish_out(1)
    for d in range(1, YN):
        wy_copy(d).wait_recv()
    gathered = w1[y].astype(F32)
    for d in range(1, YN):
        gathered += wy_r[d].astype(F32)
    w2[...] = gathered.astype(BF16)
    for d in (4, 3, 5, 2, 6, 1, 7):
        go(wz_copy(d))
    x_forward(3)
    for h in range(2):
        value = token_term(0, h)
        for d in range(2):
            t_near(d, h).wait_recv()
        tok_out[half_rows[h], :] = (
            value + td_r[0, h].astype(F32) + td_r[1, h].astype(F32)
        ).astype(tok_out.dtype)
    finish_out(2)
    for d in range(1, ZN):
        wz_copy(d).wait_recv()
    weight = w2[z].astype(F32)
    for d in range(1, ZN):
        weight += wz_r[d].astype(F32)
    weight_ref[...] = weight
    finish_out(3)
    for copy in started:
        copy.wait_send()


def fused_call(rate, ids, gate_w, beta, decay, tok, cot, mq, mk, mv, qw, kw, vw, rows):
    tok_n, width = tok.shape
    rows_n, model = rows.shape
    head = kw.shape[1]
    heads_n = beta.shape[0]
    vmem, sems = scratch_spec(tok_n, rows_n, width, head, heads_n, head // heads_n)
    part = model // (ZN * YN * CN)
    ins = ["rate", "ids", "gate_w", "beta", "decay"]
    ins += ["tok_h", "cot_h", "mq_h", "mk_h", "mv_h", "qw_h", "kw_h", "vw_h", "rows_h"]
    names = ins + ["tok_out", "out_ref", "weight_ref"] + list(vmem) + ["tab_s"] + list(sems)
    return pl.pallas_call(
        functools.partial(fused_kernel, names),
        out_shape=(
            jax.ShapeDtypeStruct((tok_n, width), BF16),
            jax.ShapeDtypeStruct((rows_n, width), BF16),
            jax.ShapeDtypeStruct((part, head), F32),
        ),
        in_specs=[SMEM_SPEC] + [VMEM_SPEC] * 4 + [ANY_SPEC] * 9,
        out_specs=(VMEM_SPEC,) * 3,
        scratch_shapes=[pltpu.VMEM(*v) for v in vmem.values()]
        + [pltpu.SMEM((2, CN * ZN, 128), jnp.int32)]
        + [DMA(s) for s in sems.values()],
        compiler_params=pltpu.CompilerParams(
            collective_id=0, has_side_effects=True, vmem_limit_bytes=67043328
        ),
        name="fused",
    )(rate, ids, gate_w, beta, decay, tok, cot, mq, mk, mv, qw, kw, vw, rows)


def body(
    tokens,
    cotangent,
    mix_query,
    mix_key,
    mix_value,
    beta_pre,
    decay_pre,
    decay_rate,
    passages,
    passage_ids,
    query_weight,
    key_weight,
    value_weight,
    gate_weight,
):
    pass_local, span_rows, model_width = passages.shape
    flat_rows = passages.reshape(pass_local * span_rows, model_width)
    req_count = passage_ids.size
    ids = jnp.pad(passage_ids.reshape(1, req_count), ((0, 7), (0, -req_count % 128)))
    token_grad, passage_grad, key_weight_grad = fused_call(
        decay_rate,
        ids,
        gate_weight,
        beta_pre,
        decay_pre,
        tokens,
        cotangent,
        mix_query,
        mix_key,
        mix_value,
        query_weight,
        key_weight,
        value_weight,
        flat_rows,
    )
    token_grad, passage_grad, key_weight_grad = settle_call(
        token_grad, passage_grad, key_weight_grad
    )
    return (token_grad, passage_grad.reshape(pass_local, span_rows, -1), key_weight_grad)


def solution(mesh):
    placed = (
        P("st", "tp"),
        P("st", "tp"),
        P("st", "tp"),
        P("st", "tp"),
        P("st", "tp"),
        P("tp", "st"),
        P("tp", "st"),
        P("tp"),
        P("st", None, None),
        P("st", None),
        P(None, "tp"),
        P(None, "tp"),
        P(None, "tp"),
        P("tp", None),
    )
    return jax.shard_map(
        body,
        mesh=mesh,
        in_specs=placed,
        out_specs=(P("st", "tp"), P("st", None, "tp"), P("st", "tp")),
        check_vma=False,
    )
```

```python
import functools

import jax
import jax.numpy as jnp
from jax import lax
from jax.experimental import pallas as pl
from jax.experimental.pallas import tpu as pltpu
from jax.sharding import PartitionSpec as P

SPAN = 64
BLOCK = 64
NORM_FLOOR = 1.0
SCORE_GAIN = 4.0
HIGHEST = lax.Precision.HIGHEST
CONTRACT_LAST = (((1,), (1,)), ((), ()))
CONTRACT_FIRST = (((0,), (0,)), ((), ()))
F32, BF16 = jnp.float32, jnp.bfloat16

MESH = pl.DeviceIdType.MESH
VMEM_SPEC = pl.BlockSpec(memory_space=pltpu.VMEM)
ANY_SPEC = pl.BlockSpec(memory_space=pl.ANY)
SMEM_SPEC = pl.BlockSpec(memory_space=pltpu.SMEM)
DMA = pltpu.SemaphoreType.DMA

ZN, YN, CN, XN = 8, 4, 2, 4
ROW = 128


def settle_kernel(*refs):
    count = len(refs) // 2
    for source, target in zip(refs[:count], refs[count:]):
        target[...] = source[...]


def settle_call(*arrays):
    return pl.pallas_call(
        settle_kernel,
        out_shape=tuple(jax.ShapeDtypeStruct(x.shape, x.dtype) for x in arrays),
        in_specs=[VMEM_SPEC] * len(arrays),
        out_specs=(VMEM_SPEC,) * len(arrays),
        name="settle",
    )(*arrays)


def exact_dot(left, right, dims=(((1,), (0,)), ((), ()))):
    return lax.dot_general(left, right, dims, precision=HIGHEST, preferred_element_type=F32)


def low_dot(left, right, dims=(((1,), (0,)), ((), ()))):
    return lax.dot_general(left, right, dims, preferred_element_type=F32)


def mixer_span(queries, keys_in, values_in, strength, log_decay, state):
    span = queries.shape[0]
    row_at = lax.broadcasted_iota(jnp.int32, (span, span), 0)
    col_at = lax.broadcasted_iota(jnp.int32, (span, span), 1)
    inclusive = row_at >= col_at
    unit_eye = jnp.where(row_at == col_at, 1.0, 0.0)
    decay_row = jnp.sum(unit_eye * log_decay, axis=0, keepdims=True)
    cum_row = jnp.sum(jnp.where(row_at <= col_at, log_decay, 0.0), axis=0, keepdims=True)
    cum_col = jnp.sum(jnp.where(inclusive, decay_row, 0.0), axis=1, keepdims=True)
    total = jnp.sum(log_decay, axis=0, keepdims=True)
    decay_map = jnp.exp(jnp.where(inclusive, cum_col - cum_row, -1e30))
    queries = (
        queries
        * lax.rsqrt(jnp.sum(queries * queries, axis=-1, keepdims=True) + NORM_FLOOR)
        * queries.shape[-1] ** (-0.5)
    )
    keys_in = keys_in * lax.rsqrt(jnp.sum(keys_in * keys_in, axis=-1, keepdims=True) + NORM_FLOOR)
    power = jnp.where(
        row_at > col_at, strength * exact_dot(keys_in, keys_in, CONTRACT_LAST) * decay_map, 0.0
    )
    inverse = unit_eye - power
    for _ in range(span.bit_length() - 2):
        power = exact_dot(power, power)
        inverse = exact_dot(inverse, unit_eye + power)
    attend = exact_dot(queries, keys_in, CONTRACT_LAST) * decay_map
    fresh = exact_dot(inverse, values_in * strength)
    correction = exact_dot(inverse, keys_in * (strength * jnp.exp(cum_col)))
    new_values = fresh - exact_dot(correction, state)
    output = exact_dot(queries * jnp.exp(cum_col), state) + exact_dot(attend, new_values)
    state = state * jnp.exp(total) + exact_dot(
        keys_in * jnp.exp(total - cum_col), new_values, CONTRACT_FIRST
    )
    return output, state


def scratch_spec(tok_n, rows_n, width, head, heads_n, mix_dim):
    model = width * XN
    slab = YN * CN
    passes = rows_n // BLOCK
    chunks = rows_n // ROW
    half = chunks // 2
    part = model // (ZN * slab)
    keys = slab * BLOCK
    vmem = dict(
        rows_v=((rows_n, model), BF16),
        kw=((model, head), BF16),
        vw=((model, head), BF16),
        qw=((model, head), BF16),
        tok4=((XN, tok_n, width), BF16),
        kv=((slab * passes, BLOCK, 2 * head), BF16),
        qc=((ZN, 2, tok_n, head), BF16),
        gates=((ZN, 8, tok_n), F32),
        mq=((tok_n, head), BF16),
        mk=((tok_n, head), BF16),
        mv=((tok_n, head), BF16),
        ids_all=((CN, ZN, 8, 128), jnp.int32),
        tab_v=((2, CN * ZN, 128), jnp.int32),
        code=((YN, CN, 8, ZN * BLOCK), jnp.int32),
        turned=((tok_n, 8), F32),
        mixed=((tok_n, head), F32),
        states=((heads_n, mix_dim, mix_dim), F32),
        key_low=((rows_n, head), BF16),
        query_low=((tok_n, head), BF16),
        kvr=((keys, 2 * head), BF16),
        e_buf=((ZN, keys, tok_n), F32),
        g_buf=((keys, tok_n), F32),
        sg=((keys, tok_n), BF16),
        pg=((keys, tok_n), BF16),
        zt=((ZN, 2, tok_n), F32),
        zt_r=((ZN, ZN, 2, tok_n), F32),
        terms=((CN, ZN, YN, BLOCK, 2 * head), BF16),
        term_r=((ZN, YN, BLOCK, 2 * head), BF16),
        qg=((ZN, tok_n, head), BF16),
        z_s=((2, ZN // 2, tok_n, head), BF16),
        z_r=((2, ZN // 2, tok_n, head), BF16),
        yf_s=((2, half, ROW, 2 * head), BF16),
        yf_r=((2, half, ROW, 2 * head), BF16),
        yd_s=((2, chunks, ROW, 2 * head), BF16),
        yd_r=((2, chunks, ROW, 2 * head), BF16),
        key_grad=((rows_n, head), BF16),
        kgv=((XN, rows_n, 2 * head), BF16),
        qga=((XN, tok_n, head), BF16),
        gga=((XN, 8, tok_n), F32),
        w_all=((XN, CN, 3, width // CN, head), BF16),
        gwb=((8, model), F32),
        gw_all=((XN, 8, width), F32),
        wbuf=((CN, YN, ZN, part, head), BF16),
        wc_r=((YN, ZN, part, head), BF16),
        w1=((YN, ZN, part, head), BF16),
        wy_r=((YN, ZN, part, head), BF16),
        w2=((ZN, part, head), BF16),
        wz_r=((ZN, part, head), BF16),
    )
    sems = dict(
        load=(16,),
        idsem=(2, CN, ZN),
        tokx=(2, 2, 2),
        cotz=(2, ZN // 2, 2),
        qz=(2, ZN // 2, 2, 2),
        gz=(2, ZN // 2, 2),
        kvy=(2, 2, 2, 4),
        kvd=(2, YN, 4),
        zts=(2, ZN, ZN),
        ters=(2, ZN),
        zrs=(2, 2, ZN // 2),
        yfs=(2, 2, half),
        yds=(2, 2, chunks),
        xrs=(2, 2, 2, chunks),
        tgs=(2, 2, 2),
        ggs=(2, 2, 2),
        wxs=(2, 3, XN),
        wxd=(2, XN),
        gws=(2, XN),
        wcs=(2,),
        wys=(2, YN),
        wzs=(2, ZN),
    )
    return vmem, sems


def fused_kernel(names, *refs):
    r = dict(zip(names, refs))

    def get(*keys):
        return [r[k] for k in keys]

    rate, ids, gate_w, beta, decay = get("rate", "ids", "gate_w", "beta", "decay")
    tok_out, out_ref, weight_ref = get("tok_out", "out_ref", "weight_ref")
    rows_v, kw, vw, qw, tok4, kv, qc, gates = get(
        "rows_v", "kw", "vw", "qw", "tok4", "kv", "qc", "gates"
    )
    tab_v, tab_s, code = get("tab_v", "tab_s", "code")
    kvr, e_buf, g_buf, sg, pg, zt, zt_r = get("kvr", "e_buf", "g_buf", "sg", "pg", "zt", "zt_r")
    terms, term_r, qg, z_s, z_r = get("terms", "term_r", "qg", "z_s", "z_r")
    key_low, key_grad, query_low = get("key_low", "key_grad", "query_low")
    kgv, qga, gga, w_all, gwb, gw_all = get("kgv", "qga", "gga", "w_all", "gwb", "gw_all")
    turned, mixed, states = get("turned", "mixed", "states")

    rows_n, model = rows_v.shape
    head = kw.shape[1]
    tok_n, width = tok_out.shape
    heads_n = beta.shape[0]
    mix_dim = head // heads_n
    slab = YN * CN
    passes = rows_n // BLOCK
    chunks = rows_n // ROW
    half = chunks // 2
    per_dev = tok_n // BLOCK
    score_scale = SCORE_GAIN * head ** (-0.5)

    st = lax.axis_index("st")
    x = lax.axis_index("tp")
    c = lax.rem(st, CN)
    y = lax.rem(st // CN, YN)
    z = st // slab
    other = 1 - c

    def at(zi, yi, ci):
        return (zi * YN + yi) * CN + ci

    def step(value, by, n):
        return lax.rem(value + (by % n), n)

    xs = [step(x, i, XN) for i in range(XN)]
    ys = [step(y, i, YN) for i in range(YN)]
    zs = [step(z, i, ZN) for i in range(ZN)]
    partner = at(z, y, other)
    x_to = (xs[1], xs[XN - 1])
    y_to = (at(z, ys[1], c), at(z, ys[YN - 1], c))
    z_to = (at(zs[1], y, c), at(zs[ZN - 1], y, c))

    started = []

    def remote(src, dst, sem, index, st_id=None, tp_id=None):
        sems = r[sem]
        device = {}
        if st_id is not None:
            device["st"] = st_id
        if tp_id is not None:
            device["tp"] = tp_id
        return pltpu.make_async_remote_copy(
            src_ref=src,
            dst_ref=dst,
            send_sem=sems.at[(0, *index)],
            recv_sem=sems.at[(1, *index)],
            device_id=device,
            device_id_type=MESH,
        )

    def go(copy):
        copy.start()
        started.append(copy)

    loads = {}

    def load(key, src, dst):
        loads[key] = pltpu.make_async_copy(src, dst, r["load"].at[len(loads)])
        loads[key].start()

    load("cot", r["cot_h"], qc.at[z, 1])
    load("tok", r["tok_h"], tok4.at[x])
    load("kw", r["kw_h"], kw)
    load("vw", r["vw_h"], vw)
    proj_rows = rows_n // 4
    proj_order = (0, 2, 1, 3)
    for k in proj_order:
        here = pl.ds(k * proj_rows, proj_rows)
        load(("rows", k), r["rows_h"].at[here, :], rows_v.at[here, :])
    load("mq", r["mq_h"], r["mq"])
    load("mk", r["mk_h"], r["mk"])
    load("mv", r["mv_h"], r["mv"])
    load("qw", r["qw_h"], qw)

    barrier = pltpu.get_barrier_semaphore()
    greeted = 0
    for target in xs[1:]:
        pl.semaphore_signal(barrier, inc=1, device_id={"tp": target}, device_id_type=MESH)
        greeted += 1
    friends = [partner] + [at(z, ys[d], c) for d in range(1, YN)]
    friends += [at(zs[d], y, ci) for d in range(1, ZN) for ci in (c, other)]
    for target in friends:
        pl.semaphore_signal(barrier, inc=1, device_id={"st": target}, device_id_type=MESH)
        greeted += 1
    pl.semaphore_wait(barrier, greeted)

    t_half = tok_n // 2
    half_rows = (pl.ds(0, t_half), pl.ds(t_half, t_half))

    def cot_copy(hop, d):
        source = zs[(1 - hop) % ZN] if d == 0 else zs[(hop - 1) % ZN]
        ref = qc.at[source, 1]
        if hop == ZN // 2:
            ref = qc.at[source, 1, half_rows[d]]
        return remote(ref, ref, "cotz", (hop - 1, d), st_id=z_to[d])

    def q_copies(hop, d, h):
        source = zs[(1 - hop) % ZN] if d == 0 else zs[(hop - 1) % ZN]
        if hop == ZN // 2 and h != d:
            return []
        ref = qc.at[source, 0, half_rows[h]]
        copies = [remote(ref, ref, "qz", (hop - 1, d, h), st_id=z_to[d])]
        if h == d and (hop < ZN // 2 or d == 0):
            copies.append(
                remote(gates.at[source], gates.at[source], "gz", (hop - 1, d), st_id=z_to[d])
            )
        return copies

    def tok_copy(hop, d):
        if hop == 1:
            ref = tok4.at[x]
        else:
            ref = tok4.at[xs[XN - 1] if d == 0 else xs[1], half_rows[d]]
        return remote(ref, ref, "tokx", (hop - 1, d), tp_id=x_to[d])

    def ids_copy(dc, dz):
        return remote(
            ids, r["ids_all"].at[c, z], "idsem", (dc, dz), st_id=at(zs[dz], y, other if dc else c)
        )

    id_peers = [(dc, dz) for dz in range(ZN) for dc in range(CN) if (dc, dz) != (0, 0)]
    for dc, dz in id_peers:
        go(ids_copy(dc, dz))
    r["ids_all"][c, z] = ids[...]
    loads["tok"].wait()
    for d in range(2):
        go(tok_copy(1, d))
    loads["cot"].wait()
    for d in range(2):
        go(cot_copy(1, d))

    per_chunk = proj_rows // BLOCK

    def kv_piece(yi, ci, k):
        return kv.at[pl.ds((yi * CN + ci) * passes + k * per_chunk, per_chunk)]

    def kv_copy(hop, d, k):
        yi = y if hop == 1 else (ys[YN - 1] if d == 0 else ys[1])
        ref = kv_piece(yi, c, k)
        return remote(ref, ref, "kvy", (hop - 1, d, k), st_id=y_to[d])

    def kv_across(rel, k):
        ref = kv_piece(ys[rel], c, k)
        return remote(ref, ref, "kvd", (rel, k), st_id=partner)

    loads["kw"].wait()
    loads["vw"].wait()
    for k in proj_order:
        loads[("rows", k)].wait()
        here = pl.ds(k * proj_rows, proj_rows)
        block = rows_v[here, :]
        low = low_dot(block, kw[...]).astype(BF16)
        key_low[here, :] = low
        low = low.astype(F32)
        scale = lax.rsqrt(jnp.mean(low * low, axis=-1, keepdims=True) + NORM_FLOOR)
        first = (y * CN + c) * passes + k * per_chunk
        kv[pl.ds(first, per_chunk), :, :head] = (
            (low * scale).astype(BF16).reshape(per_chunk, BLOCK, head)
        )
        kv[pl.ds(first, per_chunk), :, head:] = (
            low_dot(block, vw[...]).astype(BF16).reshape(per_chunk, BLOCK, head)
        )
        for d in range(2):
            go(kv_copy(1, d, k))
        go(kv_across(0, k))

    gwb[...] = jnp.broadcast_to(gate_w[...].astype(F32), gwb.shape)
    turned[...] = jnp.transpose(
        jnp.concatenate(
            [beta[...], decay[...], jnp.zeros((8 - 2 * heads_n, tok_n), F32)], axis=0
        )
    )
    states[...] = jnp.zeros_like(states)
    for key in ("mq", "mk", "mv", "qw"):
        loads[key].wait()

    def mix(b):
        here = pl.ds(pl.multiple_of(b * SPAN, SPAN), SPAN)
        for m in range(heads_n):
            cols = pl.ds(m * mix_dim, mix_dim)
            raw = turned[here, heads_n + m : heads_n + m + 1]
            softplus = jnp.maximum(raw, 0.0) + jnp.log1p(jnp.exp(-jnp.abs(raw)))
            mixed[here, cols], states[m] = mixer_span(
                r["mq"][here, cols].astype(F32),
                r["mk"][here, cols].astype(F32),
                r["mv"][here, cols].astype(F32),
                jax.nn.sigmoid(turned[here, m : m + 1]),
                -rate[m] * softplus,
                states[m],
            )

    spans_n = tok_n // SPAN

    def cot_pass(hop):
        for d in range(2):
            cot_copy(hop - 1, d).wait_recv()
            go(cot_copy(hop, d))

    def q_pass(hop, first):
        for d in range(2):
            h = d if first else 1 - d
            for copy in q_copies(hop - 1, d, h):
                copy.wait_recv()
            for copy in q_copies(hop, d, h):
                go(copy)

    def kv_pass(k):
        for d, rel in ((0, YN - 1), (1, 1)):
            kv_copy(1, d, k).wait_recv()
            if (k < 2) == (d == 0):
                go(kv_copy(2, d, k))
            go(kv_across(rel, k))

    w_half = width // CN

    def w_copy(w, d):
        rows = pl.ds(pl.multiple_of(xs[d] * width + c * w_half, w_half), w_half)
        return remote(
            (kw, vw, qw)[w].at[rows, :], w_all.at[x, c, w], "wxs", (w, d), tp_id=xs[d]
        )

    def w_across(d):
        ref = w_all.at[xs[XN - d], c]
        return remote(ref, ref, "wxd", (d,), st_id=partner)

    def gw_copy(d):
        cols = pl.ds(pl.multiple_of(xs[d] * width, width), width)
        return remote(gwb.at[:, cols], gw_all.at[x], "gws", (d,), tp_id=xs[d])

    pl.loop(0, 1)(mix)
    cot_pass(2)
    pl.loop(1, 2)(mix)
    for d in range(2):
        tok_copy(1, d).wait_recv()
        go(tok_copy(2, d))
    for d in range(1, XN):
        for w in range(3):
            go(w_copy(w, d))
        go(gw_copy(d))
    for w, ref in enumerate((kw, vw, qw)):
        for h in range(CN):
            w_all[x, h, w] = ref[pl.ds(pl.multiple_of(x * width + h * w_half, w_half), w_half), :]
    gw_all[x] = gwb[:, pl.ds(pl.multiple_of(x * width, width), width)]
    pl.loop(2, 3)(mix)
    cot_pass(3)
    kv_pass(0)
    for d in range(2):
        tok_copy(2, d).wait_recv()

    gate_rows = jnp.broadcast_to(gate_w[...], (16, model))
    logit = low_dot(gate_rows[:, :width], tok4[0], CONTRACT_LAST)
    for i in range(1, XN):
        logit += low_dot(gate_rows[:, i * width : (i + 1) * width], tok4[i], CONTRACT_LAST)
    gates[z] = jax.nn.sigmoid(logit[:8])

    @pl.loop(0, tok_n // ROW)
    def _(k):
        here = pl.ds(pl.multiple_of(k * ROW, ROW), ROW)
        low = low_dot(tok4[0, here, :], qw[pl.ds(0, width), :])
        for i in range(1, XN):
            low += low_dot(tok4[i, here, :], qw[pl.ds(i * width, width), :])
        low = low.astype(BF16)
        query_low[here, :] = low
        low = low.astype(F32)
        scale = lax.rsqrt(jnp.mean(low * low, axis=-1, keepdims=True) + NORM_FLOOR)
        qc[z, 0, here, :] = (low * scale).astype(BF16)

    for h in range(2):
        for d in range(2):
            for copy in q_copies(1, d, d if h == 0 else 1 - d):
                go(copy)
    pl.loop(3, 4)(mix)
    kv_pass(2)
    cot_pass(4)
    q_pass(2, True)
    for dc, dz in id_peers:
        ids_copy(dc, dz).wait_recv()
    every = jnp.concatenate(
        [r["ids_all"][ci, zi, 0:1, :] for ci in range(CN) for zi in range(ZN)], axis=0
    )
    lane = lax.broadcasted_iota(jnp.int32, (CN * ZN, 128), 1)
    loc_tab = jnp.zeros((CN * ZN, 128), jnp.int32)
    blk_tab = jnp.zeros((CN * ZN, 128), jnp.int32)
    owner = lax.shift_right_logical(every, 4)
    local = every & (passes - 1)
    for o in range(slab):
        match = (owner == z * slab + o) & (lane < per_dev * 4)
        loc = jnp.sum(jnp.where(match, local, 0), axis=1, keepdims=True)
        blk = jnp.sum(
            jnp.where(match, lax.shift_right_logical(lane, 2) + 1, 0), axis=1, keepdims=True
        )
        loc_tab = jnp.where(lane == o, jnp.minimum(loc, passes - 1), loc_tab)
        blk_tab = jnp.where(lane == o, blk - 1, blk_tab)
    tab_v[0] = loc_tab
    tab_v[1] = blk_tab
    tab_copy = pltpu.make_async_copy(tab_v, tab_s, r["load"].at[len(loads)])
    tab_copy.start()
    q_pass(2, False)
    kv_pass(1)
    q_pass(3, True)
    kv_pass(3)
    q_pass(3, False)
    for d in range(1, XN):
        for w in range(3):
            w_copy(w, d).wait_recv()
        go(w_across(d))
    q_pass(4, True)
    tab_copy.wait()
    lane_of = lax.broadcasted_iota(jnp.int32, (8, ZN * BLOCK), 1)
    for yi in range(YN):
        for which, ci in ((0, c), (1, other)):
            start = jnp.full((8, ZN * BLOCK), -1000000, jnp.int32)
            for zi in range(ZN):
                row = ci * ZN + zi
                base = jnp.where(
                    tab_s[1, row, yi * CN + c] >= 0,
                    tab_s[0, row, yi * CN + c] * BLOCK,
                    -1000000,
                )
                start = jnp.where(lax.shift_right_logical(lane_of, 6) == zi, base, start)
            code[yi, which] = start + (lane_of & (BLOCK - 1))
    for d in range(2):
        cot_copy(ZN // 2, d).wait_recv()
        for copy in q_copies(ZN // 2 - 1, d, 1 - d) + q_copies(ZN // 2, d, d):
            copy.wait_recv()
    for d, k in ((0, 0), (1, 2), (0, 1), (1, 3)):
        kv_copy(2, d, k).wait_recv()
        go(kv_across(2, k))
    for rel in range(YN):
        for k in range(4):
            kv_across(rel, k).wait_recv()

    tok_block = lax.shift_right_logical(lax.broadcasted_iota(jnp.int32, (BLOCK, tok_n), 1), 6)
    key_halves = [pl.ds(i * ROW * 2, ROW * 2) for i in range(slab * BLOCK // (2 * ROW))]

    def gather(reader):
        for o in range(slab):
            local_at = jnp.clip(tab_s[0, c * ZN + reader, o], 0, passes - 1)
            kvr[pl.ds(o * BLOCK, BLOCK), :] = kv[o * passes + local_at]

    def zt_copy(d, reader):
        return remote(
            zt.at[reader], zt_r.at[d, reader], "zts", (d, reader), st_id=at(zs[d], y, c)
        )

    @pl.loop(0, ZN)
    def _(reader):
        gather(reader)
        for part in key_halves:
            e_buf[reader, part, :] = low_dot(kvr[part, :head], qc[reader, 0], CONTRACT_LAST)
            g_buf[part, :] = low_dot(kvr[part, head:], qc[reader, 1], CONTRACT_LAST)
        total = jnp.zeros((1, tok_n), F32)
        product = jnp.zeros((1, tok_n), F32)
        for o in range(slab):
            here = pl.ds(o * BLOCK, BLOCK)
            mine = tok_block == tab_s[1, c * ZN + reader, o]
            e = jnp.where(mine, jnp.exp(e_buf[reader, here, :] * score_scale), 0.0)
            e_buf[reader, here, :] = e
            total += jnp.sum(e, axis=0, keepdims=True)
            product += jnp.sum(e * g_buf[here, :], axis=0, keepdims=True)
        zt[reader, 0:1, :] = total
        zt[reader, 1:2, :] = product * gates[reader, 0:1, :]
        for d in (4, 3, 5, 2, 6, 1, 7):
            zt_copy(d, reader).start()

    def summed(reader):
        both = zt[reader]
        for d in range(1, ZN):
            both += zt_r[d, reader]
        return both[0:1, :], both[1:2, :]

    def term_copy(reader):
        return remote(
            terms.at[other, reader], term_r.at[reader], "ters", (reader,), st_id=partner
        )

    @pl.loop(0, ZN)
    def _(reader):
        for d in range(1, ZN):
            zt_copy(d, reader).wait_recv()
        total, product = summed(reader)
        inverse = 1.0 / total
        mean = product * inverse
        gate = gates[reader, 0:1, :]
        gather(reader)
        for part in key_halves:
            g_buf[part, :] = low_dot(kvr[part, head:], qc[reader, 1], CONTRACT_LAST)
        for o in range(slab):
            here = pl.ds(o * BLOCK, BLOCK)
            probs = e_buf[reader, here, :] * inverse
            sg[here, :] = (probs * (g_buf[here, :] * gate - mean)).astype(BF16)
            pg[here, :] = (probs * gate).astype(BF16)
        for n, part in enumerate(key_halves):
            key_term = (low_dot(sg[part, :], qc[reader, 0]) * score_scale).astype(BF16)
            value_term = low_dot(pg[part, :], qc[reader, 1]).astype(BF16)
            for k in range(2 * ROW // BLOCK):
                o = n * (2 * ROW // BLOCK) + k
                piece = slice(k * BLOCK, (k + 1) * BLOCK)
                terms[o % CN, reader, o // CN, :, :head] = key_term[piece]
                terms[o % CN, reader, o // CN, :, head:] = value_term[piece]
        term_copy(reader).start()
        qg[reader] = (low_dot(sg[...], kvr[:, :head], CONTRACT_FIRST) * score_scale).astype(BF16)

    def z_copy(hop, d):
        if hop == 1:
            src = qg.at[zs[ZN // 2], half_rows[d]]
            dst = z_r.at[d, 0, half_rows[d]]
        else:
            src = z_s.at[d, hop - 1]
            dst = z_r.at[d, hop - 1]
        return remote(src, dst, "zrs", (d, hop - 1), st_id=z_to[d])

    def z_pass(hop):
        for d in range(2):
            z_copy(hop - 1, d).wait_recv()
            away = ZN // 2 + 1 - hop
            target = zs[away] if d == 0 else zs[(-away) % ZN]
            if hop == 2:
                mid, rest = half_rows[d], half_rows[1 - d]
                z_s[d, hop - 1, mid, :] = (
                    qg[target, mid, :].astype(F32) + z_r[d, 0, mid, :].astype(F32)
                ).astype(BF16)
                z_s[d, hop - 1, rest, :] = qg[target, rest, :]
            else:
                z_s[d, hop - 1] = (
                    qg[target].astype(F32) + z_r[d, hop - 2].astype(F32)
                ).astype(BF16)
            go(z_copy(hop, d))

    for d in range(2):
        go(z_copy(1, d))

    row_iota = lax.broadcasted_iota(jnp.int32, (ROW, ZN * BLOCK), 0)

    def pick(rel, q):
        yi = ys[rel]
        rows = row_iota + q * ROW
        ones = [
            jnp.where(rows == code[yi, which, 0:1, :], 1.0, 0.0).astype(BF16) for which in range(2)
        ]
        return low_dot(ones[0], terms[c, :, yi].reshape(ZN * BLOCK, 2 * head)) + low_dot(
            ones[1], term_r[:, yi].reshape(ZN * BLOCK, 2 * head)
        )

    yf_s, yf_r, yd_s, yd_r = get("yf_s", "yf_r", "yd_s", "yd_r")

    def two_step(far_s, far_r, near_s, near_r, far_sem, near_sem, term):
        def far(d, j):
            return remote(far_s.at[d, j], far_r.at[d, j], far_sem, (d, j), st_id=y_to[d])

        def near(d, q):
            return remote(near_s.at[d, q], near_r.at[d, q], near_sem, (d, q), st_id=y_to[d])

        def send(j):
            for d in range(2):
                q = j + half * d
                far_s[d, j] = term(2, q).astype(BF16)
                go(far(d, j))
            for d in range(2):
                q = j + half * (1 - d)
                near_s[d, q] = term(1 if d == 0 else 3, q).astype(BF16)
                go(near(d, q))

        def forward(j):
            for d in range(2):
                q = j + half * d
                value = term(1 if d == 0 else 3, q)
                far(d, j).wait_recv()
                near_s[d, q] = (value + far_r[d, j].astype(F32)).astype(BF16)
                go(near(d, q))

        def final(q):
            value = term(0, q)
            for d in range(2):
                near(d, q).wait_recv()
            return value + near_r[0, q].astype(F32) + near_r[1, q].astype(F32)

        return send, forward, final

    y_send, y_forward, y_final = two_step(yf_s, yf_r, yd_s, yd_r, "yfs", "yds", pick)

    def x_copy(hop, d, q):
        source = x if hop == 1 else (xs[XN - 1] if d == 0 else xs[1])
        ref = kgv.at[source, pl.ds(q * ROW, ROW)]
        return remote(ref, ref, "xrs", (hop - 1, d, q), tp_id=x_to[d])

    def x_send(j):
        for q in (j, j + half):
            for d in range(2):
                go(x_copy(1, d, q))

    def x_forward(j):
        for d in range(2):
            q = j + half * d
            x_copy(1, d, q).wait_recv()
            go(x_copy(2, d, q))

    def weight_of(head_at, w):
        return w_all[head_at, :, w].reshape(width, head)

    def finish_rows(j):
        for q in (j, j + half):
            here = pl.ds(q * ROW, ROW)
            value = y_final(q)
            hat = value[:, :head]
            low = key_low[here, :].astype(F32)
            scale = lax.rsqrt(jnp.mean(low * low, axis=-1, keepdims=True) + NORM_FLOOR)
            grad = (
                scale * hat
                - scale * scale * scale * low * jnp.mean(low * hat, axis=-1, keepdims=True)
            ).astype(BF16)
            key_grad[here, :] = grad
            kgv[x, here, :head] = grad
            kgv[x, here, head:] = value[:, head:].astype(BF16)

    def finish_out(j):
        for d in range(2):
            q = j + half * d
            here = pl.ds(q * ROW, ROW)
            x_copy(1, 1 - d, q).wait_recv()
            x_copy(2, d, q).wait_recv()
            value = jnp.zeros((ROW, width), F32)
            for i in range(XN):
                value += low_dot(kgv[i, here, :head], weight_of(i, 0), CONTRACT_LAST)
                value += low_dot(kgv[i, here, head:], weight_of(i, 1), CONTRACT_LAST)
            out_ref[here, :] = value.astype(out_ref.dtype)

    @pl.loop(0, ZN)
    def _(reader):
        term_copy(reader).wait_recv()

    y_send(0)
    pl.loop(4, 5)(mix)
    y_forward(0)
    y_send(1)
    z_pass(2)
    pl.loop(5, spans_n)(mix)
    finish_rows(0)
    x_send(0)
    z_pass(3)
    y_forward(1)
    y_send(2)
    x_forward(0)
    z_pass(4)
    finish_rows(1)
    x_send(1)
    y_forward(2)
    y_send(3)

    for d in range(2):
        z_copy(ZN // 2, d).wait_recv()
    total, product = summed(z)
    along = exact_dot(
        jnp.ones((8, head), F32), qc[z, 1].astype(F32) * mixed[...], CONTRACT_LAST
    )
    opened = gates[z]
    gga[x] = (1.0 - opened) * (product / total - opened * along)

    for k in range(tok_n // ROW):
        here = pl.ds(k * ROW, ROW)
        hat_grad = qg[z, here, :].astype(F32)
        for d in range(2):
            hat_grad += z_r[d, ZN // 2 - 1, here, :].astype(F32)
        low = query_low[here, :].astype(F32)
        scale = lax.rsqrt(jnp.mean(low * low, axis=-1, keepdims=True) + NORM_FLOOR)
        qga[x, here, :] = (
            scale * hat_grad
            - scale * scale * scale * low * jnp.mean(low * hat_grad, axis=-1, keepdims=True)
        ).astype(BF16)

    def t_copies(hop, d):
        source = x if hop == 1 else (xs[XN - 1] if d == 0 else xs[1])
        ref = qga.at[source] if hop == 1 else qga.at[source, half_rows[d]]
        copies = [remote(ref, ref, "tgs", (hop - 1, d), tp_id=x_to[d])]
        if hop == 1 or d == 0:
            copies.append(
                remote(gga.at[source], gga.at[source], "ggs", (hop - 1, d), tp_id=x_to[d])
            )
        return copies

    for d in range(2):
        for copy in t_copies(1, d):
            go(copy)
    x_forward(1)
    finish_rows(2)
    x_send(2)
    y_forward(3)
    for d in range(2):
        for copy in t_copies(1, d):
            copy.wait_recv()
        for copy in t_copies(2, d):
            go(copy)
    for d in range(1, XN):
        w_across(d).wait_recv()
        gw_copy(d).wait_recv()
    finish_out(0)
    x_forward(2)
    finish_rows(3)
    x_send(3)

    wbuf, wc_r, w1, wy_r, w2, wz_r = get("wbuf", "wc_r", "w1", "wy_r", "w2", "wz_r")
    part = weight_ref.shape[0]

    @pl.loop(0, ZN)
    def _(k):
        cols = pl.ds(pl.multiple_of(k * slab * part, slab * part), slab * part)
        tile = low_dot(rows_v[:, cols], key_grad[...], CONTRACT_FIRST).astype(BF16)
        for o in range(slab):
            wbuf[o % CN, o // CN, k] = tile[o * part : (o + 1) * part]

    wc_copy = remote(wbuf.at[other], wc_r, "wcs", (), st_id=partner)
    go(wc_copy)
    finish_out(1)
    wc_copy.wait_recv()
    for yi in range(YN):
        w1[yi] = (wbuf[c, yi].astype(F32) + wc_r[yi].astype(F32)).astype(BF16)

    def wy_copy(d):
        return remote(w1.at[ys[d]], wy_r.at[d], "wys", (d,), st_id=at(z, ys[d], c))

    def wz_copy(d):
        return remote(w2.at[zs[d]], wz_r.at[d], "wzs", (d,), st_id=at(zs[d], y, c))

    for d in (2, 1, 3):
        go(wy_copy(d))
    x_forward(3)
    for d in range(1, YN):
        wy_copy(d).wait_recv()
    gathered = w1[y].astype(F32)
    for d in range(1, YN):
        gathered += wy_r[d].astype(F32)
    w2[...] = gathered.astype(BF16)
    for d in (4, 3, 5, 2, 6, 1, 7):
        go(wz_copy(d))
    finish_out(2)
    for d in range(2):
        for copy in t_copies(2, d):
            copy.wait_recv()
    gate_rows = jnp.concatenate([gga[i, 0:1, :] for i in range(XN)] + [jnp.zeros((4, tok_n), F32)])
    gate_cols = jnp.concatenate([gw_all[i, 0:1, :] for i in range(XN)] + [jnp.zeros((4, width), F32)])
    for k in range(tok_n // ROW):
        here = pl.ds(k * ROW, ROW)
        value = exact_dot(gate_rows[:, k * ROW : (k + 1) * ROW], gate_cols, CONTRACT_FIRST)
        for i in range(XN):
            value += low_dot(qga[i, here, :], weight_of(i, 2), CONTRACT_LAST)
        tok_out[here, :] = value.astype(tok_out.dtype)
    for d in range(1, ZN):
        wz_copy(d).wait_recv()
    weight = w2[z].astype(F32)
    for d in range(1, ZN):
        weight += wz_r[d].astype(F32)
    weight_ref[...] = weight
    finish_out(3)
    for copy in started:
        copy.wait_send()

    @pl.loop(0, ZN)
    def _(reader):
        term_copy(reader).wait_send()
        for d in range(1, ZN):
            zt_copy(d, reader).wait_send()


def fused_call(rate, ids, gate_w, beta, decay, tok, cot, mq, mk, mv, qw, kw, vw, rows):
    tok_n, width = tok.shape
    rows_n, model = rows.shape
    head = kw.shape[1]
    heads_n = beta.shape[0]
    vmem, sems = scratch_spec(tok_n, rows_n, width, head, heads_n, head // heads_n)
    part = model // (ZN * YN * CN)
    ins = ["rate", "ids", "gate_w", "beta", "decay"]
    ins += ["tok_h", "cot_h", "mq_h", "mk_h", "mv_h", "qw_h", "kw_h", "vw_h", "rows_h"]
    names = ins + ["tok_out", "out_ref", "weight_ref"] + list(vmem) + ["tab_s"] + list(sems)
    return pl.pallas_call(
        functools.partial(fused_kernel, names),
        out_shape=(
            jax.ShapeDtypeStruct((tok_n, width), BF16),
            jax.ShapeDtypeStruct((rows_n, width), BF16),
            jax.ShapeDtypeStruct((part, head), F32),
        ),
        in_specs=[SMEM_SPEC] + [VMEM_SPEC] * 4 + [ANY_SPEC] * 9,
        out_specs=(VMEM_SPEC,) * 3,
        scratch_shapes=[pltpu.VMEM(*v) for v in vmem.values()]
        + [pltpu.SMEM((2, CN * ZN, 128), jnp.int32)]
        + [DMA(s) for s in sems.values()],
        compiler_params=pltpu.CompilerParams(
            collective_id=0, has_side_effects=True, vmem_limit_bytes=67043328
        ),
        name="fused",
    )(rate, ids, gate_w, beta, decay, tok, cot, mq, mk, mv, qw, kw, vw, rows)


def body(
    tokens,
    cotangent,
    mix_query,
    mix_key,
    mix_value,
    beta_pre,
    decay_pre,
    decay_rate,
    passages,
    passage_ids,
    query_weight,
    key_weight,
    value_weight,
    gate_weight,
):
    pass_local, span_rows, model_width = passages.shape
    flat_rows = passages.reshape(pass_local * span_rows, model_width)
    req_count = passage_ids.size
    ids = jnp.pad(passage_ids.reshape(1, req_count), ((0, 7), (0, -req_count % 128)))
    token_grad, passage_grad, key_weight_grad = fused_call(
        decay_rate,
        ids,
        gate_weight,
        beta_pre,
        decay_pre,
        tokens,
        cotangent,
        mix_query,
        mix_key,
        mix_value,
        query_weight,
        key_weight,
        value_weight,
        flat_rows,
    )
    token_grad, passage_grad, key_weight_grad = settle_call(
        token_grad, passage_grad, key_weight_grad
    )
    return (token_grad, passage_grad.reshape(pass_local, span_rows, -1), key_weight_grad)


def solution(mesh):
    placed = (
        P("st", "tp"),
        P("st", "tp"),
        P("st", "tp"),
        P("st", "tp"),
        P("st", "tp"),
        P("tp", "st"),
        P("tp", "st"),
        P("tp"),
        P("st", None, None),
        P("st", None),
        P(None, "tp"),
        P(None, "tp"),
        P(None, "tp"),
        P("tp", None),
    )
    return jax.shard_map(
        body,
        mesh=mesh,
        in_specs=placed,
        out_specs=(P("st", "tp"), P("st", None, "tp"), P("st", "tp")),
        check_vma=False,
    )
```

```python
import functools

import jax
import jax.numpy as jnp
from jax import lax
from jax.experimental import pallas as pl
from jax.experimental.pallas import tpu as pltpu
from jax.sharding import PartitionSpec as P

SPAN = 64
BLOCK = 64
NORM_FLOOR = 1.0
SCORE_GAIN = 4.0
HIGHEST = lax.Precision.HIGHEST
CONTRACT_LAST = (((1,), (1,)), ((), ()))
CONTRACT_FIRST = (((0,), (0,)), ((), ()))
F32, BF16 = jnp.float32, jnp.bfloat16

MESH = pl.DeviceIdType.MESH
VMEM_SPEC = pl.BlockSpec(memory_space=pltpu.VMEM)
ANY_SPEC = pl.BlockSpec(memory_space=pl.ANY)
SMEM_SPEC = pl.BlockSpec(memory_space=pltpu.SMEM)
DMA = pltpu.SemaphoreType.DMA

ZN, YN, CN, XN = 8, 4, 2, 4
ROW = 128


def settle_kernel(*refs):
    count = len(refs) // 2
    for source, target in zip(refs[:count], refs[count:]):
        target[...] = source[...]


def settle_call(*arrays):
    return pl.pallas_call(
        settle_kernel,
        out_shape=tuple(jax.ShapeDtypeStruct(x.shape, x.dtype) for x in arrays),
        in_specs=[VMEM_SPEC] * len(arrays),
        out_specs=(VMEM_SPEC,) * len(arrays),
        name="settle",
    )(*arrays)


def exact_dot(left, right, dims=(((1,), (0,)), ((), ()))):
    return lax.dot_general(left, right, dims, precision=HIGHEST, preferred_element_type=F32)


def low_dot(left, right, dims=(((1,), (0,)), ((), ()))):
    return lax.dot_general(left, right, dims, preferred_element_type=F32)


def mixer_span(queries, keys_in, values_in, strength, log_decay, state):
    span = queries.shape[0]
    row_at = lax.broadcasted_iota(jnp.int32, (span, span), 0)
    col_at = lax.broadcasted_iota(jnp.int32, (span, span), 1)
    inclusive = row_at >= col_at
    unit_eye = jnp.where(row_at == col_at, 1.0, 0.0)
    decay_row = jnp.sum(unit_eye * log_decay, axis=0, keepdims=True)
    cum_row = jnp.sum(jnp.where(row_at <= col_at, log_decay, 0.0), axis=0, keepdims=True)
    cum_col = jnp.sum(jnp.where(inclusive, decay_row, 0.0), axis=1, keepdims=True)
    total = jnp.sum(log_decay, axis=0, keepdims=True)
    decay_map = jnp.exp(jnp.where(inclusive, cum_col - cum_row, -1e30))
    queries = (
        queries
        * lax.rsqrt(jnp.sum(queries * queries, axis=-1, keepdims=True) + NORM_FLOOR)
        * queries.shape[-1] ** (-0.5)
    )
    keys_in = keys_in * lax.rsqrt(jnp.sum(keys_in * keys_in, axis=-1, keepdims=True) + NORM_FLOOR)
    power = jnp.where(
        row_at > col_at, strength * exact_dot(keys_in, keys_in, CONTRACT_LAST) * decay_map, 0.0
    )
    inverse = unit_eye - power
    for _ in range(span.bit_length() - 2):
        power = exact_dot(power, power)
        inverse = exact_dot(inverse, unit_eye + power)
    attend = exact_dot(queries, keys_in, CONTRACT_LAST) * decay_map
    fresh = exact_dot(inverse, values_in * strength)
    correction = exact_dot(inverse, keys_in * (strength * jnp.exp(cum_col)))
    new_values = fresh - exact_dot(correction, state)
    output = exact_dot(queries * jnp.exp(cum_col), state) + exact_dot(attend, new_values)
    state = state * jnp.exp(total) + exact_dot(
        keys_in * jnp.exp(total - cum_col), new_values, CONTRACT_FIRST
    )
    return output, state


def scratch_spec(tok_n, rows_n, width, head, heads_n, mix_dim):
    model = width * XN
    slab = YN * CN
    passes = rows_n // BLOCK
    chunks = rows_n // ROW
    half = chunks // 2
    part = model // (ZN * slab)
    keys = slab * BLOCK
    vmem = dict(
        rows_v=((rows_n, model), BF16),
        kw=((model, head), BF16),
        vw=((model, head), BF16),
        qw=((model, head), BF16),
        tok4=((XN, tok_n, width), BF16),
        kv=((slab * passes, BLOCK, 2 * head), BF16),
        qc=((ZN, 2, tok_n, head), BF16),
        gates=((ZN, 8, tok_n), F32),
        mq=((tok_n, head), BF16),
        mk=((tok_n, head), BF16),
        mv=((tok_n, head), BF16),
        ids_all=((CN, ZN, 8, 128), jnp.int32),
        tab_v=((2, CN * ZN, 128), jnp.int32),
        code=((YN, CN, 8, ZN * BLOCK), jnp.int32),
        turned=((tok_n, 8), F32),
        mixed=((tok_n, head), F32),
        states=((heads_n, mix_dim, mix_dim), F32),
        key_low=((rows_n, head), BF16),
        query_low=((tok_n, head), BF16),
        kvr=((keys, 2 * head), BF16),
        e_buf=((ZN, keys, tok_n), F32),
        g_buf=((keys, tok_n), F32),
        sg=((keys, tok_n), BF16),
        pg=((keys, tok_n), BF16),
        zt=((ZN, 2, tok_n), F32),
        zt_r=((ZN, ZN, 2, tok_n), F32),
        terms=((CN, ZN, YN, BLOCK, 2 * head), BF16),
        term_r=((ZN, YN, BLOCK, 2 * head), BF16),
        qg=((ZN, tok_n, head), BF16),
        z_s=((2, ZN // 2, tok_n, head), BF16),
        z_r=((2, ZN // 2, tok_n, head), BF16),
        yf_s=((2, half, ROW, 2 * head), BF16),
        yf_r=((2, half, ROW, 2 * head), BF16),
        yd_s=((2, chunks, ROW, 2 * head), BF16),
        yd_r=((2, chunks, ROW, 2 * head), BF16),
        key_grad=((rows_n, head), BF16),
        kgv=((XN, rows_n, 2 * head), BF16),
        qga=((XN, tok_n, head), BF16),
        gga=((XN, 8, tok_n), F32),
        w_all=((XN, CN, 3, width // CN, head), BF16),
        gwb=((8, model), F32),
        gw_all=((XN, 8, width), F32),
        wbuf=((CN, YN, ZN, part, head), BF16),
        wc_r=((YN, ZN, part, head), BF16),
        w1=((YN, ZN, part, head), BF16),
        wy_r=((YN, ZN, part, head), BF16),
        w2=((ZN, part, head), BF16),
        wz_r=((ZN, part, head), BF16),
    )
    sems = dict(
        load=(16,),
        idsem=(2, CN, ZN),
        tokx=(2, 2, 2, 2),
        cotz=(2, ZN // 2, 2),
        qz=(2, ZN // 2, 2, 2),
        gz=(2, ZN // 2, 2),
        kvy=(2, 2, 2, 4),
        kvd=(2, YN, 4),
        zts=(2, ZN, ZN),
        ters=(2, ZN),
        zrs=(2, 2, ZN // 2),
        yfs=(2, 2, half),
        yds=(2, 2, chunks),
        xrs=(2, 2, 2, chunks),
        tgs=(2, 2, 2),
        ggs=(2, 2, 2),
        wxs=(2, 3, XN),
        wxd=(2, XN),
        gws=(2, XN),
        wcs=(2,),
        wys=(2, YN),
        wzs=(2, ZN),
    )
    return vmem, sems


def fused_kernel(names, *refs):
    r = dict(zip(names, refs))

    def get(*keys):
        return [r[k] for k in keys]

    rate, ids, gate_w, beta, decay = get("rate", "ids", "gate_w", "beta", "decay")
    tok_out, out_ref, weight_ref = get("tok_out", "out_ref", "weight_ref")
    rows_v, kw, vw, qw, tok4, kv, qc, gates = get(
        "rows_v", "kw", "vw", "qw", "tok4", "kv", "qc", "gates"
    )
    tab_v, tab_s, code = get("tab_v", "tab_s", "code")
    kvr, e_buf, g_buf, sg, pg, zt, zt_r = get("kvr", "e_buf", "g_buf", "sg", "pg", "zt", "zt_r")
    terms, term_r, qg, z_s, z_r = get("terms", "term_r", "qg", "z_s", "z_r")
    key_low, key_grad, query_low = get("key_low", "key_grad", "query_low")
    kgv, qga, gga, w_all, gwb, gw_all = get("kgv", "qga", "gga", "w_all", "gwb", "gw_all")
    turned, mixed, states = get("turned", "mixed", "states")

    rows_n, model = rows_v.shape
    head = kw.shape[1]
    tok_n, width = tok_out.shape
    heads_n = beta.shape[0]
    mix_dim = head // heads_n
    slab = YN * CN
    passes = rows_n // BLOCK
    chunks = rows_n // ROW
    half = chunks // 2
    per_dev = tok_n // BLOCK
    score_scale = SCORE_GAIN * head ** (-0.5)

    st = lax.axis_index("st")
    x = lax.axis_index("tp")
    c = lax.rem(st, CN)
    y = lax.rem(st // CN, YN)
    z = st // slab
    other = 1 - c

    def at(zi, yi, ci):
        return (zi * YN + yi) * CN + ci

    def step(value, by, n):
        return lax.rem(value + (by % n), n)

    xs = [step(x, i, XN) for i in range(XN)]
    ys = [step(y, i, YN) for i in range(YN)]
    zs = [step(z, i, ZN) for i in range(ZN)]
    partner = at(z, y, other)
    x_to = (xs[1], xs[XN - 1])
    y_to = (at(z, ys[1], c), at(z, ys[YN - 1], c))
    z_to = (at(zs[1], y, c), at(zs[ZN - 1], y, c))

    started = []

    def remote(src, dst, sem, index, st_id=None, tp_id=None):
        sems = r[sem]
        device = {}
        if st_id is not None:
            device["st"] = st_id
        if tp_id is not None:
            device["tp"] = tp_id
        return pltpu.make_async_remote_copy(
            src_ref=src,
            dst_ref=dst,
            send_sem=sems.at[(0, *index)],
            recv_sem=sems.at[(1, *index)],
            device_id=device,
            device_id_type=MESH,
        )

    def go(copy):
        copy.start()
        started.append(copy)

    loads = {}

    def load(key, src, dst):
        loads[key] = pltpu.make_async_copy(src, dst, r["load"].at[len(loads)])
        loads[key].start()

    load("cot", r["cot_h"], qc.at[z, 1])
    load("tok", r["tok_h"], tok4.at[x])
    load("kw", r["kw_h"], kw)
    load("vw", r["vw_h"], vw)
    proj_rows = rows_n // 4
    proj_order = (0, 2, 1, 3)
    for k in proj_order:
        here = pl.ds(k * proj_rows, proj_rows)
        load(("rows", k), r["rows_h"].at[here, :], rows_v.at[here, :])
    load("mq", r["mq_h"], r["mq"])
    load("mk", r["mk_h"], r["mk"])
    load("mv", r["mv_h"], r["mv"])
    load("qw", r["qw_h"], qw)

    barrier = pltpu.get_barrier_semaphore()
    greeted = 0
    for target in xs[1:]:
        pl.semaphore_signal(barrier, inc=1, device_id={"tp": target}, device_id_type=MESH)
        greeted += 1
    friends = [partner] + [at(z, ys[d], c) for d in range(1, YN)]
    friends += [at(zs[d], y, ci) for d in range(1, ZN) for ci in (c, other)]
    for target in friends:
        pl.semaphore_signal(barrier, inc=1, device_id={"st": target}, device_id_type=MESH)
        greeted += 1
    pl.semaphore_wait(barrier, greeted)

    t_half = tok_n // 2
    half_rows = (pl.ds(0, t_half), pl.ds(t_half, t_half))

    def cot_copy(hop, d):
        source = zs[(1 - hop) % ZN] if d == 0 else zs[(hop - 1) % ZN]
        ref = qc.at[source, 1]
        if hop == ZN // 2:
            ref = qc.at[source, 1, half_rows[d]]
        return remote(ref, ref, "cotz", (hop - 1, d), st_id=z_to[d])

    def q_copies(hop, d, h):
        source = zs[(1 - hop) % ZN] if d == 0 else zs[(hop - 1) % ZN]
        if hop == ZN // 2 and h != d:
            return []
        ref = qc.at[source, 0, half_rows[h]]
        copies = [remote(ref, ref, "qz", (hop - 1, d, h), st_id=z_to[d])]
        if h == d and (hop < ZN // 2 or d == 0):
            copies.append(
                remote(gates.at[source], gates.at[source], "gz", (hop - 1, d), st_id=z_to[d])
            )
        return copies

    def tok_copy(hop, d, h):
        source = x if hop == 1 else (xs[XN - 1] if d == 0 else xs[1])
        ref = tok4.at[source, half_rows[h]]
        return remote(ref, ref, "tokx", (hop - 1, d, h), tp_id=x_to[d])

    def ids_copy(dc, dz):
        return remote(
            ids, r["ids_all"].at[c, z], "idsem", (dc, dz), st_id=at(zs[dz], y, other if dc else c)
        )

    id_peers = [(dc, dz) for dz in range(ZN) for dc in range(CN) if (dc, dz) != (0, 0)]
    for dc, dz in id_peers:
        go(ids_copy(dc, dz))
    r["ids_all"][c, z] = ids[...]
    loads["tok"].wait()
    for d in range(2):
        go(tok_copy(1, d, d))
    for d in range(2):
        go(tok_copy(1, d, 1 - d))
    loads["cot"].wait()
    for d in range(2):
        go(cot_copy(1, d))

    per_chunk = proj_rows // BLOCK

    def kv_piece(yi, ci, k):
        return kv.at[pl.ds((yi * CN + ci) * passes + k * per_chunk, per_chunk)]

    def kv_copy(hop, d, k):
        yi = y if hop == 1 else (ys[YN - 1] if d == 0 else ys[1])
        ref = kv_piece(yi, c, k)
        return remote(ref, ref, "kvy", (hop - 1, d, k), st_id=y_to[d])

    def kv_across(rel, k):
        ref = kv_piece(ys[rel], c, k)
        return remote(ref, ref, "kvd", (rel, k), st_id=partner)

    loads["kw"].wait()
    loads["vw"].wait()
    for k in proj_order:
        loads[("rows", k)].wait()
        here = pl.ds(k * proj_rows, proj_rows)
        block = rows_v[here, :]
        low = low_dot(block, kw[...]).astype(BF16)
        key_low[here, :] = low
        low = low.astype(F32)
        scale = lax.rsqrt(jnp.mean(low * low, axis=-1, keepdims=True) + NORM_FLOOR)
        first = (y * CN + c) * passes + k * per_chunk
        kv[pl.ds(first, per_chunk), :, :head] = (
            (low * scale).astype(BF16).reshape(per_chunk, BLOCK, head)
        )
        kv[pl.ds(first, per_chunk), :, head:] = (
            low_dot(block, vw[...]).astype(BF16).reshape(per_chunk, BLOCK, head)
        )
        for d in range(2):
            go(kv_copy(1, d, k))
        go(kv_across(0, k))

    gwb[...] = jnp.broadcast_to(gate_w[...].astype(F32), gwb.shape)
    turned[...] = jnp.transpose(
        jnp.concatenate(
            [beta[...], decay[...], jnp.zeros((8 - 2 * heads_n, tok_n), F32)], axis=0
        )
    )
    states[...] = jnp.zeros_like(states)
    for key in ("mq", "mk", "mv", "qw"):
        loads[key].wait()

    def mix(b):
        here = pl.ds(pl.multiple_of(b * SPAN, SPAN), SPAN)
        for m in range(heads_n):
            cols = pl.ds(m * mix_dim, mix_dim)
            raw = turned[here, heads_n + m : heads_n + m + 1]
            softplus = jnp.maximum(raw, 0.0) + jnp.log1p(jnp.exp(-jnp.abs(raw)))
            mixed[here, cols], states[m] = mixer_span(
                r["mq"][here, cols].astype(F32),
                r["mk"][here, cols].astype(F32),
                r["mv"][here, cols].astype(F32),
                jax.nn.sigmoid(turned[here, m : m + 1]),
                -rate[m] * softplus,
                states[m],
            )

    spans_n = tok_n // SPAN

    def cot_pass(hop):
        for d in range(2):
            cot_copy(hop - 1, d).wait_recv()
            go(cot_copy(hop, d))

    def q_pass(hop, first):
        for d in range(2):
            h = d if first else 1 - d
            for copy in q_copies(hop - 1, d, h):
                copy.wait_recv()
            for copy in q_copies(hop, d, h):
                go(copy)

    def kv_pass(k):
        for d, rel in ((0, YN - 1), (1, 1)):
            kv_copy(1, d, k).wait_recv()
            if (k < 2) == (d == 0):
                go(kv_copy(2, d, k))
            go(kv_across(rel, k))

    w_half = width // CN

    def w_copy(w, d):
        rows = pl.ds(pl.multiple_of(xs[d] * width + c * w_half, w_half), w_half)
        return remote(
            (kw, vw, qw)[w].at[rows, :], w_all.at[x, c, w], "wxs", (w, d), tp_id=xs[d]
        )

    def w_across(d):
        ref = w_all.at[xs[XN - d], c]
        return remote(ref, ref, "wxd", (d,), st_id=partner)

    def gw_copy(d):
        cols = pl.ds(pl.multiple_of(xs[d] * width, width), width)
        return remote(gwb.at[:, cols], gw_all.at[x], "gws", (d,), tp_id=xs[d])

    pl.loop(0, 1)(mix)
    cot_pass(2)
    for d in range(2):
        tok_copy(1, d, d).wait_recv()
        go(tok_copy(2, d, d))
    pl.loop(1, 3)(mix)
    cot_pass(3)
    kv_pass(0)
    for d in range(2):
        tok_copy(1, d, 1 - d).wait_recv()
        tok_copy(2, d, d).wait_recv()

    gate_rows = jnp.broadcast_to(gate_w[...], (16, model))
    logit = low_dot(gate_rows[:, :width], tok4[0], CONTRACT_LAST)
    for i in range(1, XN):
        logit += low_dot(gate_rows[:, i * width : (i + 1) * width], tok4[i], CONTRACT_LAST)
    gates[z] = jax.nn.sigmoid(logit[:8])

    @pl.loop(0, tok_n // ROW)
    def _(k):
        here = pl.ds(pl.multiple_of(k * ROW, ROW), ROW)
        low = low_dot(tok4[0, here, :], qw[pl.ds(0, width), :])
        for i in range(1, XN):
            low += low_dot(tok4[i, here, :], qw[pl.ds(i * width, width), :])
        low = low.astype(BF16)
        query_low[here, :] = low
        low = low.astype(F32)
        scale = lax.rsqrt(jnp.mean(low * low, axis=-1, keepdims=True) + NORM_FLOOR)
        qc[z, 0, here, :] = (low * scale).astype(BF16)

    for h in range(2):
        for d in range(2):
            for copy in q_copies(1, d, d if h == 0 else 1 - d):
                go(copy)
    for d in range(1, XN):
        for w in range(3):
            go(w_copy(w, d))
        go(gw_copy(d))
    for w, ref in enumerate((kw, vw, qw)):
        for h in range(CN):
            w_all[x, h, w] = ref[pl.ds(pl.multiple_of(x * width + h * w_half, w_half), w_half), :]
    gw_all[x] = gwb[:, pl.ds(pl.multiple_of(x * width, width), width)]
    pl.loop(3, 4)(mix)
    kv_pass(2)
    q_pass(2, True)
    kv_pass(1)
    cot_pass(4)
    for dc, dz in id_peers:
        ids_copy(dc, dz).wait_recv()
    every = jnp.concatenate(
        [r["ids_all"][ci, zi, 0:1, :] for ci in range(CN) for zi in range(ZN)], axis=0
    )
    lane = lax.broadcasted_iota(jnp.int32, (CN * ZN, 128), 1)
    loc_tab = jnp.zeros((CN * ZN, 128), jnp.int32)
    blk_tab = jnp.zeros((CN * ZN, 128), jnp.int32)
    owner = lax.shift_right_logical(every, 4)
    local = every & (passes - 1)
    for o in range(slab):
        match = (owner == z * slab + o) & (lane < per_dev * 4)
        loc = jnp.sum(jnp.where(match, local, 0), axis=1, keepdims=True)
        blk = jnp.sum(
            jnp.where(match, lax.shift_right_logical(lane, 2) + 1, 0), axis=1, keepdims=True
        )
        loc_tab = jnp.where(lane == o, jnp.minimum(loc, passes - 1), loc_tab)
        blk_tab = jnp.where(lane == o, blk - 1, blk_tab)
    tab_v[0] = loc_tab
    tab_v[1] = blk_tab
    tab_copy = pltpu.make_async_copy(tab_v, tab_s, r["load"].at[len(loads)])
    tab_copy.start()
    q_pass(2, False)
    kv_pass(3)
    q_pass(3, True)
    q_pass(3, False)
    q_pass(4, True)
    pl.loop(4, 5)(mix)
    tab_copy.wait()
    lane_of = lax.broadcasted_iota(jnp.int32, (8, ZN * BLOCK), 1)
    for yi in range(YN):
        for which, ci in ((0, c), (1, other)):
            start = jnp.full((8, ZN * BLOCK), -1000000, jnp.int32)
            for zi in range(ZN):
                row = ci * ZN + zi
                base = jnp.where(
                    tab_s[1, row, yi * CN + c] >= 0,
                    tab_s[0, row, yi * CN + c] * BLOCK,
                    -1000000,
                )
                start = jnp.where(lax.shift_right_logical(lane_of, 6) == zi, base, start)
            code[yi, which] = start + (lane_of & (BLOCK - 1))
    for d in range(2):
        cot_copy(ZN // 2, d).wait_recv()
        for copy in q_copies(ZN // 2 - 1, d, 1 - d) + q_copies(ZN // 2, d, d):
            copy.wait_recv()
    for d, k in ((0, 0), (1, 2), (0, 1), (1, 3)):
        kv_copy(2, d, k).wait_recv()
        go(kv_across(2, k))
    for rel in range(YN):
        for k in range(4):
            kv_across(rel, k).wait_recv()

    tok_block = lax.shift_right_logical(lax.broadcasted_iota(jnp.int32, (BLOCK, tok_n), 1), 6)
    key_halves = [pl.ds(i * ROW * 2, ROW * 2) for i in range(slab * BLOCK // (2 * ROW))]

    def gather(reader):
        for o in range(slab):
            local_at = jnp.clip(tab_s[0, c * ZN + reader, o], 0, passes - 1)
            kvr[pl.ds(o * BLOCK, BLOCK), :] = kv[o * passes + local_at]

    def zt_copy(d, reader):
        return remote(
            zt.at[reader], zt_r.at[d, reader], "zts", (d, reader), st_id=at(zs[d], y, c)
        )

    @pl.loop(0, ZN)
    def _(reader):
        gather(reader)
        for part in key_halves:
            e_buf[reader, part, :] = low_dot(kvr[part, :head], qc[reader, 0], CONTRACT_LAST)
            g_buf[part, :] = low_dot(kvr[part, head:], qc[reader, 1], CONTRACT_LAST)
        total = jnp.zeros((1, tok_n), F32)
        product = jnp.zeros((1, tok_n), F32)
        for o in range(slab):
            here = pl.ds(o * BLOCK, BLOCK)
            mine = tok_block == tab_s[1, c * ZN + reader, o]
            e = jnp.where(mine, jnp.exp(e_buf[reader, here, :] * score_scale), 0.0)
            e_buf[reader, here, :] = e
            total += jnp.sum(e, axis=0, keepdims=True)
            product += jnp.sum(e * g_buf[here, :], axis=0, keepdims=True)
        zt[reader, 0:1, :] = total
        zt[reader, 1:2, :] = product * gates[reader, 0:1, :]
        for d in (4, 3, 5, 2, 6, 1, 7):
            zt_copy(d, reader).start()

    def summed(reader):
        both = zt[reader]
        for d in range(1, ZN):
            both += zt_r[d, reader]
        return both[0:1, :], both[1:2, :]

    def term_copy(reader):
        return remote(
            terms.at[other, reader], term_r.at[reader], "ters", (reader,), st_id=partner
        )

    @pl.loop(0, ZN)
    def _(reader):
        for d in range(1, ZN):
            zt_copy(d, reader).wait_recv()
        total, product = summed(reader)
        inverse = 1.0 / total
        mean = product * inverse
        gate = gates[reader, 0:1, :]
        gather(reader)
        for part in key_halves:
            g_buf[part, :] = low_dot(kvr[part, head:], qc[reader, 1], CONTRACT_LAST)
        for o in range(slab):
            here = pl.ds(o * BLOCK, BLOCK)
            probs = e_buf[reader, here, :] * inverse
            sg[here, :] = (probs * (g_buf[here, :] * gate - mean)).astype(BF16)
            pg[here, :] = (probs * gate).astype(BF16)
        for n, part in enumerate(key_halves):
            key_term = (low_dot(sg[part, :], qc[reader, 0]) * score_scale).astype(BF16)
            value_term = low_dot(pg[part, :], qc[reader, 1]).astype(BF16)
            for k in range(2 * ROW // BLOCK):
                o = n * (2 * ROW // BLOCK) + k
                piece = slice(k * BLOCK, (k + 1) * BLOCK)
                terms[o % CN, reader, o // CN, :, :head] = key_term[piece]
                terms[o % CN, reader, o // CN, :, head:] = value_term[piece]
        term_copy(reader).start()
        qg[reader] = (low_dot(sg[...], kvr[:, :head], CONTRACT_FIRST) * score_scale).astype(BF16)

    def z_copy(hop, d):
        if hop == 1:
            src = qg.at[zs[ZN // 2], half_rows[d]]
            dst = z_r.at[d, 0, half_rows[d]]
        else:
            src = z_s.at[d, hop - 1]
            dst = z_r.at[d, hop - 1]
        return remote(src, dst, "zrs", (d, hop - 1), st_id=z_to[d])

    def z_pass(hop):
        for d in range(2):
            z_copy(hop - 1, d).wait_recv()
            away = ZN // 2 + 1 - hop
            target = zs[away] if d == 0 else zs[(-away) % ZN]
            if hop == 2:
                mid, rest = half_rows[d], half_rows[1 - d]
                z_s[d, hop - 1, mid, :] = (
                    qg[target, mid, :].astype(F32) + z_r[d, 0, mid, :].astype(F32)
                ).astype(BF16)
                z_s[d, hop - 1, rest, :] = qg[target, rest, :]
            else:
                z_s[d, hop - 1] = (
                    qg[target].astype(F32) + z_r[d, hop - 2].astype(F32)
                ).astype(BF16)
            go(z_copy(hop, d))

    for d in range(2):
        go(z_copy(1, d))

    row_iota = lax.broadcasted_iota(jnp.int32, (ROW, ZN * BLOCK), 0)

    def pick(rel, q):
        yi = ys[rel]
        rows = row_iota + q * ROW
        ones = [
            jnp.where(rows == code[yi, which, 0:1, :], 1.0, 0.0).astype(BF16) for which in range(2)
        ]
        return low_dot(ones[0], terms[c, :, yi].reshape(ZN * BLOCK, 2 * head)) + low_dot(
            ones[1], term_r[:, yi].reshape(ZN * BLOCK, 2 * head)
        )

    yf_s, yf_r, yd_s, yd_r = get("yf_s", "yf_r", "yd_s", "yd_r")

    def two_step(far_s, far_r, near_s, near_r, far_sem, near_sem, term):
        def far(d, j):
            return remote(far_s.at[d, j], far_r.at[d, j], far_sem, (d, j), st_id=y_to[d])

        def near(d, q):
            return remote(near_s.at[d, q], near_r.at[d, q], near_sem, (d, q), st_id=y_to[d])

        def send(j):
            for d in range(2):
                q = j + half * d
                far_s[d, j] = term(2, q).astype(BF16)
                go(far(d, j))
            for d in range(2):
                q = j + half * (1 - d)
                near_s[d, q] = term(1 if d == 0 else 3, q).astype(BF16)
                go(near(d, q))

        def forward(j):
            for d in range(2):
                q = j + half * d
                value = term(1 if d == 0 else 3, q)
                far(d, j).wait_recv()
                near_s[d, q] = (value + far_r[d, j].astype(F32)).astype(BF16)
                go(near(d, q))

        def final(q):
            value = term(0, q)
            for d in range(2):
                near(d, q).wait_recv()
            return value + near_r[0, q].astype(F32) + near_r[1, q].astype(F32)

        return send, forward, final

    y_send, y_forward, y_final = two_step(yf_s, yf_r, yd_s, yd_r, "yfs", "yds", pick)

    def x_copy(hop, d, q):
        source = x if hop == 1 else (xs[XN - 1] if d == 0 else xs[1])
        ref = kgv.at[source, pl.ds(q * ROW, ROW)]
        return remote(ref, ref, "xrs", (hop - 1, d, q), tp_id=x_to[d])

    def x_send(j):
        for q in (j, j + half):
            for d in range(2):
                go(x_copy(1, d, q))

    def x_forward(j):
        for d in range(2):
            q = j + half * d
            x_copy(1, d, q).wait_recv()
            go(x_copy(2, d, q))

    def weight_of(head_at, w):
        return w_all[head_at, :, w].reshape(width, head)

    def finish_rows(j):
        for q in (j, j + half):
            here = pl.ds(q * ROW, ROW)
            value = y_final(q)
            hat = value[:, :head]
            low = key_low[here, :].astype(F32)
            scale = lax.rsqrt(jnp.mean(low * low, axis=-1, keepdims=True) + NORM_FLOOR)
            grad = (
                scale * hat
                - scale * scale * scale * low * jnp.mean(low * hat, axis=-1, keepdims=True)
            ).astype(BF16)
            key_grad[here, :] = grad
            kgv[x, here, :head] = grad
            kgv[x, here, head:] = value[:, head:].astype(BF16)

    def finish_out(j):
        for d in range(2):
            q = j + half * d
            here = pl.ds(q * ROW, ROW)
            x_copy(1, 1 - d, q).wait_recv()
            x_copy(2, d, q).wait_recv()
            value = jnp.zeros((ROW, width), F32)
            for i in range(XN):
                value += low_dot(kgv[i, here, :head], weight_of(i, 0), CONTRACT_LAST)
                value += low_dot(kgv[i, here, head:], weight_of(i, 1), CONTRACT_LAST)
            out_ref[here, :] = value.astype(out_ref.dtype)

    @pl.loop(0, ZN)
    def _(reader):
        term_copy(reader).wait_recv()

    y_send(0)
    pl.loop(5, spans_n)(mix)
    y_forward(0)
    y_send(1)
    z_pass(2)
    finish_rows(0)
    x_send(0)
    y_forward(1)
    y_send(2)
    z_pass(3)
    for d in range(1, XN):
        for w in range(3):
            w_copy(w, d).wait_recv()
        go(w_across(d))
    finish_rows(1)
    x_forward(0)
    x_send(1)
    z_pass(4)
    y_forward(2)
    y_send(3)
    finish_rows(2)
    x_send(2)
    x_forward(1)
    y_forward(3)

    for d in range(2):
        z_copy(ZN // 2, d).wait_recv()
    total, product = summed(z)
    along = exact_dot(
        jnp.ones((8, head), F32), qc[z, 1].astype(F32) * mixed[...], CONTRACT_LAST
    )
    opened = gates[z]
    gga[x] = (1.0 - opened) * (product / total - opened * along)

    for k in range(tok_n // ROW):
        here = pl.ds(k * ROW, ROW)
        hat_grad = qg[z, here, :].astype(F32)
        for d in range(2):
            hat_grad += z_r[d, ZN // 2 - 1, here, :].astype(F32)
        low = query_low[here, :].astype(F32)
        scale = lax.rsqrt(jnp.mean(low * low, axis=-1, keepdims=True) + NORM_FLOOR)
        qga[x, here, :] = (
            scale * hat_grad
            - scale * scale * scale * low * jnp.mean(low * hat_grad, axis=-1, keepdims=True)
        ).astype(BF16)

    def t_copies(hop, d):
        source = x if hop == 1 else (xs[XN - 1] if d == 0 else xs[1])
        ref = qga.at[source] if hop == 1 else qga.at[source, half_rows[d]]
        copies = [remote(ref, ref, "tgs", (hop - 1, d), tp_id=x_to[d])]
        if hop == 1 or d == 0:
            copies.append(
                remote(gga.at[source], gga.at[source], "ggs", (hop - 1, d), tp_id=x_to[d])
            )
        return copies

    for d in range(2):
        for copy in t_copies(1, d):
            go(copy)
    finish_rows(3)
    x_send(3)
    x_forward(2)

    wbuf, wc_r, w1, wy_r, w2, wz_r = get("wbuf", "wc_r", "w1", "wy_r", "w2", "wz_r")
    part = weight_ref.shape[0]

    @pl.loop(0, ZN)
    def _(k):
        cols = pl.ds(pl.multiple_of(k * slab * part, slab * part), slab * part)
        tile = low_dot(rows_v[:, cols], key_grad[...], CONTRACT_FIRST).astype(BF16)
        for o in range(slab):
            wbuf[o % CN, o // CN, k] = tile[o * part : (o + 1) * part]

    wc_copy = remote(wbuf.at[other], wc_r, "wcs", (), st_id=partner)
    go(wc_copy)
    for d in range(2):
        for copy in t_copies(1, d):
            copy.wait_recv()
        for copy in t_copies(2, d):
            go(copy)
    for d in range(1, XN):
        w_across(d).wait_recv()
        gw_copy(d).wait_recv()
    finish_out(0)
    wc_copy.wait_recv()
    for yi in range(YN):
        w1[yi] = (wbuf[c, yi].astype(F32) + wc_r[yi].astype(F32)).astype(BF16)

    def wy_copy(d):
        return remote(w1.at[ys[d]], wy_r.at[d], "wys", (d,), st_id=at(z, ys[d], c))

    def wz_copy(d):
        return remote(w2.at[zs[d]], wz_r.at[d], "wzs", (d,), st_id=at(zs[d], y, c))

    for d in (2, 1, 3):
        go(wy_copy(d))
    finish_out(1)
    x_forward(3)
    for d in range(1, YN):
        wy_copy(d).wait_recv()
    gathered = w1[y].astype(F32)
    for d in range(1, YN):
        gathered += wy_r[d].astype(F32)
    w2[...] = gathered.astype(BF16)
    for d in (4, 3, 5, 2, 6, 1, 7):
        go(wz_copy(d))
    finish_out(2)
    for d in range(2):
        for copy in t_copies(2, d):
            copy.wait_recv()
    gate_rows = jnp.concatenate([gga[i, 0:1, :] for i in range(XN)] + [jnp.zeros((4, tok_n), F32)])
    gate_cols = jnp.concatenate([gw_all[i, 0:1, :] for i in range(XN)] + [jnp.zeros((4, width), F32)])
    for k in range(tok_n // ROW):
        here = pl.ds(k * ROW, ROW)
        value = exact_dot(gate_rows[:, k * ROW : (k + 1) * ROW], gate_cols, CONTRACT_FIRST)
        for i in range(XN):
            value += low_dot(qga[i, here, :], weight_of(i, 2), CONTRACT_LAST)
        tok_out[here, :] = value.astype(tok_out.dtype)
    for d in range(1, ZN):
        wz_copy(d).wait_recv()
    weight = w2[z].astype(F32)
    for d in range(1, ZN):
        weight += wz_r[d].astype(F32)
    weight_ref[...] = weight
    finish_out(3)
    for copy in started:
        copy.wait_send()

    @pl.loop(0, ZN)
    def _(reader):
        term_copy(reader).wait_send()
        for d in range(1, ZN):
            zt_copy(d, reader).wait_send()


def fused_call(rate, ids, gate_w, beta, decay, tok, cot, mq, mk, mv, qw, kw, vw, rows):
    tok_n, width = tok.shape
    rows_n, model = rows.shape
    head = kw.shape[1]
    heads_n = beta.shape[0]
    vmem, sems = scratch_spec(tok_n, rows_n, width, head, heads_n, head // heads_n)
    part = model // (ZN * YN * CN)
    ins = ["rate", "ids", "gate_w", "beta", "decay"]
    ins += ["tok_h", "cot_h", "mq_h", "mk_h", "mv_h", "qw_h", "kw_h", "vw_h", "rows_h"]
    names = ins + ["tok_out", "out_ref", "weight_ref"] + list(vmem) + ["tab_s"] + list(sems)
    return pl.pallas_call(
        functools.partial(fused_kernel, names),
        out_shape=(
            jax.ShapeDtypeStruct((tok_n, width), BF16),
            jax.ShapeDtypeStruct((rows_n, width), BF16),
            jax.ShapeDtypeStruct((part, head), F32),
        ),
        in_specs=[SMEM_SPEC] + [VMEM_SPEC] * 4 + [ANY_SPEC] * 9,
        out_specs=(VMEM_SPEC,) * 3,
        scratch_shapes=[pltpu.VMEM(*v) for v in vmem.values()]
        + [pltpu.SMEM((2, CN * ZN, 128), jnp.int32)]
        + [DMA(s) for s in sems.values()],
        compiler_params=pltpu.CompilerParams(
            collective_id=0, has_side_effects=True, vmem_limit_bytes=67043328
        ),
        name="fused",
    )(rate, ids, gate_w, beta, decay, tok, cot, mq, mk, mv, qw, kw, vw, rows)


def body(
    tokens,
    cotangent,
    mix_query,
    mix_key,
    mix_value,
    beta_pre,
    decay_pre,
    decay_rate,
    passages,
    passage_ids,
    query_weight,
    key_weight,
    value_weight,
    gate_weight,
):
    pass_local, span_rows, model_width = passages.shape
    flat_rows = passages.reshape(pass_local * span_rows, model_width)
    req_count = passage_ids.size
    ids = jnp.pad(passage_ids.reshape(1, req_count), ((0, 7), (0, -req_count % 128)))
    token_grad, passage_grad, key_weight_grad = fused_call(
        decay_rate,
        ids,
        gate_weight,
        beta_pre,
        decay_pre,
        tokens,
        cotangent,
        mix_query,
        mix_key,
        mix_value,
        query_weight,
        key_weight,
        value_weight,
        flat_rows,
    )
    token_grad, passage_grad, key_weight_grad = settle_call(
        token_grad, passage_grad, key_weight_grad
    )
    return (token_grad, passage_grad.reshape(pass_local, span_rows, -1), key_weight_grad)


def solution(mesh):
    placed = (
        P("st", "tp"),
        P("st", "tp"),
        P("st", "tp"),
        P("st", "tp"),
        P("st", "tp"),
        P("tp", "st"),
        P("tp", "st"),
        P("tp"),
        P("st", None, None),
        P("st", None),
        P(None, "tp"),
        P(None, "tp"),
        P(None, "tp"),
        P("tp", None),
    )
    return jax.shard_map(
        body,
        mesh=mesh,
        in_specs=placed,
        out_specs=(P("st", "tp"), P("st", None, "tp"), P("st", "tp")),
        check_vma=False,
    )
```

```python
import functools

import jax
import jax.numpy as jnp
from jax import lax
from jax.experimental import pallas as pl
from jax.experimental.pallas import tpu as pltpu
from jax.sharding import PartitionSpec as P

SPAN = 64
BLOCK = 64
NORM_FLOOR = 1.0
SCORE_GAIN = 4.0
HIGHEST = lax.Precision.HIGHEST
CONTRACT_LAST = (((1,), (1,)), ((), ()))
CONTRACT_FIRST = (((0,), (0,)), ((), ()))
F32, BF16 = jnp.float32, jnp.bfloat16

MESH = pl.DeviceIdType.MESH
VMEM_SPEC = pl.BlockSpec(memory_space=pltpu.VMEM)
ANY_SPEC = pl.BlockSpec(memory_space=pl.ANY)
SMEM_SPEC = pl.BlockSpec(memory_space=pltpu.SMEM)
DMA = pltpu.SemaphoreType.DMA

ZN, YN, CN, XN = 8, 4, 2, 4
ROW = 128
SENDS = ("id0", "id1", "tokx", "cotz", "qz", "gz", "kvy", "kvd", "zts", "ters", "zrs", "yfs")
SENDS += ("yds", "xrs", "tgs", "ggs", "wxs", "wxd", "gws", "wcs", "wys", "wzs")


def settle_kernel(*refs):
    count = len(refs) // 2
    for source, target in zip(refs[:count], refs[count:]):
        target[...] = source[...]


def settle_call(*arrays):
    return pl.pallas_call(
        settle_kernel,
        out_shape=tuple(jax.ShapeDtypeStruct(x.shape, x.dtype) for x in arrays),
        in_specs=[VMEM_SPEC] * len(arrays),
        out_specs=(VMEM_SPEC,) * len(arrays),
        name="settle",
    )(*arrays)


def exact_dot(left, right, dims=(((1,), (0,)), ((), ()))):
    return lax.dot_general(left, right, dims, precision=HIGHEST, preferred_element_type=F32)


def low_dot(left, right, dims=(((1,), (0,)), ((), ()))):
    return lax.dot_general(left, right, dims, preferred_element_type=F32)


def mixer_span(queries, keys_in, values_in, strength, log_decay, state):
    span = queries.shape[0]
    row_at = lax.broadcasted_iota(jnp.int32, (span, span), 0)
    col_at = lax.broadcasted_iota(jnp.int32, (span, span), 1)
    inclusive = row_at >= col_at
    unit_eye = jnp.where(row_at == col_at, 1.0, 0.0)
    decay_row = jnp.sum(unit_eye * log_decay, axis=0, keepdims=True)
    cum_row = jnp.sum(jnp.where(row_at <= col_at, log_decay, 0.0), axis=0, keepdims=True)
    cum_col = jnp.sum(jnp.where(inclusive, decay_row, 0.0), axis=1, keepdims=True)
    total = jnp.sum(log_decay, axis=0, keepdims=True)
    decay_map = jnp.exp(jnp.where(inclusive, cum_col - cum_row, -1e30))
    queries = (
        queries
        * lax.rsqrt(jnp.sum(queries * queries, axis=-1, keepdims=True) + NORM_FLOOR)
        * queries.shape[-1] ** (-0.5)
    )
    keys_in = keys_in * lax.rsqrt(jnp.sum(keys_in * keys_in, axis=-1, keepdims=True) + NORM_FLOOR)
    power = jnp.where(
        row_at > col_at, strength * exact_dot(keys_in, keys_in, CONTRACT_LAST) * decay_map, 0.0
    )
    inverse = unit_eye - power
    for _ in range(span.bit_length() - 2):
        power = exact_dot(power, power)
        inverse = exact_dot(inverse, unit_eye + power)
    attend = exact_dot(queries, keys_in, CONTRACT_LAST) * decay_map
    fresh = exact_dot(inverse, values_in * strength)
    correction = exact_dot(inverse, keys_in * (strength * jnp.exp(cum_col)))
    new_values = fresh - exact_dot(correction, state)
    output = exact_dot(queries * jnp.exp(cum_col), state) + exact_dot(attend, new_values)
    state = state * jnp.exp(total) + exact_dot(
        keys_in * jnp.exp(total - cum_col), new_values, CONTRACT_FIRST
    )
    return output, state


def scratch_spec(tok_n, rows_n, width, head, heads_n, mix_dim):
    model = width * XN
    slab = YN * CN
    passes = rows_n // BLOCK
    chunks = rows_n // ROW
    half = chunks // 2
    part = model // (ZN * slab)
    keys = slab * BLOCK
    vmem = dict(
        rows_v=((rows_n, model), BF16),
        kw=((model, head), BF16),
        vw=((model, head), BF16),
        qw=((model, head), BF16),
        tok4=((XN, tok_n, width), BF16),
        kv=((slab * passes, BLOCK, 2 * head), BF16),
        qc=((ZN, 2, tok_n, head), BF16),
        gates=((ZN, 8, tok_n), F32),
        mq=((tok_n, head), BF16),
        mk=((tok_n, head), BF16),
        mv=((tok_n, head), BF16),
        ids_all=((CN, ZN, 8, 128), jnp.int32),
        tab_v=((2, CN * ZN, 128), jnp.int32),
        code=((YN, CN, 8, ZN * BLOCK), jnp.int32),
        turned=((tok_n, 8), F32),
        mixed=((tok_n, head), F32),
        states=((heads_n, mix_dim, mix_dim), F32),
        key_low=((rows_n, head), BF16),
        query_low=((tok_n, head), BF16),
        kvr=((keys, 2 * head), BF16),
        e_buf=((ZN, keys, tok_n), F32),
        g_buf=((keys, tok_n), F32),
        sg=((keys, tok_n), BF16),
        pg=((keys, tok_n), BF16),
        zt=((ZN, 2, tok_n), F32),
        zt_r=((ZN, ZN, 2, tok_n), F32),
        terms=((CN, ZN, YN, BLOCK, 2 * head), BF16),
        term_r=((ZN, YN, BLOCK, 2 * head), BF16),
        qg=((ZN, tok_n, head), BF16),
        z_s=((2, ZN // 2, tok_n, head), BF16),
        z_r=((2, ZN // 2, tok_n, head), BF16),
        yf_s=((2, half, ROW, 2 * head), BF16),
        yf_r=((2, half, ROW, 2 * head), BF16),
        yd_s=((2, chunks, ROW, 2 * head), BF16),
        yd_r=((2, chunks, ROW, 2 * head), BF16),
        key_grad=((rows_n, head), BF16),
        kgv=((XN, rows_n, 2 * head), BF16),
        qga=((XN, tok_n, head), BF16),
        gga=((XN, 8, tok_n), F32),
        w_all=((XN, CN, 3, width // CN, head), BF16),
        gwb=((8, model), F32),
        gw_all=((XN, 8, width), F32),
        wbuf=((CN, YN, ZN, part, head), BF16),
        wc_r=((YN, ZN, part, head), BF16),
        w1=((YN, ZN, part, head), BF16),
        wy_r=((YN, ZN, part, head), BF16),
        w2=((ZN, part, head), BF16),
        wz_r=((ZN, part, head), BF16),
        tok_v=((tok_n, width), BF16),
        out_v=((rows_n, width), BF16),
        weight_v=((part, head), F32),
        w_acc=((model, head), F32),
    )
    sems = dict(
        load=(16,),
        outs=(3,),
        send=(len(SENDS),),
        idsem=(CN,),
        tokx=(2, 2, 2),
        cotz=(ZN // 2, 2),
        qz=(ZN // 2, 2, 2),
        gz=(ZN // 2, 2),
        kvy=(2, 2, 4),
        kvd=(1,),
        zts=(ZN,),
        ters=(1,),
        zrs=(2, ZN // 2),
        yfs=(2, half),
        yds=(chunks,),
        xrs=(2, chunks),
        tgs=(2, 2),
        ggs=(2, 2),
        wxs=(1,),
        wxd=(1,),
        gws=(1,),
        wcs=(1,),
        wys=(1,),
        wzs=(1,),
    )
    return vmem, sems


def fused_kernel(names, *refs):
    r = dict(zip(names, refs))

    def get(*keys):
        return [r[k] for k in keys]

    rate, ids, gate_w, beta, decay = get("rate", "ids", "gate_w", "beta", "decay")
    tok_out, out_ref, weight_ref = get("tok_v", "out_v", "weight_v")
    rows_v, kw, vw, qw, tok4, kv, qc, gates = get(
        "rows_v", "kw", "vw", "qw", "tok4", "kv", "qc", "gates"
    )
    tab_v, tab_s, code = get("tab_v", "tab_s", "code")
    kvr, e_buf, g_buf, sg, pg, zt, zt_r = get("kvr", "e_buf", "g_buf", "sg", "pg", "zt", "zt_r")
    terms, term_r, qg, z_s, z_r = get("terms", "term_r", "qg", "z_s", "z_r")
    key_low, key_grad, query_low = get("key_low", "key_grad", "query_low")
    kgv, qga, gga, w_all, gwb, gw_all = get("kgv", "qga", "gga", "w_all", "gwb", "gw_all")
    turned, mixed, states = get("turned", "mixed", "states")

    rows_n, model = rows_v.shape
    head = kw.shape[1]
    tok_n, width = tok_out.shape
    heads_n = beta.shape[0]
    mix_dim = head // heads_n
    slab = YN * CN
    passes = rows_n // BLOCK
    chunks = rows_n // ROW
    half = chunks // 2
    per_dev = tok_n // BLOCK
    score_scale = SCORE_GAIN * head ** (-0.5)

    st = lax.axis_index("st")
    x = lax.axis_index("tp")
    c = lax.rem(st, CN)
    y = lax.rem(st // CN, YN)
    z = st // slab
    other = 1 - c

    def at(zi, yi, ci):
        return (zi * YN + yi) * CN + ci

    def step(value, by, n):
        return lax.rem(value + (by % n), n)

    xs = [step(x, i, XN) for i in range(XN)]
    ys = [step(y, i, YN) for i in range(YN)]
    zs = [step(z, i, ZN) for i in range(ZN)]
    partner = at(z, y, other)
    x_to = (xs[1], xs[XN - 1])
    y_to = (at(z, ys[1], c), at(z, ys[YN - 1], c))
    z_to = (at(zs[1], y, c), at(zs[ZN - 1], y, c))

    def remote(src, dst, sem, index, st_id=None, tp_id=None, group=None):
        device = {}
        if st_id is not None:
            device["st"] = st_id
        if tp_id is not None:
            device["tp"] = tp_id
        return pltpu.make_async_remote_copy(
            src_ref=src,
            dst_ref=dst,
            send_sem=r["send"].at[SENDS.index(group or sem)],
            recv_sem=r[sem].at[index],
            device_id=device,
            device_id_type=MESH,
        )

    def go(copy):
        copy.start()

    def all_of(ref, sem, index, group=None):
        return remote(ref, ref, sem, index, st_id=partner, group=group)

    def leave(index, src, dst):
        pltpu.make_async_copy(src, dst, r["outs"].at[index]).start()

    loads = {}

    def load(key, src, dst):
        loads[key] = pltpu.make_async_copy(src, dst, r["load"].at[len(loads)])
        loads[key].start()

    load("cot", r["cot_h"], qc.at[z, 1])
    load("tok", r["tok_h"], tok4.at[x])
    load("kw", r["kw_h"], kw)
    load("vw", r["vw_h"], vw)
    proj_rows = rows_n // 4
    proj_order = (0, 2, 1, 3)
    for k in proj_order:
        here = pl.ds(k * proj_rows, proj_rows)
        load(("rows", k), r["rows_h"].at[here, :], rows_v.at[here, :])
    load("mq", r["mq_h"], r["mq"])
    load("mk", r["mk_h"], r["mk"])
    load("mv", r["mv_h"], r["mv"])
    load("qw", r["qw_h"], qw)

    barrier = pltpu.get_barrier_semaphore()
    greeted = 0
    for target in xs[1:]:
        pl.semaphore_signal(barrier, inc=1, device_id={"tp": target}, device_id_type=MESH)
        greeted += 1
    friends = [partner] + [at(z, ys[d], c) for d in range(1, YN)]
    friends += [at(zs[d], y, ci) for d in range(1, ZN) for ci in (c, other)]
    for target in friends:
        pl.semaphore_signal(barrier, inc=1, device_id={"st": target}, device_id_type=MESH)
        greeted += 1
    pl.semaphore_wait(barrier, greeted)

    t_half = tok_n // 2
    half_rows = (pl.ds(0, t_half), pl.ds(t_half, t_half))

    def cot_copy(hop, d):
        source = zs[(1 - hop) % ZN] if d == 0 else zs[(hop - 1) % ZN]
        ref = qc.at[source, 1]
        if hop == ZN // 2:
            ref = qc.at[source, 1, half_rows[d]]
        return remote(ref, ref, "cotz", (hop - 1, d), st_id=z_to[d])

    def q_copies(hop, d, h):
        source = zs[(1 - hop) % ZN] if d == 0 else zs[(hop - 1) % ZN]
        if hop == ZN // 2 and h != d:
            return []
        ref = qc.at[source, 0, half_rows[h]]
        copies = [remote(ref, ref, "qz", (hop - 1, d, h), st_id=z_to[d])]
        if h == d and (hop < ZN // 2 or d == 0):
            copies.append(
                remote(gates.at[source], gates.at[source], "gz", (hop - 1, d), st_id=z_to[d])
            )
        return copies

    def tok_copy(hop, d, h):
        source = x if hop == 1 else (xs[XN - 1] if d == 0 else xs[1])
        ref = tok4.at[source, half_rows[h]]
        return remote(ref, ref, "tokx", (hop - 1, d, h), tp_id=x_to[d])

    def ids_copy(dc, dz):
        return remote(
            ids,
            r["ids_all"].at[c, z],
            "idsem",
            (dc,),
            st_id=at(zs[dz], y, other if dc else c),
            group="id1" if dc else "id0",
        )

    id_peers = [(dc, dz) for dz in range(ZN) for dc in range(CN) if (dc, dz) != (0, 0)]
    for dc, dz in id_peers:
        go(ids_copy(dc, dz))
    r["ids_all"][c, z] = ids[...]
    loads["tok"].wait()
    for d in range(2):
        go(tok_copy(1, d, d))
    for d in range(2):
        go(tok_copy(1, d, 1 - d))
    loads["cot"].wait()
    for d in range(2):
        go(cot_copy(1, d))

    per_chunk = proj_rows // BLOCK

    def kv_piece(yi, ci, k):
        return kv.at[pl.ds((yi * CN + ci) * passes + k * per_chunk, per_chunk)]

    def kv_copy(hop, d, k):
        yi = y if hop == 1 else (ys[YN - 1] if d == 0 else ys[1])
        ref = kv_piece(yi, c, k)
        return remote(ref, ref, "kvy", (hop - 1, d, k), st_id=y_to[d])

    def kv_across(rel, k):
        ref = kv_piece(ys[rel], c, k)
        return remote(ref, ref, "kvd", (0,), st_id=partner)

    loads["kw"].wait()
    loads["vw"].wait()
    for k in proj_order:
        loads[("rows", k)].wait()
        here = pl.ds(k * proj_rows, proj_rows)
        block = rows_v[here, :]
        low = low_dot(block, kw[...]).astype(BF16)
        key_low[here, :] = low
        low = low.astype(F32)
        scale = lax.rsqrt(jnp.mean(low * low, axis=-1, keepdims=True) + NORM_FLOOR)
        first = (y * CN + c) * passes + k * per_chunk
        kv[pl.ds(first, per_chunk), :, :head] = (
            (low * scale).astype(BF16).reshape(per_chunk, BLOCK, head)
        )
        kv[pl.ds(first, per_chunk), :, head:] = (
            low_dot(block, vw[...]).astype(BF16).reshape(per_chunk, BLOCK, head)
        )
        for d in range(2):
            go(kv_copy(1, d, k))
        go(kv_across(0, k))

    gwb[...] = jnp.broadcast_to(gate_w[...].astype(F32), gwb.shape)
    turned[...] = jnp.transpose(
        jnp.concatenate(
            [beta[...], decay[...], jnp.zeros((8 - 2 * heads_n, tok_n), F32)], axis=0
        )
    )
    states[...] = jnp.zeros_like(states)
    for key in ("mq", "mk", "mv", "qw"):
        loads[key].wait()

    def mix(b):
        here = pl.ds(pl.multiple_of(b * SPAN, SPAN), SPAN)
        for m in range(heads_n):
            cols = pl.ds(m * mix_dim, mix_dim)
            raw = turned[here, heads_n + m : heads_n + m + 1]
            softplus = jnp.maximum(raw, 0.0) + jnp.log1p(jnp.exp(-jnp.abs(raw)))
            mixed[here, cols], states[m] = mixer_span(
                r["mq"][here, cols].astype(F32),
                r["mk"][here, cols].astype(F32),
                r["mv"][here, cols].astype(F32),
                jax.nn.sigmoid(turned[here, m : m + 1]),
                -rate[m] * softplus,
                states[m],
            )

    spans_n = tok_n // SPAN

    def cot_pass(hop):
        for d in range(2):
            cot_copy(hop - 1, d).wait_recv()
            go(cot_copy(hop, d))

    def q_pass(hop, first):
        for d in range(2):
            h = d if first else 1 - d
            for copy in q_copies(hop - 1, d, h):
                copy.wait_recv()
            for copy in q_copies(hop, d, h):
                go(copy)

    def kv_pass(k):
        for d, rel in ((0, YN - 1), (1, 1)):
            kv_copy(1, d, k).wait_recv()
            if (k < 2) == (d == 0):
                go(kv_copy(2, d, k))
            go(kv_across(rel, k))

    w_half = width // CN

    def w_copy(w, d):
        rows = pl.ds(pl.multiple_of(xs[d] * width + c * w_half, w_half), w_half)
        return remote(
            (kw, vw, qw)[w].at[rows, :], w_all.at[x, c, w], "wxs", (0,), tp_id=xs[d]
        )

    def w_across(d):
        ref = w_all.at[xs[XN - d], c]
        return remote(ref, ref, "wxd", (0,), st_id=partner)

    def gw_copy(d):
        cols = pl.ds(pl.multiple_of(xs[d] * width, width), width)
        return remote(gwb.at[:, cols], gw_all.at[x], "gws", (0,), tp_id=xs[d])

    pl.loop(0, 1)(mix)
    cot_pass(2)
    for d in range(2):
        tok_copy(1, d, d).wait_recv()
        go(tok_copy(2, d, d))
    pl.loop(1, 3)(mix)
    cot_pass(3)
    kv_pass(0)
    for d in range(2):
        tok_copy(1, d, 1 - d).wait_recv()
        tok_copy(2, d, d).wait_recv()

    gate_rows = jnp.broadcast_to(gate_w[...], (16, model))
    logit = low_dot(gate_rows[:, :width], tok4[0], CONTRACT_LAST)
    for i in range(1, XN):
        logit += low_dot(gate_rows[:, i * width : (i + 1) * width], tok4[i], CONTRACT_LAST)
    gates[z] = jax.nn.sigmoid(logit[:8])

    @pl.loop(0, tok_n // ROW)
    def _(k):
        here = pl.ds(pl.multiple_of(k * ROW, ROW), ROW)
        low = low_dot(tok4[0, here, :], qw[pl.ds(0, width), :])
        for i in range(1, XN):
            low += low_dot(tok4[i, here, :], qw[pl.ds(i * width, width), :])
        low = low.astype(BF16)
        query_low[here, :] = low
        low = low.astype(F32)
        scale = lax.rsqrt(jnp.mean(low * low, axis=-1, keepdims=True) + NORM_FLOOR)
        qc[z, 0, here, :] = (low * scale).astype(BF16)

    for h in range(2):
        for d in range(2):
            for copy in q_copies(1, d, d if h == 0 else 1 - d):
                go(copy)
    for d in range(1, XN):
        for w in range(3):
            go(w_copy(w, d))
        go(gw_copy(d))
    for w, ref in enumerate((kw, vw, qw)):
        for h in range(CN):
            w_all[x, h, w] = ref[pl.ds(pl.multiple_of(x * width + h * w_half, w_half), w_half), :]
    gw_all[x] = gwb[:, pl.ds(pl.multiple_of(x * width, width), width)]
    pl.loop(3, 4)(mix)
    kv_pass(2)
    q_pass(2, True)
    kv_pass(1)
    cot_pass(4)
    id_refs = (r["ids_all"].at[0, pl.ds(0, ZN - 1)], r["ids_all"].at[1])
    for dc in range(CN):
        all_of(id_refs[dc], "idsem", (dc,), f"id{dc}").wait_recv()
    every = jnp.concatenate(
        [r["ids_all"][ci, zi, 0:1, :] for ci in range(CN) for zi in range(ZN)], axis=0
    )
    lane = lax.broadcasted_iota(jnp.int32, (CN * ZN, 128), 1)
    loc_tab = jnp.zeros((CN * ZN, 128), jnp.int32)
    blk_tab = jnp.zeros((CN * ZN, 128), jnp.int32)
    owner = lax.shift_right_logical(every, 4)
    local = every & (passes - 1)
    for o in range(slab):
        match = (owner == z * slab + o) & (lane < per_dev * 4)
        loc = jnp.sum(jnp.where(match, local, 0), axis=1, keepdims=True)
        blk = jnp.sum(
            jnp.where(match, lax.shift_right_logical(lane, 2) + 1, 0), axis=1, keepdims=True
        )
        loc_tab = jnp.where(lane == o, jnp.minimum(loc, passes - 1), loc_tab)
        blk_tab = jnp.where(lane == o, blk - 1, blk_tab)
    tab_v[0] = loc_tab
    tab_v[1] = blk_tab
    tab_copy = pltpu.make_async_copy(tab_v, tab_s, r["load"].at[len(loads)])
    tab_copy.start()
    q_pass(2, False)
    kv_pass(3)
    q_pass(3, True)
    q_pass(3, False)
    q_pass(4, True)
    pl.loop(4, 5)(mix)
    tab_copy.wait()
    lane_of = lax.broadcasted_iota(jnp.int32, (8, ZN * BLOCK), 1)
    for yi in range(YN):
        for which, ci in ((0, c), (1, other)):
            start = jnp.full((8, ZN * BLOCK), -1000000, jnp.int32)
            for zi in range(ZN):
                row = ci * ZN + zi
                base = jnp.where(
                    tab_s[1, row, yi * CN + c] >= 0,
                    tab_s[0, row, yi * CN + c] * BLOCK,
                    -1000000,
                )
                start = jnp.where(lax.shift_right_logical(lane_of, 6) == zi, base, start)
            code[yi, which] = start + (lane_of & (BLOCK - 1))
    for d in range(2):
        cot_copy(ZN // 2, d).wait_recv()
        for copy in q_copies(ZN // 2 - 1, d, 1 - d) + q_copies(ZN // 2, d, d):
            copy.wait_recv()
    for d, k in ((0, 0), (1, 2), (0, 1), (1, 3)):
        kv_copy(2, d, k).wait_recv()
        go(kv_across(2, k))
    kv_across_all = all_of(kv.at[pl.ds(0, YN * passes)], "kvd", (0,))
    kv_across_all.wait_recv()

    tok_block = lax.shift_right_logical(lax.broadcasted_iota(jnp.int32, (BLOCK, tok_n), 1), 6)
    key_halves = [pl.ds(i * ROW * 2, ROW * 2) for i in range(slab * BLOCK // (2 * ROW))]

    def gather(reader):
        for o in range(slab):
            local_at = jnp.clip(tab_s[0, c * ZN + reader, o], 0, passes - 1)
            kvr[pl.ds(o * BLOCK, BLOCK), :] = kv[o * passes + local_at]

    def zt_copy(d, reader):
        return remote(
            zt.at[reader], zt_r.at[d, reader], "zts", (reader,), st_id=at(zs[d], y, c)
        )

    @pl.loop(0, ZN)
    def _(reader):
        gather(reader)
        for part in key_halves:
            e_buf[reader, part, :] = low_dot(kvr[part, :head], qc[reader, 0], CONTRACT_LAST)
            g_buf[part, :] = low_dot(kvr[part, head:], qc[reader, 1], CONTRACT_LAST)
        total = jnp.zeros((1, tok_n), F32)
        product = jnp.zeros((1, tok_n), F32)
        for o in range(slab):
            here = pl.ds(o * BLOCK, BLOCK)
            mine = tok_block == tab_s[1, c * ZN + reader, o]
            e = jnp.where(mine, jnp.exp(e_buf[reader, here, :] * score_scale), 0.0)
            e_buf[reader, here, :] = e
            total += jnp.sum(e, axis=0, keepdims=True)
            product += jnp.sum(e * g_buf[here, :], axis=0, keepdims=True)
        zt[reader, 0:1, :] = total
        zt[reader, 1:2, :] = product * gates[reader, 0:1, :]
        for d in (4, 3, 5, 2, 6, 1, 7):
            zt_copy(d, reader).start()

    def summed(reader):
        both = zt[reader]
        for d in range(1, ZN):
            both += zt_r[d, reader]
        return both[0:1, :], both[1:2, :]

    def term_copy(reader):
        return remote(
            terms.at[other, reader], term_r.at[reader], "ters", (0,), st_id=partner
        )

    @pl.loop(0, ZN)
    def _(reader):
        all_of(zt_r.at[pl.ds(1, ZN - 1), reader], "zts", (reader,)).wait_recv()
        total, product = summed(reader)
        inverse = 1.0 / total
        mean = product * inverse
        gate = gates[reader, 0:1, :]
        gather(reader)
        for part in key_halves:
            g_buf[part, :] = low_dot(kvr[part, head:], qc[reader, 1], CONTRACT_LAST)
        for o in range(slab):
            here = pl.ds(o * BLOCK, BLOCK)
            probs = e_buf[reader, here, :] * inverse
            sg[here, :] = (probs * (g_buf[here, :] * gate - mean)).astype(BF16)
            pg[here, :] = (probs * gate).astype(BF16)
        for n, part in enumerate(key_halves):
            key_term = (low_dot(sg[part, :], qc[reader, 0]) * score_scale).astype(BF16)
            value_term = low_dot(pg[part, :], qc[reader, 1]).astype(BF16)
            for k in range(2 * ROW // BLOCK):
                o = n * (2 * ROW // BLOCK) + k
                piece = slice(k * BLOCK, (k + 1) * BLOCK)
                terms[o % CN, reader, o // CN, :, :head] = key_term[piece]
                terms[o % CN, reader, o // CN, :, head:] = value_term[piece]
        term_copy(reader).start()
        qg[reader] = (low_dot(sg[...], kvr[:, :head], CONTRACT_FIRST) * score_scale).astype(BF16)

    def z_copy(hop, d):
        if hop == 1:
            src = qg.at[zs[ZN // 2], half_rows[d]]
            dst = z_r.at[d, 0, half_rows[d]]
        else:
            src = z_s.at[d, hop - 1]
            dst = z_r.at[d, hop - 1]
        return remote(src, dst, "zrs", (d, hop - 1), st_id=z_to[d])

    def z_pass(hop):
        for d in range(2):
            z_copy(hop - 1, d).wait_recv()
            away = ZN // 2 + 1 - hop
            target = zs[away] if d == 0 else zs[(-away) % ZN]
            if hop == 2:
                mid, rest = half_rows[d], half_rows[1 - d]
                z_s[d, hop - 1, mid, :] = (
                    qg[target, mid, :].astype(F32) + z_r[d, 0, mid, :].astype(F32)
                ).astype(BF16)
                z_s[d, hop - 1, rest, :] = qg[target, rest, :]
            else:
                z_s[d, hop - 1] = (
                    qg[target].astype(F32) + z_r[d, hop - 2].astype(F32)
                ).astype(BF16)
            go(z_copy(hop, d))

    for d in range(2):
        go(z_copy(1, d))

    row_iota = lax.broadcasted_iota(jnp.int32, (ROW, ZN * BLOCK), 0)

    def pick(rel, q):
        yi = ys[rel]
        rows = row_iota + q * ROW
        ones = [
            jnp.where(rows == code[yi, which, 0:1, :], 1.0, 0.0).astype(BF16) for which in range(2)
        ]
        return low_dot(ones[0], terms[c, :, yi].reshape(ZN * BLOCK, 2 * head)) + low_dot(
            ones[1], term_r[:, yi].reshape(ZN * BLOCK, 2 * head)
        )

    yf_s, yf_r, yd_s, yd_r = get("yf_s", "yf_r", "yd_s", "yd_r")

    def two_step(far_s, far_r, near_s, near_r, far_sem, near_sem, term):
        def far(d, j):
            return remote(far_s.at[d, j], far_r.at[d, j], far_sem, (d, j), st_id=y_to[d])

        def near(d, q):
            return remote(near_s.at[d, q], near_r.at[d, q], near_sem, (q,), st_id=y_to[d])

        def send(j):
            for d in range(2):
                q = j + half * d
                far_s[d, j] = term(2, q).astype(BF16)
                go(far(d, j))
            for d in range(2):
                q = j + half * (1 - d)
                near_s[d, q] = term(1 if d == 0 else 3, q).astype(BF16)
                go(near(d, q))

        def forward(j):
            for d in range(2):
                q = j + half * d
                value = term(1 if d == 0 else 3, q)
                far(d, j).wait_recv()
                near_s[d, q] = (value + far_r[d, j].astype(F32)).astype(BF16)
                go(near(d, q))

        def final(q):
            value = term(0, q)
            all_of(near_r.at[:, q], near_sem, (q,)).wait_recv()
            return value + near_r[0, q].astype(F32) + near_r[1, q].astype(F32)

        return send, forward, final

    y_send, y_forward, y_final = two_step(yf_s, yf_r, yd_s, yd_r, "yfs", "yds", pick)

    def x_copy(hop, d, q):
        source = x if hop == 1 else (xs[XN - 1] if d == 0 else xs[1])
        ref = kgv.at[source, pl.ds(q * ROW, ROW)]
        passed_on = hop == 1 and (q < half) == (d == 0)
        return remote(ref, ref, "xrs", (0 if passed_on else 1, q), tp_id=x_to[d])

    def x_send(j):
        for q in (j, j + half):
            for d in range(2):
                go(x_copy(1, d, q))

    def x_forward(j):
        for d in range(2):
            q = j + half * d
            x_copy(1, d, q).wait_recv()
            go(x_copy(2, d, q))

    def weight_of(head_at, w):
        return w_all[head_at, :, w].reshape(width, head)

    def finish_rows(j):
        for q in (j, j + half):
            here = pl.ds(q * ROW, ROW)
            value = y_final(q)
            hat = value[:, :head]
            low = key_low[here, :].astype(F32)
            scale = lax.rsqrt(jnp.mean(low * low, axis=-1, keepdims=True) + NORM_FLOOR)
            grad = (
                scale * hat
                - scale * scale * scale * low * jnp.mean(low * hat, axis=-1, keepdims=True)
            ).astype(BF16)
            key_grad[here, :] = grad
            kgv[x, here, :head] = grad
            kgv[x, here, head:] = value[:, head:].astype(BF16)

    def finish_out(j):
        for d in range(2):
            q = j + half * d
            here = pl.ds(q * ROW, ROW)
            all_of(kgv.at[pl.ds(0, 2), here], "xrs", (1, q)).wait_recv()
            value = jnp.zeros((ROW, width), F32)
            for i in range(XN):
                value += low_dot(kgv[i, here, :head], weight_of(i, 0), CONTRACT_LAST)
                value += low_dot(kgv[i, here, head:], weight_of(i, 1), CONTRACT_LAST)
            out_ref[here, :] = value.astype(out_ref.dtype)
            leave(0, out_ref.at[here, :], r["out_ref"].at[here, :])

    wbuf, wc_r, w1, wy_r, w2, wz_r = get("wbuf", "wc_r", "w1", "wy_r", "w2", "wz_r")
    w_acc = r["w_acc"]
    part = weight_ref.shape[0]

    def weight_rows(j):
        low, high = pl.ds(j * ROW, ROW), pl.ds((j + half) * ROW, ROW)
        grad = jnp.concatenate([key_grad[low, :], key_grad[high, :]], axis=0)

        @pl.loop(0, ZN)
        def _(k):
            cols = pl.ds(pl.multiple_of(k * slab * part, slab * part), slab * part)
            rows = jnp.concatenate([rows_v[low, cols], rows_v[high, cols]], axis=0)
            tile = low_dot(rows, grad, CONTRACT_FIRST)
            if j > 0:
                tile += w_acc[cols, :]
            if j < half - 1:
                w_acc[cols, :] = tile
            else:
                tile = tile.astype(BF16)
                for o in range(slab):
                    wbuf[o % CN, o // CN, k] = tile[o * part : (o + 1) * part]

    all_of(term_r, "ters", (0,)).wait_recv()

    y_send(0)
    pl.loop(5, spans_n)(mix)
    y_forward(0)
    y_send(1)
    z_pass(2)
    finish_rows(0)
    x_send(0)
    y_forward(1)
    y_send(2)
    z_pass(3)
    all_of(w_all.at[pl.ds(0, XN - 1), 0], "wxs", (0,)).wait_recv()
    for d in range(1, XN):
        go(w_across(d))
    weight_rows(0)
    finish_rows(1)
    x_forward(0)
    x_send(1)
    z_pass(4)
    y_forward(2)
    y_send(3)
    weight_rows(1)
    all_of(w_all.at[pl.ds(0, XN - 1), 0], "wxd", (0,)).wait_recv()
    all_of(gw_all.at[pl.ds(0, XN - 1)], "gws", (0,)).wait_recv()
    finish_out(0)
    finish_rows(2)
    x_forward(1)
    x_send(2)
    y_forward(3)

    for d in range(2):
        z_copy(ZN // 2, d).wait_recv()
    total, product = summed(z)
    along = exact_dot(
        jnp.ones((8, head), F32), qc[z, 1].astype(F32) * mixed[...], CONTRACT_LAST
    )
    opened = gates[z]
    gga[x] = (1.0 - opened) * (product / total - opened * along)

    for k in range(tok_n // ROW):
        here = pl.ds(k * ROW, ROW)
        hat_grad = qg[z, here, :].astype(F32)
        for d in range(2):
            hat_grad += z_r[d, ZN // 2 - 1, here, :].astype(F32)
        low = query_low[here, :].astype(F32)
        scale = lax.rsqrt(jnp.mean(low * low, axis=-1, keepdims=True) + NORM_FLOOR)
        qga[x, here, :] = (
            scale * hat_grad
            - scale * scale * scale * low * jnp.mean(low * hat_grad, axis=-1, keepdims=True)
        ).astype(BF16)

    def t_copies(hop, d):
        source = x if hop == 1 else (xs[XN - 1] if d == 0 else xs[1])
        ref = qga.at[source] if hop == 1 else qga.at[source, half_rows[d]]
        copies = [remote(ref, ref, "tgs", (hop - 1, d), tp_id=x_to[d])]
        if hop == 1 or d == 0:
            copies.append(
                remote(gga.at[source], gga.at[source], "ggs", (hop - 1, d), tp_id=x_to[d])
            )
        return copies

    for d in range(2):
        for copy in t_copies(1, d):
            go(copy)
    weight_rows(2)
    finish_out(1)
    finish_rows(3)
    x_send(3)

    weight_rows(half - 1)
    wc_copy = remote(wbuf.at[other], wc_r, "wcs", (0,), st_id=partner)
    go(wc_copy)
    x_forward(2)
    for d in range(2):
        for copy in t_copies(1, d):
            copy.wait_recv()
        for copy in t_copies(2, d):
            go(copy)
    wc_copy.wait_recv()
    for yi in range(YN):
        w1[yi] = (wbuf[c, yi].astype(F32) + wc_r[yi].astype(F32)).astype(BF16)

    def wy_copy(d):
        return remote(w1.at[ys[d]], wy_r.at[d], "wys", (0,), st_id=at(z, ys[d], c))

    def wz_copy(d):
        return remote(w2.at[zs[d]], wz_r.at[d], "wzs", (0,), st_id=at(zs[d], y, c))

    for d in (2, 1, 3):
        go(wy_copy(d))
    finish_out(2)
    x_forward(3)
    all_of(wy_r.at[pl.ds(1, YN - 1)], "wys", (0,)).wait_recv()
    gathered = w1[y].astype(F32)
    for d in range(1, YN):
        gathered += wy_r[d].astype(F32)
    w2[...] = gathered.astype(BF16)
    for d in (4, 3, 5, 2, 6, 1, 7):
        go(wz_copy(d))
    for d in range(2):
        for copy in t_copies(2, d):
            copy.wait_recv()
    gate_rows = jnp.concatenate([gga[i, 0:1, :] for i in range(XN)] + [jnp.zeros((4, tok_n), F32)])
    gate_cols = jnp.concatenate([gw_all[i, 0:1, :] for i in range(XN)] + [jnp.zeros((4, width), F32)])
    for k in range(tok_n // ROW):
        here = pl.ds(k * ROW, ROW)
        value = exact_dot(gate_rows[:, k * ROW : (k + 1) * ROW], gate_cols, CONTRACT_FIRST)
        for i in range(XN):
            value += low_dot(qga[i, here, :], weight_of(i, 2), CONTRACT_LAST)
        tok_out[here, :] = value.astype(tok_out.dtype)
        leave(1, tok_out.at[here, :], r["tok_out"].at[here, :])
    all_of(wz_r.at[pl.ds(1, ZN - 1)], "wzs", (0,)).wait_recv()
    weight = w2[z].astype(F32)
    for d in range(1, ZN):
        weight += wz_r[d].astype(F32)
    weight_ref[...] = weight
    leave(2, weight_ref, r["weight_ref"])
    finish_out(3)
    moved = dict(
        id0=(id_refs[0], "idsem"),
        id1=(id_refs[1], "idsem"),
        tokx=(tok4.at[pl.ds(0, XN - 1)], "tokx"),
        cotz=(qg.at[pl.ds(0, ZN - 1)], "cotz"),
        qz=(qg.at[pl.ds(0, ZN - 1)], "qz"),
        gz=(gates.at[pl.ds(0, ZN - 1)], "gz"),
        kvy=(kv.at[pl.ds(0, 3 * passes)], "kvy"),
        kvd=(kv.at[pl.ds(0, YN * passes)], "kvd"),
        zts=(zt_r.at[pl.ds(1, ZN - 1)], "zts"),
        ters=(term_r, "ters"),
        zrs=(qg.at[pl.ds(0, ZN - 1)], "zrs"),
        yfs=(yf_s, "yfs"),
        yds=(yd_s, "yds"),
        xrs=(kgv.at[pl.ds(0, 3)], "xrs"),
        tgs=(qga.at[pl.ds(0, 3)], "tgs"),
        ggs=(gga.at[pl.ds(0, 3)], "ggs"),
        wxs=(w_all.at[pl.ds(0, XN - 1), 0], "wxs"),
        wxd=(w_all.at[pl.ds(0, XN - 1), 0], "wxd"),
        gws=(gw_all.at[pl.ds(0, XN - 1)], "gws"),
        wcs=(wc_r, "wcs"),
        wys=(wy_r.at[pl.ds(1, YN - 1)], "wys"),
        wzs=(wz_r.at[pl.ds(1, ZN - 1)], "wzs"),
    )
    for group, (ref, sem) in moved.items():
        index = (0,) * len(r[sem].shape)
        all_of(ref, sem, index, group).wait_send()
    for index, (src, dst) in enumerate(
        ((out_ref, "out_ref"), (tok_out, "tok_out"), (weight_ref, "weight_ref"))
    ):
        pltpu.make_async_copy(src, r[dst], r["outs"].at[index]).wait()


def fused_call(rate, ids, gate_w, beta, decay, tok, cot, mq, mk, mv, qw, kw, vw, rows):
    tok_n, width = tok.shape
    rows_n, model = rows.shape
    head = kw.shape[1]
    heads_n = beta.shape[0]
    vmem, sems = scratch_spec(tok_n, rows_n, width, head, heads_n, head // heads_n)
    part = model // (ZN * YN * CN)
    ins = ["rate", "ids", "gate_w", "beta", "decay"]
    ins += ["tok_h", "cot_h", "mq_h", "mk_h", "mv_h", "qw_h", "kw_h", "vw_h", "rows_h"]
    names = ins + ["tok_out", "out_ref", "weight_ref"] + list(vmem) + ["tab_s"] + list(sems)
    return pl.pallas_call(
        functools.partial(fused_kernel, names),
        out_shape=(
            jax.ShapeDtypeStruct((tok_n, width), BF16),
            jax.ShapeDtypeStruct((rows_n, width), BF16),
            jax.ShapeDtypeStruct((part, head), F32),
        ),
        in_specs=[SMEM_SPEC] + [VMEM_SPEC] * 4 + [ANY_SPEC] * 9,
        out_specs=(ANY_SPEC,) * 3,
        scratch_shapes=[pltpu.VMEM(*v) for v in vmem.values()]
        + [pltpu.SMEM((2, CN * ZN, 128), jnp.int32)]
        + [DMA(s) for s in sems.values()],
        compiler_params=pltpu.CompilerParams(
            collective_id=0, has_side_effects=True, vmem_limit_bytes=67043328
        ),
        name="fused",
    )(rate, ids, gate_w, beta, decay, tok, cot, mq, mk, mv, qw, kw, vw, rows)


def body(
    tokens,
    cotangent,
    mix_query,
    mix_key,
    mix_value,
    beta_pre,
    decay_pre,
    decay_rate,
    passages,
    passage_ids,
    query_weight,
    key_weight,
    value_weight,
    gate_weight,
):
    pass_local, span_rows, model_width = passages.shape
    flat_rows = passages.reshape(pass_local * span_rows, model_width)
    req_count = passage_ids.size
    ids = jnp.pad(passage_ids.reshape(1, req_count), ((0, 7), (0, -req_count % 128)))
    token_grad, passage_grad, key_weight_grad = fused_call(
        decay_rate,
        ids,
        gate_weight,
        beta_pre,
        decay_pre,
        tokens,
        cotangent,
        mix_query,
        mix_key,
        mix_value,
        query_weight,
        key_weight,
        value_weight,
        flat_rows,
    )
    token_grad, passage_grad, key_weight_grad = settle_call(
        token_grad, passage_grad, key_weight_grad
    )
    return (token_grad, passage_grad.reshape(pass_local, span_rows, -1), key_weight_grad)


def solution(mesh):
    placed = (
        P("st", "tp"),
        P("st", "tp"),
        P("st", "tp"),
        P("st", "tp"),
        P("st", "tp"),
        P("tp", "st"),
        P("tp", "st"),
        P("tp"),
        P("st", None, None),
        P("st", None),
        P(None, "tp"),
        P(None, "tp"),
        P(None, "tp"),
        P("tp", None),
    )
    return jax.shard_map(
        body,
        mesh=mesh,
        in_specs=placed,
        out_specs=(P("st", "tp"), P("st", None, "tp"), P("st", "tp")),
        check_vma=False,
    )
```

```python
import functools

import jax
import jax.numpy as jnp
from jax import lax
from jax.experimental import pallas as pl
from jax.experimental.pallas import tpu as pltpu
from jax.sharding import PartitionSpec as P

SPAN = 64
BLOCK = 64
NORM_FLOOR = 1.0
SCORE_GAIN = 4.0
HIGHEST = lax.Precision.HIGHEST
CONTRACT_LAST = (((1,), (1,)), ((), ()))
CONTRACT_FIRST = (((0,), (0,)), ((), ()))
F32, BF16 = jnp.float32, jnp.bfloat16

MESH = pl.DeviceIdType.MESH
VMEM_SPEC = pl.BlockSpec(memory_space=pltpu.VMEM)
ANY_SPEC = pl.BlockSpec(memory_space=pl.ANY)
SMEM_SPEC = pl.BlockSpec(memory_space=pltpu.SMEM)
DMA = pltpu.SemaphoreType.DMA

ZN, YN, CN, XN = 8, 4, 2, 4
ROW = 128
SENDS = ("id0", "id1", "tokx", "cotz", "qz", "gz", "kvy", "kvd", "zts", "ters", "zrs", "yfs")
SENDS += ("yds", "xrs", "tgs", "ggs", "wxs", "wxd", "gws", "wcs", "wys", "wzs")


def settle_kernel(*refs):
    count = (len(refs) - 1) // 3
    sources, targets, buffers, sems = refs[:count], refs[count : 2 * count], refs[2 * count : -1], refs[-1]
    moves = []
    for source, target, buffer in zip(sources, targets, buffers):
        pieces = 4 if source.shape[0] >= 512 else 1
        rows = source.shape[0] // pieces
        for k in range(pieces):
            here = pl.ds(k * rows, rows)
            n = len(moves)
            moves.append(
                (
                    pltpu.make_async_copy(source.at[here, :], buffer.at[here, :], sems.at[0, n]),
                    pltpu.make_async_copy(buffer.at[here, :], target.at[here, :], sems.at[1, n]),
                )
            )
    for inward, _ in moves:
        inward.start()
    for inward, outward in moves:
        inward.wait()
        outward.start()
    for _, outward in moves:
        outward.wait()


def settle_call(*arrays):
    return pl.pallas_call(
        settle_kernel,
        out_shape=tuple(jax.ShapeDtypeStruct(x.shape, x.dtype) for x in arrays),
        in_specs=[ANY_SPEC] * len(arrays),
        out_specs=(ANY_SPEC,) * len(arrays),
        scratch_shapes=[pltpu.VMEM(x.shape, x.dtype) for x in arrays] + [DMA((2, 6))],
        name="settle",
    )(*arrays)


def exact_dot(left, right, dims=(((1,), (0,)), ((), ()))):
    return lax.dot_general(left, right, dims, precision=HIGHEST, preferred_element_type=F32)


def low_dot(left, right, dims=(((1,), (0,)), ((), ()))):
    return lax.dot_general(left, right, dims, preferred_element_type=F32)


def mixer_span(queries, keys_in, values_in, strength, log_decay, state):
    span = queries.shape[0]
    row_at = lax.broadcasted_iota(jnp.int32, (span, span), 0)
    col_at = lax.broadcasted_iota(jnp.int32, (span, span), 1)
    inclusive = row_at >= col_at
    unit_eye = jnp.where(row_at == col_at, 1.0, 0.0)
    decay_row = jnp.sum(unit_eye * log_decay, axis=0, keepdims=True)
    cum_row = jnp.sum(jnp.where(row_at <= col_at, log_decay, 0.0), axis=0, keepdims=True)
    cum_col = jnp.sum(jnp.where(inclusive, decay_row, 0.0), axis=1, keepdims=True)
    total = jnp.sum(log_decay, axis=0, keepdims=True)
    decay_map = jnp.exp(jnp.where(inclusive, cum_col - cum_row, -1e30))
    queries = (
        queries
        * lax.rsqrt(jnp.sum(queries * queries, axis=-1, keepdims=True) + NORM_FLOOR)
        * queries.shape[-1] ** (-0.5)
    )
    keys_in = keys_in * lax.rsqrt(jnp.sum(keys_in * keys_in, axis=-1, keepdims=True) + NORM_FLOOR)
    power = jnp.where(
        row_at > col_at, strength * exact_dot(keys_in, keys_in, CONTRACT_LAST) * decay_map, 0.0
    )
    inverse = unit_eye - power
    for _ in range(span.bit_length() - 2):
        power = exact_dot(power, power)
        inverse = exact_dot(inverse, unit_eye + power)
    attend = exact_dot(queries, keys_in, CONTRACT_LAST) * decay_map
    fresh = exact_dot(inverse, values_in * strength)
    correction = exact_dot(inverse, keys_in * (strength * jnp.exp(cum_col)))
    new_values = fresh - exact_dot(correction, state)
    output = exact_dot(queries * jnp.exp(cum_col), state) + exact_dot(attend, new_values)
    state = state * jnp.exp(total) + exact_dot(
        keys_in * jnp.exp(total - cum_col), new_values, CONTRACT_FIRST
    )
    return output, state


def scratch_spec(tok_n, rows_n, width, head, heads_n, mix_dim):
    model = width * XN
    slab = YN * CN
    passes = rows_n // BLOCK
    chunks = rows_n // ROW
    half = chunks // 2
    part = model // (ZN * slab)
    keys = slab * BLOCK
    vmem = dict(
        rows_v=((rows_n, model), BF16),
        kw=((model, head), BF16),
        vw=((model, head), BF16),
        qw=((model, head), BF16),
        tok4=((XN, tok_n, width), BF16),
        kv=((slab * passes, BLOCK, 2 * head), BF16),
        qc=((ZN, 2, tok_n, head), BF16),
        gates=((ZN, 8, tok_n), F32),
        mq=((tok_n, head), BF16),
        mk=((tok_n, head), BF16),
        mv=((tok_n, head), BF16),
        ids_all=((CN, ZN, 8, 128), jnp.int32),
        tab_v=((2, CN * ZN, 128), jnp.int32),
        ids_v=((8, 128), jnp.int32),
        code=((YN, CN, 8, ZN * BLOCK), jnp.int32),
        turned=((tok_n, 8), F32),
        mixed=((tok_n, head), F32),
        states=((heads_n, mix_dim, mix_dim), F32),
        key_low=((rows_n, head), BF16),
        query_low=((tok_n, head), BF16),
        kvr=((keys, 2 * head), BF16),
        e_buf=((ZN, keys, tok_n), F32),
        g_buf=((keys, tok_n), F32),
        sg=((keys, tok_n), BF16),
        pg=((keys, tok_n), BF16),
        zt=((ZN, 2, tok_n), F32),
        zt_r=((ZN, ZN, 2, tok_n), F32),
        terms=((CN, ZN, YN, BLOCK, 2 * head), BF16),
        term_r=((ZN, YN, BLOCK, 2 * head), BF16),
        qg=((ZN, tok_n, head), BF16),
        z_s=((2, ZN // 2, tok_n, head), BF16),
        z_r=((2, ZN // 2, tok_n, head), BF16),
        yf_s=((2, half, ROW, 2 * head), BF16),
        yf_r=((2, half, ROW, 2 * head), BF16),
        yd_s=((2, chunks, ROW, 2 * head), BF16),
        yd_r=((2, chunks, ROW, 2 * head), BF16),
        key_grad=((rows_n, head), BF16),
        kgv=((XN, rows_n, 2 * head), BF16),
        qga=((XN, tok_n, head), BF16),
        gga=((XN, 8, tok_n), F32),
        w_all=((XN, CN, 3, width // CN, head), BF16),
        gwb=((8, model), F32),
        gw_all=((XN, 8, width), F32),
        wbuf=((CN, YN, ZN, part, head), BF16),
        wc_r=((YN, ZN, part, head), BF16),
        w1=((YN, ZN, part, head), BF16),
        wy_r=((YN, ZN, part, head), BF16),
        w2=((ZN, part, head), BF16),
        wz_r=((ZN, part, head), BF16),
        tok_v=((tok_n, width), BF16),
        out_v=((rows_n, width), BF16),
        weight_v=((part, head), F32),
        w_acc=((model, head), F32),
    )
    sems = dict(
        load=(16,),
        outs=(3,),
        send=(len(SENDS),),
        idsem=(CN,),
        tokx=(2, 2, 2),
        cotz=(ZN // 2, 2),
        qz=(ZN // 2, 2, 2),
        gz=(ZN // 2, 2),
        kvy=(2, 2, 4),
        kvd=(1,),
        zts=(ZN,),
        ters=(1,),
        zrs=(2, ZN // 2),
        yfs=(2, half),
        yds=(chunks,),
        xrs=(2, chunks),
        tgs=(2, 2),
        ggs=(2, 2),
        wxs=(1,),
        wxd=(1,),
        gws=(1,),
        wcs=(1,),
        wys=(1,),
        wzs=(1,),
    )
    return vmem, sems


def fused_kernel(names, *refs):
    r = dict(zip(names, refs))

    def get(*keys):
        return [r[k] for k in keys]

    rate, ids, gate_w, beta, decay = get("rate", "ids", "gate_w", "beta", "decay")
    tok_out, out_ref, weight_ref = get("tok_v", "out_v", "weight_v")
    rows_v, kw, vw, qw, tok4, kv, qc, gates = get(
        "rows_v", "kw", "vw", "qw", "tok4", "kv", "qc", "gates"
    )
    tab_v, tab_s, code = get("tab_v", "tab_s", "code")
    kvr, e_buf, g_buf, sg, pg, zt, zt_r = get("kvr", "e_buf", "g_buf", "sg", "pg", "zt", "zt_r")
    terms, term_r, qg, z_s, z_r = get("terms", "term_r", "qg", "z_s", "z_r")
    key_low, key_grad, query_low = get("key_low", "key_grad", "query_low")
    kgv, qga, gga, w_all, gwb, gw_all = get("kgv", "qga", "gga", "w_all", "gwb", "gw_all")
    turned, mixed, states = get("turned", "mixed", "states")

    rows_n, model = rows_v.shape
    head = kw.shape[1]
    tok_n, width = tok_out.shape
    heads_n = beta.shape[0]
    mix_dim = head // heads_n
    slab = YN * CN
    passes = rows_n // BLOCK
    chunks = rows_n // ROW
    half = chunks // 2
    per_dev = tok_n // BLOCK
    score_scale = SCORE_GAIN * head ** (-0.5)

    st = lax.axis_index("st")
    x = lax.axis_index("tp")
    c = lax.rem(st, CN)
    y = lax.rem(st // CN, YN)
    z = st // slab
    other = 1 - c

    def at(zi, yi, ci):
        return (zi * YN + yi) * CN + ci

    def step(value, by, n):
        return lax.rem(value + (by % n), n)

    xs = [step(x, i, XN) for i in range(XN)]
    ys = [step(y, i, YN) for i in range(YN)]
    zs = [step(z, i, ZN) for i in range(ZN)]
    partner = at(z, y, other)
    x_to = (xs[1], xs[XN - 1])
    y_to = (at(z, ys[1], c), at(z, ys[YN - 1], c))
    z_to = (at(zs[1], y, c), at(zs[ZN - 1], y, c))

    def remote(src, dst, sem, index, st_id=None, tp_id=None, group=None):
        device = {}
        if st_id is not None:
            device["st"] = st_id
        if tp_id is not None:
            device["tp"] = tp_id
        return pltpu.make_async_remote_copy(
            src_ref=src,
            dst_ref=dst,
            send_sem=r["send"].at[SENDS.index(group or sem)],
            recv_sem=r[sem].at[index],
            device_id=device,
            device_id_type=MESH,
        )

    def go(copy):
        copy.start()

    def all_of(ref, sem, index, group=None):
        return remote(ref, ref, sem, index, st_id=partner, group=group)

    def leave(index, src, dst):
        pltpu.make_async_copy(src, dst, r["outs"].at[index]).start()

    loads = {}

    def load(key, src, dst):
        loads[key] = pltpu.make_async_copy(src, dst, r["load"].at[len(loads)])
        loads[key].start()

    load("cot", r["cot_h"], qc.at[z, 1])
    load("tok", r["tok_h"], tok4.at[x])
    load("kw", r["kw_h"], kw)
    load("vw", r["vw_h"], vw)
    proj_rows = rows_n // 4
    proj_order = (0, 2, 1, 3)
    for k in proj_order:
        here = pl.ds(k * proj_rows, proj_rows)
        load(("rows", k), r["rows_h"].at[here, :], rows_v.at[here, :])
    load("mq", r["mq_h"], r["mq"])
    load("mk", r["mk_h"], r["mk"])
    load("mv", r["mv_h"], r["mv"])
    load("qw", r["qw_h"], qw)

    id_lane = lax.broadcasted_iota(jnp.int32, (8, 128), 1)
    id_row = jnp.zeros((8, 128), jnp.int32)
    per_block, blocks_n = ids.shape
    for b in range(blocks_n):
        for k in range(per_block):
            id_row = jnp.where(id_lane == b * per_block + k, ids[k, b], id_row)
    r["ids_v"][...] = id_row

    barrier = pltpu.get_barrier_semaphore()
    greeted = 0
    for target in xs[1:]:
        pl.semaphore_signal(barrier, inc=1, device_id={"tp": target}, device_id_type=MESH)
        greeted += 1
    friends = [partner] + [at(z, ys[d], c) for d in range(1, YN)]
    friends += [at(zs[d], y, ci) for d in range(1, ZN) for ci in (c, other)]
    for target in friends:
        pl.semaphore_signal(barrier, inc=1, device_id={"st": target}, device_id_type=MESH)
        greeted += 1
    pl.semaphore_wait(barrier, greeted)

    t_half = tok_n // 2
    half_rows = (pl.ds(0, t_half), pl.ds(t_half, t_half))

    def cot_copy(hop, d):
        source = zs[(1 - hop) % ZN] if d == 0 else zs[(hop - 1) % ZN]
        ref = qc.at[source, 1]
        if hop == ZN // 2:
            ref = qc.at[source, 1, half_rows[d]]
        return remote(ref, ref, "cotz", (hop - 1, d), st_id=z_to[d])

    def q_copies(hop, d, h):
        source = zs[(1 - hop) % ZN] if d == 0 else zs[(hop - 1) % ZN]
        if hop == ZN // 2 and h != d:
            return []
        ref = qc.at[source, 0, half_rows[h]]
        copies = [remote(ref, ref, "qz", (hop - 1, d, h), st_id=z_to[d])]
        if h == d and (hop < ZN // 2 or d == 0):
            copies.append(
                remote(gates.at[source], gates.at[source], "gz", (hop - 1, d), st_id=z_to[d])
            )
        return copies

    def tok_copy(hop, d, h):
        source = x if hop == 1 else (xs[XN - 1] if d == 0 else xs[1])
        ref = tok4.at[source, half_rows[h]]
        return remote(ref, ref, "tokx", (hop - 1, d, h), tp_id=x_to[d])

    def ids_copy(dc, dz):
        return remote(
            r["ids_v"],
            r["ids_all"].at[c, z],
            "idsem",
            (dc,),
            st_id=at(zs[dz], y, other if dc else c),
            group="id1" if dc else "id0",
        )

    id_peers = [(dc, dz) for dz in range(ZN) for dc in range(CN) if (dc, dz) != (0, 0)]
    for dc, dz in id_peers:
        go(ids_copy(dc, dz))
    r["ids_all"][c, z] = id_row
    loads["tok"].wait()
    for d in range(2):
        go(tok_copy(1, d, d))
    for d in range(2):
        go(tok_copy(1, d, 1 - d))
    loads["cot"].wait()
    for d in range(2):
        go(cot_copy(1, d))

    per_chunk = proj_rows // BLOCK

    def kv_piece(yi, ci, k):
        return kv.at[pl.ds((yi * CN + ci) * passes + k * per_chunk, per_chunk)]

    def kv_copy(hop, d, k):
        yi = y if hop == 1 else (ys[YN - 1] if d == 0 else ys[1])
        ref = kv_piece(yi, c, k)
        return remote(ref, ref, "kvy", (hop - 1, d, k), st_id=y_to[d])

    def kv_across(rel, k):
        ref = kv_piece(ys[rel], c, k)
        return remote(ref, ref, "kvd", (0,), st_id=partner)

    loads["kw"].wait()
    loads["vw"].wait()
    for k in proj_order:
        loads[("rows", k)].wait()
        here = pl.ds(k * proj_rows, proj_rows)
        block = rows_v[here, :]
        low = low_dot(block, kw[...]).astype(BF16)
        key_low[here, :] = low
        low = low.astype(F32)
        scale = lax.rsqrt(jnp.mean(low * low, axis=-1, keepdims=True) + NORM_FLOOR)
        first = (y * CN + c) * passes + k * per_chunk
        kv[pl.ds(first, per_chunk), :, :head] = (
            (low * scale).astype(BF16).reshape(per_chunk, BLOCK, head)
        )
        kv[pl.ds(first, per_chunk), :, head:] = (
            low_dot(block, vw[...]).astype(BF16).reshape(per_chunk, BLOCK, head)
        )
        for d in range(2):
            go(kv_copy(1, d, k))
        go(kv_across(0, k))

    gwb[...] = jnp.broadcast_to(gate_w[...].astype(F32), gwb.shape)
    turned[...] = jnp.transpose(
        jnp.concatenate(
            [beta[...], decay[...], jnp.zeros((8 - 2 * heads_n, tok_n), F32)], axis=0
        )
    )
    states[...] = jnp.zeros_like(states)
    for key in ("mq", "mk", "mv", "qw"):
        loads[key].wait()

    def mix(b):
        here = pl.ds(pl.multiple_of(b * SPAN, SPAN), SPAN)
        for m in range(heads_n):
            cols = pl.ds(m * mix_dim, mix_dim)
            raw = turned[here, heads_n + m : heads_n + m + 1]
            softplus = jnp.maximum(raw, 0.0) + jnp.log1p(jnp.exp(-jnp.abs(raw)))
            mixed[here, cols], states[m] = mixer_span(
                r["mq"][here, cols].astype(F32),
                r["mk"][here, cols].astype(F32),
                r["mv"][here, cols].astype(F32),
                jax.nn.sigmoid(turned[here, m : m + 1]),
                -rate[m] * softplus,
                states[m],
            )

    spans_n = tok_n // SPAN

    def cot_pass(hop):
        for d in range(2):
            cot_copy(hop - 1, d).wait_recv()
            go(cot_copy(hop, d))

    def q_pass(hop, first):
        for d in range(2):
            h = d if first else 1 - d
            for copy in q_copies(hop - 1, d, h):
                copy.wait_recv()
            for copy in q_copies(hop, d, h):
                go(copy)

    def kv_pass(k):
        for d, rel in ((0, YN - 1), (1, 1)):
            kv_copy(1, d, k).wait_recv()
            if (k < 2) == (d == 0):
                go(kv_copy(2, d, k))
            go(kv_across(rel, k))

    w_half = width // CN

    def w_copy(w, d):
        rows = pl.ds(pl.multiple_of(xs[d] * width + c * w_half, w_half), w_half)
        return remote(
            (kw, vw, qw)[w].at[rows, :], w_all.at[x, c, w], "wxs", (0,), tp_id=xs[d]
        )

    def w_across(d):
        ref = w_all.at[xs[XN - d], c]
        return remote(ref, ref, "wxd", (0,), st_id=partner)

    def gw_copy(d):
        cols = pl.ds(pl.multiple_of(xs[d] * width, width), width)
        return remote(gwb.at[:, cols], gw_all.at[x], "gws", (0,), tp_id=xs[d])

    pl.loop(0, 1)(mix)
    cot_pass(2)
    for d in range(2):
        tok_copy(1, d, d).wait_recv()
        go(tok_copy(2, d, d))
    pl.loop(1, 3)(mix)
    cot_pass(3)
    kv_pass(0)
    for d in range(2):
        tok_copy(1, d, 1 - d).wait_recv()
        tok_copy(2, d, d).wait_recv()

    gate_rows = jnp.broadcast_to(gate_w[...], (16, model))
    logit = low_dot(gate_rows[:, :width], tok4[0], CONTRACT_LAST)
    for i in range(1, XN):
        logit += low_dot(gate_rows[:, i * width : (i + 1) * width], tok4[i], CONTRACT_LAST)
    gates[z] = jax.nn.sigmoid(logit[:8])

    @pl.loop(0, tok_n // ROW)
    def _(k):
        here = pl.ds(pl.multiple_of(k * ROW, ROW), ROW)
        low = low_dot(tok4[0, here, :], qw[pl.ds(0, width), :])
        for i in range(1, XN):
            low += low_dot(tok4[i, here, :], qw[pl.ds(i * width, width), :])
        low = low.astype(BF16)
        query_low[here, :] = low
        low = low.astype(F32)
        scale = lax.rsqrt(jnp.mean(low * low, axis=-1, keepdims=True) + NORM_FLOOR)
        qc[z, 0, here, :] = (low * scale).astype(BF16)

    for h in range(2):
        for d in range(2):
            for copy in q_copies(1, d, d if h == 0 else 1 - d):
                go(copy)
    for d in range(1, XN):
        for w in range(3):
            go(w_copy(w, d))
        go(gw_copy(d))
    for w, ref in enumerate((kw, vw, qw)):
        for h in range(CN):
            w_all[x, h, w] = ref[pl.ds(pl.multiple_of(x * width + h * w_half, w_half), w_half), :]
    gw_all[x] = gwb[:, pl.ds(pl.multiple_of(x * width, width), width)]
    pl.loop(3, 4)(mix)
    kv_pass(2)
    q_pass(2, True)
    kv_pass(1)
    cot_pass(4)
    id_refs = (r["ids_all"].at[0, pl.ds(0, ZN - 1)], r["ids_all"].at[1])
    for dc in range(CN):
        all_of(id_refs[dc], "idsem", (dc,), f"id{dc}").wait_recv()
    every = jnp.concatenate(
        [r["ids_all"][ci, zi, 0:1, :] for ci in range(CN) for zi in range(ZN)], axis=0
    )
    lane = lax.broadcasted_iota(jnp.int32, (CN * ZN, 128), 1)
    loc_tab = jnp.zeros((CN * ZN, 128), jnp.int32)
    blk_tab = jnp.zeros((CN * ZN, 128), jnp.int32)
    owner = lax.shift_right_logical(every, 4)
    local = every & (passes - 1)
    for o in range(slab):
        match = (owner == z * slab + o) & (lane < per_dev * 4)
        loc = jnp.sum(jnp.where(match, local, 0), axis=1, keepdims=True)
        blk = jnp.sum(
            jnp.where(match, lax.shift_right_logical(lane, 2) + 1, 0), axis=1, keepdims=True
        )
        loc_tab = jnp.where(lane == o, jnp.minimum(loc, passes - 1), loc_tab)
        blk_tab = jnp.where(lane == o, blk - 1, blk_tab)
    tab_v[0] = loc_tab
    tab_v[1] = blk_tab
    tab_copy = pltpu.make_async_copy(tab_v, tab_s, r["load"].at[len(loads)])
    tab_copy.start()
    q_pass(2, False)
    kv_pass(3)
    q_pass(3, True)
    q_pass(3, False)
    q_pass(4, True)
    tab_copy.wait()
    lane_of = lax.broadcasted_iota(jnp.int32, (8, ZN * BLOCK), 1)
    for yi in range(YN):
        for which, ci in ((0, c), (1, other)):
            start = jnp.full((8, ZN * BLOCK), -1000000, jnp.int32)
            for zi in range(ZN):
                row = ci * ZN + zi
                base = jnp.where(
                    tab_s[1, row, yi * CN + c] >= 0,
                    tab_s[0, row, yi * CN + c] * BLOCK,
                    -1000000,
                )
                start = jnp.where(lax.shift_right_logical(lane_of, 6) == zi, base, start)
            code[yi, which] = start + (lane_of & (BLOCK - 1))
    for d in range(2):
        cot_copy(ZN // 2, d).wait_recv()
        for copy in q_copies(ZN // 2 - 1, d, 1 - d) + q_copies(ZN // 2, d, d):
            copy.wait_recv()
    for d, k in ((0, 0), (1, 2), (0, 1), (1, 3)):
        kv_copy(2, d, k).wait_recv()
        go(kv_across(2, k))
    kv_across_all = all_of(kv.at[pl.ds(0, YN * passes)], "kvd", (0,))
    kv_across_all.wait_recv()

    tok_block = lax.shift_right_logical(lax.broadcasted_iota(jnp.int32, (BLOCK, tok_n), 1), 6)
    key_halves = [pl.ds(i * ROW * 2, ROW * 2) for i in range(slab * BLOCK // (2 * ROW))]

    def gather(reader):
        for o in range(slab):
            local_at = jnp.clip(tab_s[0, c * ZN + reader, o], 0, passes - 1)
            kvr[pl.ds(o * BLOCK, BLOCK), :] = kv[o * passes + local_at]

    def zt_copy(d, reader):
        return remote(
            zt.at[reader], zt_r.at[d, reader], "zts", (reader,), st_id=at(zs[d], y, c)
        )

    @pl.loop(0, ZN)
    def _(reader):
        gather(reader)
        for part in key_halves:
            e_buf[reader, part, :] = low_dot(kvr[part, :head], qc[reader, 0], CONTRACT_LAST)
            g_buf[part, :] = low_dot(kvr[part, head:], qc[reader, 1], CONTRACT_LAST)
        total = jnp.zeros((1, tok_n), F32)
        product = jnp.zeros((1, tok_n), F32)
        for o in range(slab):
            here = pl.ds(o * BLOCK, BLOCK)
            mine = tok_block == tab_s[1, c * ZN + reader, o]
            e = jnp.where(mine, jnp.exp(e_buf[reader, here, :] * score_scale), 0.0)
            e_buf[reader, here, :] = e
            total += jnp.sum(e, axis=0, keepdims=True)
            product += jnp.sum(e * g_buf[here, :], axis=0, keepdims=True)
        zt[reader, 0:1, :] = total
        zt[reader, 1:2, :] = product * gates[reader, 0:1, :]
        for d in (4, 3, 5, 2, 6, 1, 7):
            zt_copy(d, reader).start()

    def summed(reader):
        both = zt[reader]
        for d in range(1, ZN):
            both += zt_r[d, reader]
        return both[0:1, :], both[1:2, :]

    def term_copy(reader):
        return remote(
            terms.at[other, reader], term_r.at[reader], "ters", (0,), st_id=partner
        )

    @pl.loop(0, ZN)
    def _(reader):
        all_of(zt_r.at[pl.ds(1, ZN - 1), reader], "zts", (reader,)).wait_recv()
        total, product = summed(reader)
        inverse = 1.0 / total
        mean = product * inverse
        gate = gates[reader, 0:1, :]
        gather(reader)
        for part in key_halves:
            g_buf[part, :] = low_dot(kvr[part, head:], qc[reader, 1], CONTRACT_LAST)
        for o in range(slab):
            here = pl.ds(o * BLOCK, BLOCK)
            probs = e_buf[reader, here, :] * inverse
            sg[here, :] = (probs * (g_buf[here, :] * gate - mean)).astype(BF16)
            pg[here, :] = (probs * gate).astype(BF16)
        for n, part in enumerate(key_halves):
            key_term = (low_dot(sg[part, :], qc[reader, 0]) * score_scale).astype(BF16)
            value_term = low_dot(pg[part, :], qc[reader, 1]).astype(BF16)
            for k in range(2 * ROW // BLOCK):
                o = n * (2 * ROW // BLOCK) + k
                piece = slice(k * BLOCK, (k + 1) * BLOCK)
                terms[o % CN, reader, o // CN, :, :head] = key_term[piece]
                terms[o % CN, reader, o // CN, :, head:] = value_term[piece]
        term_copy(reader).start()
        qg[reader] = (low_dot(sg[...], kvr[:, :head], CONTRACT_FIRST) * score_scale).astype(BF16)

    def z_copy(hop, d):
        if hop == 1:
            src = qg.at[zs[ZN // 2], half_rows[d]]
            dst = z_r.at[d, 0, half_rows[d]]
        else:
            src = z_s.at[d, hop - 1]
            dst = z_r.at[d, hop - 1]
        return remote(src, dst, "zrs", (d, hop - 1), st_id=z_to[d])

    def z_pass(hop):
        for d in range(2):
            z_copy(hop - 1, d).wait_recv()
            away = ZN // 2 + 1 - hop
            target = zs[away] if d == 0 else zs[(-away) % ZN]
            if hop == 2:
                mid, rest = half_rows[d], half_rows[1 - d]
                z_s[d, hop - 1, mid, :] = (
                    qg[target, mid, :].astype(F32) + z_r[d, 0, mid, :].astype(F32)
                ).astype(BF16)
                z_s[d, hop - 1, rest, :] = qg[target, rest, :]
            else:
                z_s[d, hop - 1] = (
                    qg[target].astype(F32) + z_r[d, hop - 2].astype(F32)
                ).astype(BF16)
            go(z_copy(hop, d))

    for d in range(2):
        go(z_copy(1, d))

    row_iota = lax.broadcasted_iota(jnp.int32, (ROW, ZN * BLOCK), 0)

    def pick(rel, q):
        yi = ys[rel]
        rows = row_iota + q * ROW
        ones = [
            jnp.where(rows == code[yi, which, 0:1, :], 1.0, 0.0).astype(BF16) for which in range(2)
        ]
        return low_dot(ones[0], terms[c, :, yi].reshape(ZN * BLOCK, 2 * head)) + low_dot(
            ones[1], term_r[:, yi].reshape(ZN * BLOCK, 2 * head)
        )

    yf_s, yf_r, yd_s, yd_r = get("yf_s", "yf_r", "yd_s", "yd_r")

    def two_step(far_s, far_r, near_s, near_r, far_sem, near_sem, term):
        def far(d, j):
            return remote(far_s.at[d, j], far_r.at[d, j], far_sem, (d, j), st_id=y_to[d])

        def near(d, q):
            return remote(near_s.at[d, q], near_r.at[d, q], near_sem, (q,), st_id=y_to[d])

        def send(j):
            for d in range(2):
                q = j + half * d
                far_s[d, j] = term(2, q).astype(BF16)
                go(far(d, j))
            for d in range(2):
                q = j + half * (1 - d)
                near_s[d, q] = term(1 if d == 0 else 3, q).astype(BF16)
                go(near(d, q))

        def forward(j):
            for d in range(2):
                q = j + half * d
                value = term(1 if d == 0 else 3, q)
                far(d, j).wait_recv()
                near_s[d, q] = (value + far_r[d, j].astype(F32)).astype(BF16)
                go(near(d, q))

        def final(q):
            value = term(0, q)
            all_of(near_r.at[:, q], near_sem, (q,)).wait_recv()
            return value + near_r[0, q].astype(F32) + near_r[1, q].astype(F32)

        return send, forward, final

    y_send, y_forward, y_final = two_step(yf_s, yf_r, yd_s, yd_r, "yfs", "yds", pick)

    def x_copy(hop, d, q):
        source = x if hop == 1 else (xs[XN - 1] if d == 0 else xs[1])
        ref = kgv.at[source, pl.ds(q * ROW, ROW)]
        passed_on = hop == 1 and (q < half) == (d == 0)
        return remote(ref, ref, "xrs", (0 if passed_on else 1, q), tp_id=x_to[d])

    def x_send(j):
        for q in (j, j + half):
            for d in range(2):
                go(x_copy(1, d, q))

    def x_forward(j):
        for d in range(2):
            q = j + half * d
            x_copy(1, d, q).wait_recv()
            go(x_copy(2, d, q))

    def weight_of(head_at, w):
        return w_all[head_at, :, w].reshape(width, head)

    def finish_rows(j):
        for q in (j, j + half):
            here = pl.ds(q * ROW, ROW)
            value = y_final(q)
            hat = value[:, :head]
            low = key_low[here, :].astype(F32)
            scale = lax.rsqrt(jnp.mean(low * low, axis=-1, keepdims=True) + NORM_FLOOR)
            grad = (
                scale * hat
                - scale * scale * scale * low * jnp.mean(low * hat, axis=-1, keepdims=True)
            ).astype(BF16)
            key_grad[here, :] = grad
            kgv[x, here, :head] = grad
            kgv[x, here, head:] = value[:, head:].astype(BF16)

    def finish_out(j):
        for d in range(2):
            q = j + half * d
            here = pl.ds(q * ROW, ROW)
            all_of(kgv.at[pl.ds(0, 2), here], "xrs", (1, q)).wait_recv()
            value = jnp.zeros((ROW, width), F32)
            for i in range(XN):
                value += low_dot(kgv[i, here, :head], weight_of(i, 0), CONTRACT_LAST)
                value += low_dot(kgv[i, here, head:], weight_of(i, 1), CONTRACT_LAST)
            out_ref[here, :] = value.astype(out_ref.dtype)
            leave(0, out_ref.at[here, :], r["out_ref"].at[here, :])

    wbuf, wc_r, w1, wy_r, w2, wz_r = get("wbuf", "wc_r", "w1", "wy_r", "w2", "wz_r")
    w_acc = r["w_acc"]
    part = weight_ref.shape[0]

    def weight_rows(j):
        low, high = pl.ds(j * ROW, ROW), pl.ds((j + half) * ROW, ROW)
        grad = jnp.concatenate([key_grad[low, :], key_grad[high, :]], axis=0)

        @pl.loop(0, ZN)
        def _(k):
            cols = pl.ds(pl.multiple_of(k * slab * part, slab * part), slab * part)
            rows = jnp.concatenate([rows_v[low, cols], rows_v[high, cols]], axis=0)
            tile = low_dot(rows, grad, CONTRACT_FIRST)
            if j > 0:
                tile += w_acc[cols, :]
            if j < half - 1:
                w_acc[cols, :] = tile
            else:
                tile = tile.astype(BF16)
                for o in range(slab):
                    wbuf[o % CN, o // CN, k] = tile[o * part : (o + 1) * part]

    all_of(term_r, "ters", (0,)).wait_recv()

    y_send(0)
    pl.loop(4, 5)(mix)
    y_forward(0)
    y_send(1)
    z_pass(2)
    pl.loop(5, spans_n)(mix)
    finish_rows(0)
    x_send(0)
    y_forward(1)
    y_send(2)
    z_pass(3)
    all_of(w_all.at[pl.ds(0, XN - 1), 0], "wxs", (0,)).wait_recv()
    for d in range(1, XN):
        go(w_across(d))
    weight_rows(0)
    finish_rows(1)
    x_forward(0)
    x_send(1)
    z_pass(4)
    y_forward(2)
    y_send(3)
    weight_rows(1)
    all_of(w_all.at[pl.ds(0, XN - 1), 0], "wxd", (0,)).wait_recv()
    all_of(gw_all.at[pl.ds(0, XN - 1)], "gws", (0,)).wait_recv()
    finish_out(0)
    finish_rows(2)
    x_forward(1)
    x_send(2)
    y_forward(3)

    for d in range(2):
        z_copy(ZN // 2, d).wait_recv()
    total, product = summed(z)
    along = exact_dot(
        jnp.ones((8, head), F32), qc[z, 1].astype(F32) * mixed[...], CONTRACT_LAST
    )
    opened = gates[z]
    gga[x] = (1.0 - opened) * (product / total - opened * along)

    for k in range(tok_n // ROW):
        here = pl.ds(k * ROW, ROW)
        hat_grad = qg[z, here, :].astype(F32)
        for d in range(2):
            hat_grad += z_r[d, ZN // 2 - 1, here, :].astype(F32)
        low = query_low[here, :].astype(F32)
        scale = lax.rsqrt(jnp.mean(low * low, axis=-1, keepdims=True) + NORM_FLOOR)
        qga[x, here, :] = (
            scale * hat_grad
            - scale * scale * scale * low * jnp.mean(low * hat_grad, axis=-1, keepdims=True)
        ).astype(BF16)

    def t_copies(hop, d):
        source = x if hop == 1 else (xs[XN - 1] if d == 0 else xs[1])
        ref = qga.at[source] if hop == 1 else qga.at[source, half_rows[d]]
        copies = [remote(ref, ref, "tgs", (hop - 1, d), tp_id=x_to[d])]
        if hop == 1 or d == 0:
            copies.append(
                remote(gga.at[source], gga.at[source], "ggs", (hop - 1, d), tp_id=x_to[d])
            )
        return copies

    for d in range(2):
        for copy in t_copies(1, d):
            go(copy)
    weight_rows(2)
    finish_out(1)
    finish_rows(3)
    x_send(3)

    weight_rows(half - 1)
    wc_copy = remote(wbuf.at[other], wc_r, "wcs", (0,), st_id=partner)
    go(wc_copy)
    x_forward(2)
    wc_copy.wait_recv()
    for yi in range(YN):
        w1[yi] = (wbuf[c, yi].astype(F32) + wc_r[yi].astype(F32)).astype(BF16)

    def wy_copy(d):
        return remote(w1.at[ys[d]], wy_r.at[d], "wys", (0,), st_id=at(z, ys[d], c))

    def wz_copy(d):
        return remote(w2.at[zs[d]], wz_r.at[d], "wzs", (0,), st_id=at(zs[d], y, c))

    for d in (2, 1, 3):
        go(wy_copy(d))
    for d in range(2):
        for copy in t_copies(1, d):
            copy.wait_recv()
        for copy in t_copies(2, d):
            go(copy)
    x_forward(3)
    all_of(wy_r.at[pl.ds(1, YN - 1)], "wys", (0,)).wait_recv()
    gathered = w1[y].astype(F32)
    for d in range(1, YN):
        gathered += wy_r[d].astype(F32)
    w2[...] = gathered.astype(BF16)
    for d in (4, 3, 5, 2, 6, 1, 7):
        go(wz_copy(d))
    finish_out(2)
    for d in range(2):
        for copy in t_copies(2, d):
            copy.wait_recv()
    gate_rows = jnp.concatenate([gga[i, 0:1, :] for i in range(XN)] + [jnp.zeros((4, tok_n), F32)])
    gate_cols = jnp.concatenate([gw_all[i, 0:1, :] for i in range(XN)] + [jnp.zeros((4, width), F32)])
    for k in range(tok_n // ROW):
        here = pl.ds(k * ROW, ROW)
        value = exact_dot(gate_rows[:, k * ROW : (k + 1) * ROW], gate_cols, CONTRACT_FIRST)
        for i in range(XN):
            value += low_dot(qga[i, here, :], weight_of(i, 2), CONTRACT_LAST)
        tok_out[here, :] = value.astype(tok_out.dtype)
        leave(1, tok_out.at[here, :], r["tok_out"].at[here, :])
    all_of(wz_r.at[pl.ds(1, ZN - 1)], "wzs", (0,)).wait_recv()
    weight = w2[z].astype(F32)
    for d in range(1, ZN):
        weight += wz_r[d].astype(F32)
    weight_ref[...] = weight
    leave(2, weight_ref, r["weight_ref"])
    finish_out(3)
    moved = dict(
        id0=(id_refs[0], "idsem"),
        id1=(id_refs[1], "idsem"),
        tokx=(tok4.at[pl.ds(0, XN - 1)], "tokx"),
        cotz=(qg.at[pl.ds(0, ZN - 1)], "cotz"),
        qz=(qg.at[pl.ds(0, ZN - 1)], "qz"),
        gz=(gates.at[pl.ds(0, ZN - 1)], "gz"),
        kvy=(kv.at[pl.ds(0, 3 * passes)], "kvy"),
        kvd=(kv.at[pl.ds(0, YN * passes)], "kvd"),
        zts=(zt_r.at[pl.ds(1, ZN - 1)], "zts"),
        ters=(term_r, "ters"),
        zrs=(qg.at[pl.ds(0, ZN - 1)], "zrs"),
        yfs=(yf_s, "yfs"),
        yds=(yd_s, "yds"),
        xrs=(kgv.at[pl.ds(0, 3)], "xrs"),
        tgs=(qga.at[pl.ds(0, 3)], "tgs"),
        ggs=(gga.at[pl.ds(0, 3)], "ggs"),
        wxs=(w_all.at[pl.ds(0, XN - 1), 0], "wxs"),
        wxd=(w_all.at[pl.ds(0, XN - 1), 0], "wxd"),
        gws=(gw_all.at[pl.ds(0, XN - 1)], "gws"),
        wcs=(wc_r, "wcs"),
        wys=(wy_r.at[pl.ds(1, YN - 1)], "wys"),
        wzs=(wz_r.at[pl.ds(1, ZN - 1)], "wzs"),
    )
    for group, (ref, sem) in moved.items():
        index = (0,) * len(r[sem].shape)
        all_of(ref, sem, index, group).wait_send()
    for index, (src, dst) in enumerate(
        ((out_ref, "out_ref"), (tok_out, "tok_out"), (weight_ref, "weight_ref"))
    ):
        pltpu.make_async_copy(src, r[dst], r["outs"].at[index]).wait()


def fused_call(rate, ids, gate_w, beta, decay, tok, cot, mq, mk, mv, qw, kw, vw, rows):
    tok_n, width = tok.shape
    rows_n, model = rows.shape
    head = kw.shape[1]
    heads_n = beta.shape[0]
    vmem, sems = scratch_spec(tok_n, rows_n, width, head, heads_n, head // heads_n)
    part = model // (ZN * YN * CN)
    ins = ["rate", "ids", "gate_w", "beta", "decay"]
    ins += ["tok_h", "cot_h", "mq_h", "mk_h", "mv_h", "qw_h", "kw_h", "vw_h", "rows_h"]
    names = ins + ["tok_out", "out_ref", "weight_ref"] + list(vmem) + ["tab_s"] + list(sems)
    return pl.pallas_call(
        functools.partial(fused_kernel, names),
        out_shape=(
            jax.ShapeDtypeStruct((tok_n, width), BF16),
            jax.ShapeDtypeStruct((rows_n, width), BF16),
            jax.ShapeDtypeStruct((part, head), F32),
        ),
        in_specs=[SMEM_SPEC] * 2 + [VMEM_SPEC] * 3 + [ANY_SPEC] * 9,
        out_specs=(ANY_SPEC,) * 3,
        scratch_shapes=[pltpu.VMEM(*v) for v in vmem.values()]
        + [pltpu.SMEM((2, CN * ZN, 128), jnp.int32)]
        + [DMA(s) for s in sems.values()],
        compiler_params=pltpu.CompilerParams(
            collective_id=0, has_side_effects=True, vmem_limit_bytes=67043328
        ),
        name="fused",
    )(rate, ids, gate_w, beta, decay, tok, cot, mq, mk, mv, qw, kw, vw, rows)


def body(
    tokens,
    cotangent,
    mix_query,
    mix_key,
    mix_value,
    beta_pre,
    decay_pre,
    decay_rate,
    passages,
    passage_ids,
    query_weight,
    key_weight,
    value_weight,
    gate_weight,
):
    pass_local, span_rows, model_width = passages.shape
    flat_rows = passages.reshape(pass_local * span_rows, model_width)
    token_grad, passage_grad, key_weight_grad = fused_call(
        decay_rate,
        passage_ids.T,
        gate_weight,
        beta_pre,
        decay_pre,
        tokens,
        cotangent,
        mix_query,
        mix_key,
        mix_value,
        query_weight,
        key_weight,
        value_weight,
        flat_rows,
    )
    token_grad, passage_grad, key_weight_grad = settle_call(
        token_grad, passage_grad, key_weight_grad
    )
    return (token_grad, passage_grad.reshape(pass_local, span_rows, -1), key_weight_grad)


def solution(mesh):
    placed = (
        P("st", "tp"),
        P("st", "tp"),
        P("st", "tp"),
        P("st", "tp"),
        P("st", "tp"),
        P("tp", "st"),
        P("tp", "st"),
        P("tp"),
        P("st", None, None),
        P("st", None),
        P(None, "tp"),
        P(None, "tp"),
        P(None, "tp"),
        P("tp", None),
    )
    return jax.shard_map(
        body,
        mesh=mesh,
        in_specs=placed,
        out_specs=(P("st", "tp"), P("st", None, "tp"), P("st", "tp")),
        check_vma=False,
    )
```

```python
import functools

import jax
import jax.numpy as jnp
from jax import lax
from jax.experimental import pallas as pl
from jax.experimental.pallas import tpu as pltpu
from jax.sharding import PartitionSpec as P

SPAN = 64
BLOCK = 64
NORM_FLOOR = 1.0
SCORE_GAIN = 4.0
HIGHEST = lax.Precision.HIGHEST
CONTRACT_LAST = (((1,), (1,)), ((), ()))
CONTRACT_FIRST = (((0,), (0,)), ((), ()))
F32, BF16 = jnp.float32, jnp.bfloat16

MESH = pl.DeviceIdType.MESH
VMEM_SPEC = pl.BlockSpec(memory_space=pltpu.VMEM)
ANY_SPEC = pl.BlockSpec(memory_space=pl.ANY)
SMEM_SPEC = pl.BlockSpec(memory_space=pltpu.SMEM)
DMA = pltpu.SemaphoreType.DMA

ZN, YN, CN, XN = 8, 4, 2, 4
ROW = 128
SENDS = ("id0", "id1", "tokx", "cotz", "qz", "gz", "kvy", "kvd", "zts", "ters", "zrs", "yfs")
SENDS += ("yds", "xrs", "tgs", "ggs", "wxs", "wxd", "gws", "wcs", "wys", "wzs")


def settle_kernel(*refs):
    count = (len(refs) - 1) // 3
    sources, targets, buffers, sems = refs[:count], refs[count : 2 * count], refs[2 * count : -1], refs[-1]
    moves = []
    for source, target, buffer in zip(sources, targets, buffers):
        pieces = 4 if source.shape[0] >= 512 else 1
        rows = source.shape[0] // pieces
        for k in range(pieces):
            here = pl.ds(k * rows, rows)
            n = len(moves)
            moves.append(
                (
                    pltpu.make_async_copy(source.at[here, :], buffer.at[here, :], sems.at[0, n]),
                    pltpu.make_async_copy(buffer.at[here, :], target.at[here, :], sems.at[1, n]),
                )
            )
    for inward, _ in moves:
        inward.start()
    for inward, outward in moves:
        inward.wait()
        outward.start()
    for _, outward in moves:
        outward.wait()


def settle_call(*arrays):
    return pl.pallas_call(
        settle_kernel,
        out_shape=tuple(jax.ShapeDtypeStruct(x.shape, x.dtype) for x in arrays),
        in_specs=[ANY_SPEC] * len(arrays),
        out_specs=(ANY_SPEC,) * len(arrays),
        scratch_shapes=[pltpu.VMEM(x.shape, x.dtype) for x in arrays] + [DMA((2, 6))],
        name="settle",
    )(*arrays)


def exact_dot(left, right, dims=(((1,), (0,)), ((), ()))):
    return lax.dot_general(left, right, dims, precision=HIGHEST, preferred_element_type=F32)


def low_dot(left, right, dims=(((1,), (0,)), ((), ()))):
    return lax.dot_general(left, right, dims, preferred_element_type=F32)


def mixer_span(queries, keys_in, values_in, strength, log_decay, state):
    span = queries.shape[0]
    row_at = lax.broadcasted_iota(jnp.int32, (span, span), 0)
    col_at = lax.broadcasted_iota(jnp.int32, (span, span), 1)
    inclusive = row_at >= col_at
    unit_eye = jnp.where(row_at == col_at, 1.0, 0.0)
    decay_row = jnp.sum(unit_eye * log_decay, axis=0, keepdims=True)
    cum_row = jnp.sum(jnp.where(row_at <= col_at, log_decay, 0.0), axis=0, keepdims=True)
    cum_col = jnp.sum(jnp.where(inclusive, decay_row, 0.0), axis=1, keepdims=True)
    total = jnp.sum(log_decay, axis=0, keepdims=True)
    decay_map = jnp.exp(jnp.where(inclusive, cum_col - cum_row, -1e30))
    queries = (
        queries
        * lax.rsqrt(jnp.sum(queries * queries, axis=-1, keepdims=True) + NORM_FLOOR)
        * queries.shape[-1] ** (-0.5)
    )
    keys_in = keys_in * lax.rsqrt(jnp.sum(keys_in * keys_in, axis=-1, keepdims=True) + NORM_FLOOR)
    power = jnp.where(
        row_at > col_at, strength * exact_dot(keys_in, keys_in, CONTRACT_LAST) * decay_map, 0.0
    )
    inverse = unit_eye - power
    for _ in range(span.bit_length() - 2):
        power = exact_dot(power, power)
        inverse = exact_dot(inverse, unit_eye + power)
    attend = exact_dot(queries, keys_in, CONTRACT_LAST) * decay_map
    fresh = exact_dot(inverse, values_in * strength)
    correction = exact_dot(inverse, keys_in * (strength * jnp.exp(cum_col)))
    new_values = fresh - exact_dot(correction, state)
    output = exact_dot(queries * jnp.exp(cum_col), state) + exact_dot(attend, new_values)
    state = state * jnp.exp(total) + exact_dot(
        keys_in * jnp.exp(total - cum_col), new_values, CONTRACT_FIRST
    )
    return output, state


def scratch_spec(tok_n, rows_n, width, head, heads_n, mix_dim):
    model = width * XN
    slab = YN * CN
    passes = rows_n // BLOCK
    chunks = rows_n // ROW
    half = chunks // 2
    part = model // (ZN * slab)
    keys = slab * BLOCK
    vmem = dict(
        rows_v=((rows_n, model), BF16),
        kw=((model, head), BF16),
        vw=((model, head), BF16),
        qw=((model, head), BF16),
        tok4=((XN, tok_n, width), BF16),
        kv=((slab * passes, BLOCK, 2 * head), BF16),
        qc=((ZN, 2, tok_n, head), BF16),
        gates=((ZN, 8, tok_n), F32),
        mq=((tok_n, head), BF16),
        mk=((tok_n, head), BF16),
        mv=((tok_n, head), BF16),
        ids_all=((CN, ZN, 8, 128), jnp.int32),
        tab_v=((2, CN * ZN, 128), jnp.int32),
        ids_v=((8, 128), jnp.int32),
        code=((YN, CN, 8, ZN * BLOCK), jnp.int32),
        turned=((tok_n, 8), F32),
        mixed=((tok_n, head), F32),
        states=((heads_n, mix_dim, mix_dim), F32),
        key_low=((rows_n, head), BF16),
        query_low=((tok_n, head), BF16),
        kvr=((keys, 2 * head), BF16),
        e_buf=((ZN, keys, tok_n), F32),
        g_buf=((keys, tok_n), F32),
        sg=((keys, tok_n), BF16),
        pg=((keys, tok_n), BF16),
        zt=((ZN, 2, tok_n), F32),
        zt_r=((ZN, ZN, 2, tok_n), F32),
        terms=((CN, ZN, YN, BLOCK, 2 * head), BF16),
        term_r=((ZN, YN, BLOCK, 2 * head), BF16),
        qg=((ZN, tok_n, head), BF16),
        z_s=((2, ZN // 2 - 1, tok_n, head), BF16),
        z_r=((2, ZN // 2, tok_n, head), BF16),
        yf_s=((2, half, ROW, 2 * head), BF16),
        yf_r=((2, half, ROW, 2 * head), BF16),
        yd_s=((2, chunks, ROW, 2 * head), BF16),
        yd_r=((2, chunks, ROW, 2 * head), BF16),
        kgv=((XN, rows_n, 2 * head), BF16),
        qga=((XN, tok_n, head), BF16),
        gga=((XN, 8, tok_n), F32),
        w_all=((XN, CN, 3, width // CN, head), BF16),
        gwb=((8, model), F32),
        gw_all=((XN, 8, width), F32),
        wbuf=((CN, YN, ZN, part, head), BF16),
        wc_r=((YN, ZN, part, head), BF16),
        w1=((YN, ZN, part, head), BF16),
        wy_r=((YN, ZN, part, head), BF16),
        w2=((ZN, part, head), BF16),
        wz_r=((ZN, part, head), BF16),
        tok_v=((tok_n, width), BF16),
        out_v=((rows_n, width), BF16),
        weight_v=((part, head), F32),
        w_acc=((model, head), F32),
        out_part=((2, 2, ROW, width), F32),
        tok_part=((tok_n, width), F32),
    )
    sems = dict(
        load=(16,),
        outs=(3,),
        send=(len(SENDS),),
        idsem=(CN,),
        tokx=(2, 2, 2),
        cotz=(ZN // 2, 2),
        qz=(ZN // 2, 2, 2),
        gz=(ZN // 2, 2),
        kvy=(2, 2, 4),
        kvd=(1,),
        zts=(ZN,),
        ters=(1,),
        zrs=(2, ZN // 2),
        yfs=(2, half),
        yds=(chunks,),
        xrs=(3, chunks),
        tgs=(2, 2),
        ggs=(2, 2),
        wxs=(1,),
        wxd=(1,),
        gws=(1,),
        wcs=(1,),
        wys=(1,),
        wzs=(1,),
    )
    return vmem, sems


def fused_kernel(names, *refs):
    r = dict(zip(names, refs))

    def get(*keys):
        return [r[k] for k in keys]

    rate, ids, gate_w, beta, decay = get("rate", "ids", "gate_w", "beta", "decay")
    tok_out, out_ref, weight_ref = get("tok_v", "out_v", "weight_v")
    rows_v, kw, vw, qw, tok4, kv, qc, gates = get(
        "rows_v", "kw", "vw", "qw", "tok4", "kv", "qc", "gates"
    )
    tab_v, tab_s, code = get("tab_v", "tab_s", "code")
    kvr, e_buf, g_buf, sg, pg, zt, zt_r = get("kvr", "e_buf", "g_buf", "sg", "pg", "zt", "zt_r")
    terms, term_r, qg, z_s, z_r = get("terms", "term_r", "qg", "z_s", "z_r")
    key_low, query_low = get("key_low", "query_low")
    kgv, qga, gga, w_all, gwb, gw_all = get("kgv", "qga", "gga", "w_all", "gwb", "gw_all")
    turned, mixed, states = get("turned", "mixed", "states")

    rows_n, model = rows_v.shape
    head = kw.shape[1]
    tok_n, width = tok_out.shape
    heads_n = beta.shape[0]
    mix_dim = head // heads_n
    slab = YN * CN
    passes = rows_n // BLOCK
    chunks = rows_n // ROW
    half = chunks // 2
    per_dev = tok_n // BLOCK
    score_scale = SCORE_GAIN * head ** (-0.5)

    st = lax.axis_index("st")
    x = lax.axis_index("tp")
    c = lax.rem(st, CN)
    y = lax.rem(st // CN, YN)
    z = st // slab
    other = 1 - c

    def at(zi, yi, ci):
        return (zi * YN + yi) * CN + ci

    def step(value, by, n):
        return lax.rem(value + (by % n), n)

    xs = [step(x, i, XN) for i in range(XN)]
    ys = [step(y, i, YN) for i in range(YN)]
    zs = [step(z, i, ZN) for i in range(ZN)]
    partner = at(z, y, other)
    x_to = (xs[1], xs[XN - 1])
    y_to = (at(z, ys[1], c), at(z, ys[YN - 1], c))
    z_to = (at(zs[1], y, c), at(zs[ZN - 1], y, c))

    def remote(src, dst, sem, index, st_id=None, tp_id=None, group=None):
        device = {}
        if st_id is not None:
            device["st"] = st_id
        if tp_id is not None:
            device["tp"] = tp_id
        return pltpu.make_async_remote_copy(
            src_ref=src,
            dst_ref=dst,
            send_sem=r["send"].at[SENDS.index(group or sem)],
            recv_sem=r[sem].at[index],
            device_id=device,
            device_id_type=MESH,
        )

    def go(copy):
        copy.start()

    def all_of(ref, sem, index, group=None):
        return remote(ref, ref, sem, index, st_id=partner, group=group)

    def leave(index, src, dst):
        pltpu.make_async_copy(src, dst, r["outs"].at[index]).start()

    loads = {}

    def load(key, src, dst):
        loads[key] = pltpu.make_async_copy(src, dst, r["load"].at[len(loads)])
        loads[key].start()

    load("cot", r["cot_h"], qc.at[z, 1])
    load("tok", r["tok_h"], tok4.at[x])
    load("kw", r["kw_h"], kw)
    load("vw", r["vw_h"], vw)
    proj_rows = rows_n // 4
    proj_order = (0, 2, 1, 3)
    for k in proj_order:
        here = pl.ds(k * proj_rows, proj_rows)
        load(("rows", k), r["rows_h"].at[here, :], rows_v.at[here, :])
    load("mq", r["mq_h"], r["mq"])
    load("mk", r["mk_h"], r["mk"])
    load("mv", r["mv_h"], r["mv"])
    load("qw", r["qw_h"], qw)

    id_lane = lax.broadcasted_iota(jnp.int32, (8, 128), 1)
    id_row = jnp.zeros((8, 128), jnp.int32)
    per_block, blocks_n = ids.shape
    for b in range(blocks_n):
        for k in range(per_block):
            id_row = jnp.where(id_lane == b * per_block + k, ids[k, b], id_row)
    r["ids_v"][...] = id_row

    barrier = pltpu.get_barrier_semaphore()
    greeted = 0
    for target in xs[1:]:
        pl.semaphore_signal(barrier, inc=1, device_id={"tp": target}, device_id_type=MESH)
        greeted += 1
    friends = [partner] + [at(z, ys[d], c) for d in range(1, YN)]
    friends += [at(zs[d], y, ci) for d in range(1, ZN) for ci in (c, other)]
    for target in friends:
        pl.semaphore_signal(barrier, inc=1, device_id={"st": target}, device_id_type=MESH)
        greeted += 1
    pl.semaphore_wait(barrier, greeted)

    t_half = tok_n // 2
    half_rows = (pl.ds(0, t_half), pl.ds(t_half, t_half))

    def cot_copy(hop, d):
        source = zs[(1 - hop) % ZN] if d == 0 else zs[(hop - 1) % ZN]
        ref = qc.at[source, 1]
        if hop == ZN // 2:
            ref = qc.at[source, 1, half_rows[d]]
        return remote(ref, ref, "cotz", (hop - 1, d), st_id=z_to[d])

    def q_copies(hop, d, h):
        source = zs[(1 - hop) % ZN] if d == 0 else zs[(hop - 1) % ZN]
        if hop == ZN // 2 and h != d:
            return []
        ref = qc.at[source, 0, half_rows[h]]
        copies = [remote(ref, ref, "qz", (hop - 1, d, h), st_id=z_to[d])]
        if h == d and (hop < ZN // 2 or d == 0):
            copies.append(
                remote(gates.at[source], gates.at[source], "gz", (hop - 1, d), st_id=z_to[d])
            )
        return copies

    def tok_copy(hop, d, h):
        source = x if hop == 1 else (xs[XN - 1] if d == 0 else xs[1])
        ref = tok4.at[source, half_rows[h]]
        return remote(ref, ref, "tokx", (hop - 1, d, h), tp_id=x_to[d])

    def ids_copy(dc, dz):
        return remote(
            r["ids_v"],
            r["ids_all"].at[c, z],
            "idsem",
            (dc,),
            st_id=at(zs[dz], y, other if dc else c),
            group="id1" if dc else "id0",
        )

    id_peers = [(dc, dz) for dz in range(ZN) for dc in range(CN) if (dc, dz) != (0, 0)]
    for dc, dz in id_peers:
        go(ids_copy(dc, dz))
    r["ids_all"][c, z] = id_row
    loads["tok"].wait()
    for d in range(2):
        go(tok_copy(1, d, d))
    for d in range(2):
        go(tok_copy(1, d, 1 - d))
    loads["cot"].wait()
    for d in range(2):
        go(cot_copy(1, d))

    per_chunk = proj_rows // BLOCK

    def kv_piece(yi, ci, k):
        return kv.at[pl.ds((yi * CN + ci) * passes + k * per_chunk, per_chunk)]

    def kv_copy(hop, d, k):
        yi = y if hop == 1 else (ys[YN - 1] if d == 0 else ys[1])
        ref = kv_piece(yi, c, k)
        return remote(ref, ref, "kvy", (hop - 1, d, k), st_id=y_to[d])

    def kv_across(rel, k):
        ref = kv_piece(ys[rel], c, k)
        return remote(ref, ref, "kvd", (0,), st_id=partner)

    loads["kw"].wait()
    loads["vw"].wait()
    for k in proj_order:
        loads[("rows", k)].wait()
        here = pl.ds(k * proj_rows, proj_rows)
        block = rows_v[here, :]
        low = low_dot(block, kw[...]).astype(BF16)
        key_low[here, :] = low
        low = low.astype(F32)
        scale = lax.rsqrt(jnp.mean(low * low, axis=-1, keepdims=True) + NORM_FLOOR)
        first = (y * CN + c) * passes + k * per_chunk
        kv[pl.ds(first, per_chunk), :, :head] = (
            (low * scale).astype(BF16).reshape(per_chunk, BLOCK, head)
        )
        kv[pl.ds(first, per_chunk), :, head:] = (
            low_dot(block, vw[...]).astype(BF16).reshape(per_chunk, BLOCK, head)
        )
        for d in range(2):
            go(kv_copy(1, d, k))
        go(kv_across(0, k))

    gwb[...] = jnp.broadcast_to(gate_w[...].astype(F32), gwb.shape)
    turned[...] = jnp.transpose(
        jnp.concatenate(
            [beta[...], decay[...], jnp.zeros((8 - 2 * heads_n, tok_n), F32)], axis=0
        )
    )
    states[...] = jnp.zeros_like(states)
    for key in ("mq", "mk", "mv", "qw"):
        loads[key].wait()

    def mix(b):
        here = pl.ds(pl.multiple_of(b * SPAN, SPAN), SPAN)
        for m in range(heads_n):
            cols = pl.ds(m * mix_dim, mix_dim)
            raw = turned[here, heads_n + m : heads_n + m + 1]
            softplus = jnp.maximum(raw, 0.0) + jnp.log1p(jnp.exp(-jnp.abs(raw)))
            mixed[here, cols], states[m] = mixer_span(
                r["mq"][here, cols].astype(F32),
                r["mk"][here, cols].astype(F32),
                r["mv"][here, cols].astype(F32),
                jax.nn.sigmoid(turned[here, m : m + 1]),
                -rate[m] * softplus,
                states[m],
            )

    spans_n = tok_n // SPAN

    def cot_pass(hop):
        for d in range(2):
            cot_copy(hop - 1, d).wait_recv()
            go(cot_copy(hop, d))

    def q_pass(hop, first):
        for d in range(2):
            h = d if first else 1 - d
            for copy in q_copies(hop - 1, d, h):
                copy.wait_recv()
            for copy in q_copies(hop, d, h):
                go(copy)

    def kv_pass(k):
        for d, rel in ((0, YN - 1), (1, 1)):
            kv_copy(1, d, k).wait_recv()
            if (k < 2) == (d == 0):
                go(kv_copy(2, d, k))
            go(kv_across(rel, k))

    w_half = width // CN

    def w_copy(w, d):
        rows = pl.ds(pl.multiple_of(xs[d] * width + c * w_half, w_half), w_half)
        return remote(
            (kw, vw, qw)[w].at[rows, :], w_all.at[x, c, w], "wxs", (0,), tp_id=xs[d]
        )

    def w_across(d):
        ref = w_all.at[xs[XN - d], c]
        return remote(ref, ref, "wxd", (0,), st_id=partner)

    def gw_copy(d):
        cols = pl.ds(pl.multiple_of(xs[d] * width, width), width)
        return remote(gwb.at[:, cols], gw_all.at[x], "gws", (0,), tp_id=xs[d])

    pl.loop(0, 1)(mix)
    cot_pass(2)
    for d in range(2):
        tok_copy(1, d, d).wait_recv()
        go(tok_copy(2, d, d))
    pl.loop(1, 3)(mix)
    cot_pass(3)
    kv_pass(0)
    for d in range(2):
        tok_copy(1, d, 1 - d).wait_recv()
        tok_copy(2, d, d).wait_recv()

    gate_rows = jnp.broadcast_to(gate_w[...], (16, model))
    logit = low_dot(gate_rows[:, :width], tok4[0], CONTRACT_LAST)
    for i in range(1, XN):
        logit += low_dot(gate_rows[:, i * width : (i + 1) * width], tok4[i], CONTRACT_LAST)
    gates[z] = jax.nn.sigmoid(logit[:8])

    @pl.loop(0, tok_n // ROW)
    def _(k):
        here = pl.ds(pl.multiple_of(k * ROW, ROW), ROW)
        low = low_dot(tok4[0, here, :], qw[pl.ds(0, width), :])
        for i in range(1, XN):
            low += low_dot(tok4[i, here, :], qw[pl.ds(i * width, width), :])
        low = low.astype(BF16)
        query_low[here, :] = low
        low = low.astype(F32)
        scale = lax.rsqrt(jnp.mean(low * low, axis=-1, keepdims=True) + NORM_FLOOR)
        qc[z, 0, here, :] = (low * scale).astype(BF16)

    for h in range(2):
        for d in range(2):
            for copy in q_copies(1, d, d if h == 0 else 1 - d):
                go(copy)
    for d in range(1, XN):
        for w in range(3):
            go(w_copy(w, d))
        go(gw_copy(d))
    for w, ref in enumerate((kw, vw, qw)):
        for h in range(CN):
            w_all[x, h, w] = ref[pl.ds(pl.multiple_of(x * width + h * w_half, w_half), w_half), :]
    gw_all[x] = gwb[:, pl.ds(pl.multiple_of(x * width, width), width)]
    pl.loop(3, 4)(mix)
    kv_pass(2)
    q_pass(2, True)
    kv_pass(1)
    cot_pass(4)
    id_refs = (r["ids_all"].at[0, pl.ds(0, ZN - 1)], r["ids_all"].at[1])
    for dc in range(CN):
        all_of(id_refs[dc], "idsem", (dc,), f"id{dc}").wait_recv()
    every = jnp.concatenate(
        [r["ids_all"][ci, zi, 0:1, :] for ci in range(CN) for zi in range(ZN)], axis=0
    )
    lane = lax.broadcasted_iota(jnp.int32, (CN * ZN, 128), 1)
    loc_tab = jnp.zeros((CN * ZN, 128), jnp.int32)
    blk_tab = jnp.zeros((CN * ZN, 128), jnp.int32)
    owner = lax.shift_right_logical(every, 4)
    local = every & (passes - 1)
    for o in range(slab):
        match = (owner == z * slab + o) & (lane < per_dev * 4)
        loc = jnp.sum(jnp.where(match, local, 0), axis=1, keepdims=True)
        blk = jnp.sum(
            jnp.where(match, lax.shift_right_logical(lane, 2) + 1, 0), axis=1, keepdims=True
        )
        loc_tab = jnp.where(lane == o, jnp.minimum(loc, passes - 1), loc_tab)
        blk_tab = jnp.where(lane == o, blk - 1, blk_tab)
    tab_v[0] = loc_tab
    tab_v[1] = blk_tab
    tab_copy = pltpu.make_async_copy(tab_v, tab_s, r["load"].at[len(loads)])
    tab_copy.start()
    q_pass(2, False)
    kv_pass(3)
    q_pass(3, True)
    q_pass(3, False)
    q_pass(4, True)
    tab_copy.wait()
    lane_of = lax.broadcasted_iota(jnp.int32, (8, ZN * BLOCK), 1)
    for yi in range(YN):
        for which, ci in ((0, c), (1, other)):
            start = jnp.full((8, ZN * BLOCK), -1000000, jnp.int32)
            for zi in range(ZN):
                row = ci * ZN + zi
                base = jnp.where(
                    tab_s[1, row, yi * CN + c] >= 0,
                    tab_s[0, row, yi * CN + c] * BLOCK,
                    -1000000,
                )
                start = jnp.where(lax.shift_right_logical(lane_of, 6) == zi, base, start)
            code[yi, which] = start + (lane_of & (BLOCK - 1))
    for d, k in ((0, 0), (1, 2), (0, 1), (1, 3)):
        kv_copy(2, d, k).wait_recv()
        go(kv_across(2, k))
    for d in range(2):
        cot_copy(ZN // 2, d).wait_recv()
        for copy in q_copies(ZN // 2 - 1, d, 1 - d) + q_copies(ZN // 2, d, d):
            copy.wait_recv()
    kv_across_all = all_of(kv.at[pl.ds(0, YN * passes)], "kvd", (0,))
    kv_across_all.wait_recv()

    tok_block = lax.shift_right_logical(lax.broadcasted_iota(jnp.int32, (BLOCK, tok_n), 1), 6)
    key_halves = [pl.ds(i * ROW * 2, ROW * 2) for i in range(slab * BLOCK // (2 * ROW))]

    def gather(reader):
        for o in range(slab):
            local_at = jnp.clip(tab_s[0, c * ZN + reader, o], 0, passes - 1)
            kvr[pl.ds(o * BLOCK, BLOCK), :] = kv[o * passes + local_at]

    def zt_copy(d, reader):
        return remote(
            zt.at[reader], zt_r.at[d, reader], "zts", (reader,), st_id=at(zs[d], y, c)
        )

    @pl.loop(0, ZN)
    def _(reader):
        gather(reader)
        for part in key_halves:
            e_buf[reader, part, :] = low_dot(kvr[part, :head], qc[reader, 0], CONTRACT_LAST)
            g_buf[part, :] = low_dot(kvr[part, head:], qc[reader, 1], CONTRACT_LAST)
        total = jnp.zeros((1, tok_n), F32)
        product = jnp.zeros((1, tok_n), F32)
        for o in range(slab):
            here = pl.ds(o * BLOCK, BLOCK)
            mine = tok_block == tab_s[1, c * ZN + reader, o]
            e = jnp.where(mine, jnp.exp(e_buf[reader, here, :] * score_scale), 0.0)
            e_buf[reader, here, :] = e
            total += jnp.sum(e, axis=0, keepdims=True)
            product += jnp.sum(e * g_buf[here, :], axis=0, keepdims=True)
        zt[reader, 0:1, :] = total
        zt[reader, 1:2, :] = product * gates[reader, 0:1, :]
        for d in (4, 3, 5, 2, 6, 1, 7):
            zt_copy(d, reader).start()

    def summed(reader):
        both = zt[reader]
        for d in range(1, ZN):
            both += zt_r[d, reader]
        return both[0:1, :], both[1:2, :]

    def term_copy(reader):
        return remote(
            terms.at[other, reader], term_r.at[reader], "ters", (0,), st_id=partner
        )

    @pl.loop(0, ZN)
    def _(reader):
        all_of(zt_r.at[pl.ds(1, ZN - 1), reader], "zts", (reader,)).wait_recv()
        total, product = summed(reader)
        inverse = 1.0 / total
        mean = product * inverse
        gate = gates[reader, 0:1, :]
        gather(reader)
        for part in key_halves:
            g_buf[part, :] = low_dot(kvr[part, head:], qc[reader, 1], CONTRACT_LAST)
        for o in range(slab):
            here = pl.ds(o * BLOCK, BLOCK)
            probs = e_buf[reader, here, :] * inverse
            sg[here, :] = (probs * (g_buf[here, :] * gate - mean)).astype(BF16)
            pg[here, :] = (probs * gate).astype(BF16)
        for n, part in enumerate(key_halves):
            key_term = (low_dot(sg[part, :], qc[reader, 0]) * score_scale).astype(BF16)
            value_term = low_dot(pg[part, :], qc[reader, 1]).astype(BF16)
            for k in range(2 * ROW // BLOCK):
                o = n * (2 * ROW // BLOCK) + k
                piece = slice(k * BLOCK, (k + 1) * BLOCK)
                terms[o % CN, reader, o // CN, :, :head] = key_term[piece]
                terms[o % CN, reader, o // CN, :, head:] = value_term[piece]
        term_copy(reader).start()
        qg[reader] = (low_dot(sg[...], kvr[:, :head], CONTRACT_FIRST) * score_scale).astype(BF16)

    def z_copy(hop, d):
        if hop == 1:
            src = qg.at[zs[ZN // 2], half_rows[d]]
            dst = z_r.at[d, 0, half_rows[d]]
        else:
            src = z_s.at[d, hop - 2]
            dst = z_r.at[d, hop - 1]
        return remote(src, dst, "zrs", (d, hop - 1), st_id=z_to[d])

    def z_pass(hop):
        for d in range(2):
            z_copy(hop - 1, d).wait_recv()
            away = ZN // 2 + 1 - hop
            target = zs[away] if d == 0 else zs[(-away) % ZN]
            if hop == 2:
                mid, rest = half_rows[d], half_rows[1 - d]
                z_s[d, hop - 2, mid, :] = (
                    qg[target, mid, :].astype(F32) + z_r[d, 0, mid, :].astype(F32)
                ).astype(BF16)
                z_s[d, hop - 2, rest, :] = qg[target, rest, :]
            else:
                z_s[d, hop - 2] = (
                    qg[target].astype(F32) + z_r[d, hop - 2].astype(F32)
                ).astype(BF16)
            go(z_copy(hop, d))

    for d in range(2):
        go(z_copy(1, d))

    row_iota = lax.broadcasted_iota(jnp.int32, (ROW, ZN * BLOCK), 0)

    def pick(rel, q):
        yi = ys[rel]
        rows = row_iota + q * ROW
        ones = [
            jnp.where(rows == code[yi, which, 0:1, :], 1.0, 0.0).astype(BF16) for which in range(2)
        ]
        return low_dot(ones[0], terms[c, :, yi].reshape(ZN * BLOCK, 2 * head)) + low_dot(
            ones[1], term_r[:, yi].reshape(ZN * BLOCK, 2 * head)
        )

    yf_s, yf_r, yd_s, yd_r = get("yf_s", "yf_r", "yd_s", "yd_r")

    def two_step(far_s, far_r, near_s, near_r, far_sem, near_sem, term):
        def far(d, j):
            return remote(far_s.at[d, j], far_r.at[d, j], far_sem, (d, j), st_id=y_to[d])

        def near(d, q):
            return remote(near_s.at[d, q], near_r.at[d, q], near_sem, (q,), st_id=y_to[d])

        def send(j):
            for d in range(2):
                q = j + half * d
                far_s[d, j] = term(2, q).astype(BF16)
                go(far(d, j))
            for d in range(2):
                q = j + half * (1 - d)
                near_s[d, q] = term(1 if d == 0 else 3, q).astype(BF16)
                go(near(d, q))

        def forward(j):
            for d in range(2):
                q = j + half * d
                value = term(1 if d == 0 else 3, q)
                far(d, j).wait_recv()
                near_s[d, q] = (value + far_r[d, j].astype(F32)).astype(BF16)
                go(near(d, q))

        def final(q):
            value = term(0, q)
            all_of(near_r.at[:, q], near_sem, (q,)).wait_recv()
            return value + near_r[0, q].astype(F32) + near_r[1, q].astype(F32)

        return send, forward, final

    y_send, y_forward, y_final = two_step(yf_s, yf_r, yd_s, yd_r, "yfs", "yds", pick)

    def x_copy(hop, d, q):
        source = x if hop == 1 else (xs[XN - 1] if d == 0 else xs[1])
        ref = kgv.at[source, pl.ds(q * ROW, ROW)]
        kind = 2 if hop == 2 else 0 if (q < half) == (d == 0) else 1
        return remote(ref, ref, "xrs", (kind, q), tp_id=x_to[d])

    def x_send(j):
        for q in (j, j + half):
            for d in range(2):
                go(x_copy(1, d, q))

    def x_forward(j):
        for d in range(2):
            q = j + half * d
            x_copy(1, d, q).wait_recv()
            go(x_copy(2, d, q))

    def weight_of(head_at, w):
        return w_all[head_at, :, w].reshape(width, head)

    def finish_rows(j):
        for q in (j, j + half):
            here = pl.ds(q * ROW, ROW)
            value = y_final(q)
            hat = value[:, :head]
            low = key_low[here, :].astype(F32)
            scale = lax.rsqrt(jnp.mean(low * low, axis=-1, keepdims=True) + NORM_FLOOR)
            grad = (
                scale * hat
                - scale * scale * scale * low * jnp.mean(low * hat, axis=-1, keepdims=True)
            ).astype(BF16)
            kgv[x, here, :head] = grad
            kgv[x, here, head:] = value[:, head:].astype(BF16)

    def rows_of(q, rels):
        here = pl.ds(q * ROW, ROW)
        value = jnp.zeros((ROW, width), F32)
        for rel in rels:
            i = xs[rel]
            value += low_dot(kgv[i, here, :head], weight_of(i, 0), CONTRACT_LAST)
            value += low_dot(kgv[i, here, head:], weight_of(i, 1), CONTRACT_LAST)
        return value

    near_heads, far_head = (0, 1, 3), (2,)
    out_part, tok_part = get("out_part", "tok_part")

    def near_out(j):
        for d in range(2):
            q = j + half * d
            x_copy(1, 1 - d, q).wait_recv()
            out_part[j - half + 2, d] = rows_of(q, near_heads)

    def far_out(j):
        for d in range(2):
            q = j + half * d
            here = pl.ds(q * ROW, ROW)
            x_copy(2, d, q).wait_recv()
            out_ref[here, :] = (out_part[j - half + 2, d] + rows_of(q, far_head)).astype(out_ref.dtype)
            leave(0, out_ref.at[here, :], r["out_ref"].at[here, :])

    def finish_out(j):
        for d in range(2):
            q = j + half * d
            here = pl.ds(q * ROW, ROW)
            x_copy(1, 1 - d, q).wait_recv()
            x_copy(2, d, q).wait_recv()
            out_ref[here, :] = rows_of(q, range(XN)).astype(out_ref.dtype)
            leave(0, out_ref.at[here, :], r["out_ref"].at[here, :])

    wbuf, wc_r, w1, wy_r, w2, wz_r = get("wbuf", "wc_r", "w1", "wy_r", "w2", "wz_r")
    w_acc = r["w_acc"]
    part = weight_ref.shape[0]

    def weight_rows(j):
        low, high = pl.ds(j * ROW, ROW), pl.ds((j + half) * ROW, ROW)
        grad = jnp.concatenate([kgv[x, low, :head], kgv[x, high, :head]], axis=0)

        @pl.loop(0, ZN)
        def _(k):
            cols = pl.ds(pl.multiple_of(k * slab * part, slab * part), slab * part)
            rows = jnp.concatenate([rows_v[low, cols], rows_v[high, cols]], axis=0)
            tile = low_dot(rows, grad, CONTRACT_FIRST)
            if j > 0:
                tile += w_acc[cols, :]
            if j < half - 1:
                w_acc[cols, :] = tile
            else:
                tile = tile.astype(BF16)
                for o in range(slab):
                    wbuf[o % CN, o // CN, k] = tile[o * part : (o + 1) * part]

    all_of(term_r, "ters", (0,)).wait_recv()

    y_send(0)
    pl.loop(4, 5)(mix)
    y_forward(0)
    y_send(1)
    z_pass(2)
    pl.loop(5, spans_n)(mix)
    finish_rows(0)
    x_send(0)
    y_forward(1)
    y_send(2)
    z_pass(3)
    all_of(w_all.at[pl.ds(0, XN - 1), 0], "wxs", (0,)).wait_recv()
    for d in range(1, XN):
        go(w_across(d))
    weight_rows(0)
    finish_rows(1)
    x_forward(0)
    x_send(1)
    z_pass(4)
    y_forward(2)
    y_send(3)
    weight_rows(1)
    all_of(w_all.at[pl.ds(0, XN - 1), 0], "wxd", (0,)).wait_recv()
    all_of(gw_all.at[pl.ds(0, XN - 1)], "gws", (0,)).wait_recv()
    finish_out(0)
    finish_rows(2)
    x_forward(1)
    x_send(2)
    y_forward(3)

    for d in range(2):
        z_copy(ZN // 2, d).wait_recv()
    total, product = summed(z)
    along = exact_dot(
        jnp.ones((8, head), F32), qc[z, 1].astype(F32) * mixed[...], CONTRACT_LAST
    )
    opened = gates[z]
    gga[x] = (1.0 - opened) * (product / total - opened * along)

    for k in range(tok_n // ROW):
        here = pl.ds(k * ROW, ROW)
        hat_grad = qg[z, here, :].astype(F32)
        for d in range(2):
            hat_grad += z_r[d, ZN // 2 - 1, here, :].astype(F32)
        low = query_low[here, :].astype(F32)
        scale = lax.rsqrt(jnp.mean(low * low, axis=-1, keepdims=True) + NORM_FLOOR)
        qga[x, here, :] = (
            scale * hat_grad
            - scale * scale * scale * low * jnp.mean(low * hat_grad, axis=-1, keepdims=True)
        ).astype(BF16)

    def t_copies(hop, d):
        source = x if hop == 1 else (xs[XN - 1] if d == 0 else xs[1])
        ref = qga.at[source] if hop == 1 else qga.at[source, half_rows[d]]
        copies = [remote(ref, ref, "tgs", (hop - 1, d), tp_id=x_to[d])]
        if hop == 1 or d == 0:
            copies.append(
                remote(gga.at[source], gga.at[source], "ggs", (hop - 1, d), tp_id=x_to[d])
            )
        return copies

    for d in range(2):
        for copy in t_copies(1, d):
            go(copy)
    weight_rows(2)
    finish_out(1)
    finish_rows(3)
    x_send(3)

    weight_rows(half - 1)
    wc_copy = remote(wbuf.at[other], wc_r, "wcs", (0,), st_id=partner)
    go(wc_copy)
    x_forward(2)
    wc_copy.wait_recv()
    for yi in range(YN):
        w1[yi] = (wbuf[c, yi].astype(F32) + wc_r[yi].astype(F32)).astype(BF16)

    def wy_copy(d):
        return remote(w1.at[ys[d]], wy_r.at[d], "wys", (0,), st_id=at(z, ys[d], c))

    def wz_copy(d):
        return remote(w2.at[zs[d]], wz_r.at[d], "wzs", (0,), st_id=at(zs[d], y, c))

    for d in (2, 1, 3):
        go(wy_copy(d))
    for d in range(2):
        for copy in t_copies(1, d):
            copy.wait_recv()
        for copy in t_copies(2, d):
            go(copy)
    for k in range(tok_n // ROW):
        here = pl.ds(k * ROW, ROW)
        value = jnp.zeros((ROW, width), F32)
        for rel in near_heads:
            value += low_dot(qga[xs[rel], here, :], weight_of(xs[rel], 2), CONTRACT_LAST)
        tok_part[here, :] = value
    near_out(2)
    x_forward(3)
    all_of(wy_r.at[pl.ds(1, YN - 1)], "wys", (0,)).wait_recv()
    gathered = w1[y].astype(F32)
    for d in range(1, YN):
        gathered += wy_r[d].astype(F32)
    w2[...] = gathered.astype(BF16)
    for d in (4, 3, 5, 2, 6, 1, 7):
        go(wz_copy(d))
    near_out(3)
    far_out(2)
    for d in range(2):
        for copy in t_copies(2, d):
            copy.wait_recv()
    gate_rows = jnp.concatenate([gga[i, 0:1, :] for i in range(XN)] + [jnp.zeros((4, tok_n), F32)])
    gate_cols = jnp.concatenate([gw_all[i, 0:1, :] for i in range(XN)] + [jnp.zeros((4, width), F32)])
    for k in range(tok_n // ROW):
        here = pl.ds(k * ROW, ROW)
        value = exact_dot(gate_rows[:, k * ROW : (k + 1) * ROW], gate_cols, CONTRACT_FIRST)
        value += tok_part[here, :] + low_dot(
            qga[xs[2], here, :], weight_of(xs[2], 2), CONTRACT_LAST
        )
        tok_out[here, :] = value.astype(tok_out.dtype)
        leave(1, tok_out.at[here, :], r["tok_out"].at[here, :])
    all_of(wz_r.at[pl.ds(1, ZN - 1)], "wzs", (0,)).wait_recv()
    weight = w2[z].astype(F32)
    for d in range(1, ZN):
        weight += wz_r[d].astype(F32)
    weight_ref[...] = weight
    leave(2, weight_ref, r["weight_ref"])
    far_out(3)
    moved = dict(
        id0=(id_refs[0], "idsem"),
        id1=(id_refs[1], "idsem"),
        tokx=(tok4.at[pl.ds(0, XN - 1)], "tokx"),
        cotz=(qg.at[pl.ds(0, ZN - 1)], "cotz"),
        qz=(qg.at[pl.ds(0, ZN - 1)], "qz"),
        gz=(gates.at[pl.ds(0, ZN - 1)], "gz"),
        kvy=(kv.at[pl.ds(0, 3 * passes)], "kvy"),
        kvd=(kv.at[pl.ds(0, YN * passes)], "kvd"),
        zts=(zt_r.at[pl.ds(1, ZN - 1)], "zts"),
        ters=(term_r, "ters"),
        zrs=(qg.at[pl.ds(0, ZN - 1)], "zrs"),
        yfs=(yf_s, "yfs"),
        yds=(yd_s, "yds"),
        xrs=(kgv.at[pl.ds(0, 3)], "xrs"),
        tgs=(qga.at[pl.ds(0, 3)], "tgs"),
        ggs=(gga.at[pl.ds(0, 3)], "ggs"),
        wxs=(w_all.at[pl.ds(0, XN - 1), 0], "wxs"),
        wxd=(w_all.at[pl.ds(0, XN - 1), 0], "wxd"),
        gws=(gw_all.at[pl.ds(0, XN - 1)], "gws"),
        wcs=(wc_r, "wcs"),
        wys=(wy_r.at[pl.ds(1, YN - 1)], "wys"),
        wzs=(wz_r.at[pl.ds(1, ZN - 1)], "wzs"),
    )
    for group, (ref, sem) in moved.items():
        index = (0,) * len(r[sem].shape)
        all_of(ref, sem, index, group).wait_send()
    for index, (src, dst) in enumerate(
        ((out_ref, "out_ref"), (tok_out, "tok_out"), (weight_ref, "weight_ref"))
    ):
        pltpu.make_async_copy(src, r[dst], r["outs"].at[index]).wait()


def fused_call(rate, ids, gate_w, beta, decay, tok, cot, mq, mk, mv, qw, kw, vw, rows):
    tok_n, width = tok.shape
    rows_n, model = rows.shape
    head = kw.shape[1]
    heads_n = beta.shape[0]
    vmem, sems = scratch_spec(tok_n, rows_n, width, head, heads_n, head // heads_n)
    part = model // (ZN * YN * CN)
    ins = ["rate", "ids", "gate_w", "beta", "decay"]
    ins += ["tok_h", "cot_h", "mq_h", "mk_h", "mv_h", "qw_h", "kw_h", "vw_h", "rows_h"]
    names = ins + ["tok_out", "out_ref", "weight_ref"] + list(vmem) + ["tab_s"] + list(sems)
    return pl.pallas_call(
        functools.partial(fused_kernel, names),
        out_shape=(
            jax.ShapeDtypeStruct((tok_n, width), BF16),
            jax.ShapeDtypeStruct((rows_n, width), BF16),
            jax.ShapeDtypeStruct((part, head), F32),
        ),
        in_specs=[SMEM_SPEC] * 2 + [VMEM_SPEC] * 3 + [ANY_SPEC] * 9,
        out_specs=(ANY_SPEC,) * 3,
        scratch_shapes=[pltpu.VMEM(*v) for v in vmem.values()]
        + [pltpu.SMEM((2, CN * ZN, 128), jnp.int32)]
        + [DMA(s) for s in sems.values()],
        compiler_params=pltpu.CompilerParams(
            collective_id=0, has_side_effects=True, vmem_limit_bytes=67043328
        ),
        name="fused",
    )(rate, ids, gate_w, beta, decay, tok, cot, mq, mk, mv, qw, kw, vw, rows)


def body(
    tokens,
    cotangent,
    mix_query,
    mix_key,
    mix_value,
    beta_pre,
    decay_pre,
    decay_rate,
    passages,
    passage_ids,
    query_weight,
    key_weight,
    value_weight,
    gate_weight,
):
    pass_local, span_rows, model_width = passages.shape
    flat_rows = passages.reshape(pass_local * span_rows, model_width)
    token_grad, passage_grad, key_weight_grad = fused_call(
        decay_rate,
        passage_ids.T,
        gate_weight,
        beta_pre,
        decay_pre,
        tokens,
        cotangent,
        mix_query,
        mix_key,
        mix_value,
        query_weight,
        key_weight,
        value_weight,
        flat_rows,
    )
    token_grad, passage_grad, key_weight_grad = settle_call(
        token_grad, passage_grad, key_weight_grad
    )
    return (token_grad, passage_grad.reshape(pass_local, span_rows, -1), key_weight_grad)


def solution(mesh):
    placed = (
        P("st", "tp"),
        P("st", "tp"),
        P("st", "tp"),
        P("st", "tp"),
        P("st", "tp"),
        P("tp", "st"),
        P("tp", "st"),
        P("tp"),
        P("st", None, None),
        P("st", None),
        P(None, "tp"),
        P(None, "tp"),
        P(None, "tp"),
        P("tp", None),
    )
    return jax.shard_map(
        body,
        mesh=mesh,
        in_specs=placed,
        out_specs=(P("st", "tp"), P("st", None, "tp"), P("st", "tp")),
        check_vma=False,
    )
```
